768 devices in a mesh: gr: 3 (over z_hi), sp: 32 (over z_lo, y), tp: 8 (over x, core).
Axes of the slice: x: 4, y: 8, z: 12 (z_hi: 3, z_lo: 4; z = z_hi * 4 + z_lo), core: 2. Of those that a mesh axis runs over, the one named last changes fastest.
Arguments:
- tokens: bfloat16 [6, 16384, 4096], P('gr', ('sp', 'tp')), parts along dimension 0, may hold values from -6 to 6
- norm_gain: bfloat16 [4096], replicated, may hold values from 0.099609375 to 1.8984375
- key_weight: bfloat16 [4096, 1024], P(None, 'tp'), may hold values from -0.09375 to 0.09375
- value_weight: bfloat16 [4096, 1024], P(None, 'tp'), may hold values from -0.09375 to 0.09375
- cum_gates: float32 [6, 16384, 16], P('gr', 'sp', 'tp'), parts along dimension 0, may hold values from -2733 to 0, as said below
- new_query: bfloat16 [6, 1024], P('gr', 'tp'), parts along dimension 0, may hold values from -240 to 240
- new_key: bfloat16 [6, 1024], P('gr', 'tp'), parts along dimension 0, may hold values from -6 to 6
- new_value: bfloat16 [6, 1024], P('gr', 'tp'), parts along dimension 0, may hold values from -6 to 6
- new_gate: float32 [6, 16], P('gr', 'tp'), parts along dimension 0, may hold values from -5 to -1.5
Outputs:
- key_cache: bfloat16 [6, 16384, 1024], P('gr', 'sp', 'tp'), parts along dimension 0
- value_cache: bfloat16 [6, 16384, 1024], P('gr', 'sp', 'tp'), parts along dimension 0
- readout: bfloat16 [6, 1024], P('gr', 'tp'), parts along dimension 0
The draws below stay inside these ranges and needn't reach their ends.
There are 3 independent parts, one for each index of `gr`. The reference program is written for one: setup_inputs(seed, part) draws one part's arguments, and reference() takes and returns one part's arrays. A program takes and returns all parts, laid end to end along the dimension named above; an argument that names none is the same for every part. Nothing has to cross between parts.
Inputs may be any that keep to these rules, and one draw needn't show every extreme that they name: `cum_gates`: along positions, for each prompt and head, the values never rise.
All inputs are finite; a program needn't handle non-finite values.
Results may differ from the reference program's by a relative error of at most 0.005.
The reference program's roundings to bfloat16 on the way (of `normed`) count: a program that leaves them out, or rounds other values in their place, can miss the bound.
Values may be sent and summed in bfloat16 or wider, within the bound.
No kernel may reach another device: no remote copies, remote signals or barrier semaphores. Data moves between devices by JAX's collectives and lax.ppermute only.
A program may use at most 64 MiB of HBM per device.

```python
import jax
import jax.numpy as jnp
from jax import lax

D = 4096
HEAD_COUNT = 16
HD = 64
PROMPTS_PER_GROUP = 2
KW = 1024
PROMPT_LENGTH = 16384


def draw_cum_gates(key, part):
    key_pieces = jax.random.split(jax.random.fold_in(key, 11), 7)
    decaying_heads = jax.random.uniform(key_pieces[0], (PROMPTS_PER_GROUP, 1, HEAD_COUNT)) < 0.5
    slow_rate = jax.random.uniform(key_pieces[1], (PROMPTS_PER_GROUP, 1, HEAD_COUNT), jnp.float32, 0.5, 1.5) / PROMPT_LENGTH
    fast_rate = 1.0 / jax.random.uniform(key_pieces[2], (PROMPTS_PER_GROUP, 1, HEAD_COUNT), jnp.float32, 30.0, 100.0)
    base_rate = jnp.where(decaying_heads, slow_rate, fast_rate)
    block_size = max(PROMPT_LENGTH // 32, 1)
    token_positions = jnp.arange(PROMPT_LENGTH)
    block_ids = jnp.minimum(token_positions // block_size, 31)
    log_factor = jax.random.uniform(key_pieces[3], (PROMPTS_PER_GROUP, 32, HEAD_COUNT), jnp.float32, -1.05, 1.05)
    block_factor = jnp.exp(log_factor)[:, block_ids, :]
    noise = jax.random.uniform(key_pieces[4], (PROMPTS_PER_GROUP, PROMPT_LENGTH, HEAD_COUNT), jnp.float32, 0.5, 1.5)
    per_step_decay = base_rate * block_factor * noise
    segment_position = jax.random.randint(key_pieces[5], (PROMPTS_PER_GROUP, 3, HEAD_COUNT), 0, PROMPT_LENGTH)
    segment_length = jax.random.uniform(key_pieces[6], (PROMPTS_PER_GROUP, 3, HEAD_COUNT), jnp.float32, 0.22, 0.69)
    match_count = (token_positions[None, :, None, None] == segment_position[:, None, :, :]).astype(jnp.float32)
    prompt_segments = jnp.sum(match_count * segment_length[:, None, :, :], axis=2)
    per_step_decay = per_step_decay + prompt_segments * decaying_heads.astype(jnp.float32)
    return -jnp.cumsum(per_step_decay, axis=1)


def draw_new_query(key, part):
    key_pieces = jax.random.split(jax.random.fold_in(key, 23), 1)
    normal_part = jax.random.normal(key_pieces[0], (PROMPTS_PER_GROUP, HEAD_COUNT, HD), jnp.float32)
    values_out = jnp.clip(normal_part * 2.0, -12.0, 12.0)
    return values_out.reshape(PROMPTS_PER_GROUP, KW).astype(jnp.bfloat16)


def levels(key, shape, shards, least, largest):
    level, own = 1.0, jax.random.fold_in(key, 6)
    for dim, shards_of in shards:
        draws = jnp.exp(jax.random.uniform(jax.random.fold_in(own, dim), (shards_of,), jnp.float32, least / len(shards), largest / len(shards)))
        level = level * jnp.repeat(draws, shape[dim] // shards_of).reshape([-1 if axis == dim else 1 for axis in range(len(shape))])
    return level


def bell_draw(rng, shape, scale, most, cuts=(), kind=jnp.bfloat16):
    factor_of = levels(rng, shape, cuts, -0.22, 0.18) if cuts else 1.0
    result = jax.random.normal(rng, shape, jnp.float32) * scale * factor_of
    return jnp.minimum(jnp.maximum(result, -most), most).astype(kind)


def setup_inputs(seed: int = 0, part: int = 0) -> dict:
    key_list = jax.random.split(jax.random.key(seed), 10)
    part_keys = jax.random.split(jax.random.fold_in(key_list[9], part), 10)
    return {
        "tokens": bell_draw(part_keys[0], (PROMPTS_PER_GROUP, PROMPT_LENGTH, D), 1.0, 6.0, ((1, 256),)),
        "norm_gain": jnp.clip(1.0 + 0.18 * jax.random.normal(key_list[1], (D,), jnp.float32), 0.099609375, 1.8984375).astype(jnp.bfloat16),
        "key_weight": bell_draw(key_list[2], (D, KW), D ** -0.5, 0.09375, ((1, 8),)),
        "value_weight": bell_draw(key_list[3], (D, KW), D ** -0.5, 0.09375, ((1, 8),)),
        "cum_gates": draw_cum_gates(jax.random.fold_in(jax.random.fold_in(key_list[9], part), 71), part),
        "new_query": draw_new_query(jax.random.fold_in(jax.random.fold_in(key_list[9], part), 71), part),
        "new_key": bell_draw(part_keys[6], (PROMPTS_PER_GROUP, KW), 1.0, 6.0, ((1, 8),)),
        "new_value": bell_draw(part_keys[7], (PROMPTS_PER_GROUP, KW), 1.0, 6.0, ((1, 8),)),
        "new_gate": jnp.clip(-5.0 + 3.5 * jax.random.uniform(part_keys[8], (PROMPTS_PER_GROUP, HEAD_COUNT), jnp.float32) ** levels(part_keys[8], (PROMPTS_PER_GROUP, HEAD_COUNT), ((1, 8),), -0.2, 0.2), -5.0, -1.5),
    }


epsilon = 1e-06

def reference(tokens, norm_gain, key_weight, value_weight, cum_gates, new_query, new_key, new_value, new_gate):
    as_float = tokens.astype(jnp.float32)
    normed = (as_float * lax.rsqrt(lax.optimization_barrier(jnp.mean(as_float * as_float, axis=-1, keepdims=True)) + epsilon) * norm_gain.astype(jnp.float32)).astype(jnp.bfloat16)
    flat_rows = normed.reshape(PROMPTS_PER_GROUP * PROMPT_LENGTH, D)
    key_cache = jnp.dot(flat_rows, key_weight, preferred_element_type=jnp.float32).astype(jnp.bfloat16).reshape(PROMPTS_PER_GROUP, PROMPT_LENGTH, KW)
    value_cache = jnp.dot(flat_rows, value_weight, preferred_element_type=jnp.float32).astype(jnp.bfloat16).reshape(PROMPTS_PER_GROUP, PROMPT_LENGTH, KW)
    score_scale = HD ** (-0.5)
    queries = new_query.reshape(PROMPTS_PER_GROUP, HEAD_COUNT, HD).astype(jnp.float32)
    key_heads = key_cache.reshape(PROMPTS_PER_GROUP, PROMPT_LENGTH, HEAD_COUNT, HD).astype(jnp.float32)
    value_heads = value_cache.reshape(PROMPTS_PER_GROUP, PROMPT_LENGTH, HEAD_COUNT, HD).astype(jnp.float32)
    fresh_key = new_key.reshape(PROMPTS_PER_GROUP, HEAD_COUNT, HD).astype(jnp.float32)
    fresh_value = new_value.reshape(PROMPTS_PER_GROUP, HEAD_COUNT, HD).astype(jnp.float32)
    scores = jnp.einsum('shd,slhd->shl', queries, key_heads, precision=lax.Precision.HIGHEST) * score_scale
    scores = scores + (new_gate + cum_gates[:, PROMPT_LENGTH - 1, :])[:, :, None] - jnp.transpose(cum_gates, (0, 2, 1))
    fresh_score = lax.optimization_barrier(jnp.sum(queries * fresh_key, axis=-1)) * score_scale
    maxima = jnp.maximum(lax.optimization_barrier(jnp.max(scores, axis=-1)), fresh_score)
    weights = jnp.exp(scores - maxima[:, :, None])
    fresh_weight = jnp.exp(fresh_score - maxima)
    totals = lax.optimization_barrier(jnp.sum(weights, axis=-1)) + fresh_weight
    weighted = jnp.einsum('shl,slhd->shd', weights, value_heads, precision=lax.Precision.HIGHEST)
    weighted = weighted + fresh_weight[:, :, None] * fresh_value
    readout = (weighted / totals[:, :, None]).reshape(PROMPTS_PER_GROUP, KW).astype(jnp.bfloat16)
    return (key_cache, value_cache, readout)
```

```python
import functools

import jax
import jax.numpy as jnp
from jax import lax
from jax.experimental import pallas as pl
from jax.experimental.pallas import tpu as pltpu
from jax.sharding import PartitionSpec as P

HD = 64
EPS = 1e-06
MASKED = -1e30
CHUNKS = 4


VMEM = pl.BlockSpec(memory_space=pltpu.VMEM)
ANY = pl.BlockSpec(memory_space=pl.ANY)


def project_kernel(
    xa, xb, gain, wk, wv, pk, pv, own, par, x_s, n_s, w_s, x_sem, w_sem
):
    half, width = xa.shape
    cols = wk.shape[1]
    depth = width // CHUNKS
    x_copies = [
        pltpu.make_async_copy(x, x_s.at[pl.ds(k * half, half)], x_sem.at[k])
        for k, x in enumerate((xa, xb))
    ]
    for copy in x_copies:
        copy.start()
    w_copies = []
    for c in range(CHUNKS):
        rows = pl.ds(c * depth, depth)
        for j, w in enumerate((wk, wv, pk, pv)):
            copy = pltpu.make_async_copy(
                w.at[rows], w_s.at[rows, pl.ds(j * cols, cols)], w_sem.at[c, j]
            )
            copy.start()
            w_copies.append(copy)
    for copy in x_copies:
        copy.wait()

    step = 16

    def normalize(i, carry):
        rows = pl.ds(pl.multiple_of(i * step, step), step)
        total = jnp.zeros((step, 128), jnp.float32)
        for c in range(width // 1024):
            part = x_s[rows, pl.ds(c * 1024, 1024)].astype(jnp.float32)
            part = part * part
            for j in range(8):
                total = total + part[:, j * 128 : (j + 1) * 128]
        mean = jnp.sum(total, axis=-1, keepdims=True) * (1.0 / width)
        scale = lax.rsqrt(mean + EPS)
        for c in range(width // 1024):
            at = pl.ds(c * 1024, 1024)
            part = x_s[rows, at].astype(jnp.float32)
            part = part * scale * gain[:, at].astype(jnp.float32)
            n_s[rows, at] = part.astype(jnp.bfloat16)
        return carry

    lax.fori_loop(0, 2 * half // step, normalize, 0, unroll=2)

    acc = None
    for c in range(CHUNKS):
        for j in range(4):
            w_copies[c * 4 + j].wait()
        rows = pl.ds(c * depth, depth)
        part = jnp.dot(n_s[:, rows], w_s[rows], preferred_element_type=jnp.float32)
        acc = part if acc is None else acc + part
    result = acc.astype(jnp.bfloat16).reshape(2, half, 4 * cols)
    own[...] = result[:, :, : 2 * cols]
    par[...] = result[:, :, 2 * cols :]


def project(xa, xb, gain, wk, wv, pk, pv):
    half, width = xa.shape
    cols = wk.shape[1]
    out = jax.ShapeDtypeStruct((2, half, 2 * cols), jnp.bfloat16)
    return pl.pallas_call(
        project_kernel,
        out_shape=(out, out),
        in_specs=[ANY, ANY, VMEM, ANY, ANY, ANY, ANY],
        out_specs=(VMEM, VMEM),
        scratch_shapes=[
            pltpu.VMEM((2 * half, width), jnp.bfloat16),
            pltpu.VMEM((2 * half, width), jnp.bfloat16),
            pltpu.VMEM((width, 4 * cols), jnp.bfloat16),
            pltpu.SemaphoreType.DMA((2,)),
            pltpu.SemaphoreType.DMA((CHUNKS, 4)),
        ],
        compiler_params=pltpu.CompilerParams(vmem_limit_bytes=20 * 1024 * 1024),
        cost_estimate=pl.CostEstimate(
            flops=2 * 2 * half * width * 4 * cols,
            bytes_accessed=6 * 1024 * 1024,
            transcendentals=0,
        ),
        name="project",
    )(xa, xb, gain, wk, wv, pk, pv)


def attend_kernel(*refs):
    pieces, (gates, qm, q, fk, fv, fg, keys, values, part) = refs[:8], refs[8:]
    tp = lax.axis_index("tp")
    x, core = tp // 2, lax.rem(tp, 2)
    half = pieces[0].shape[1]
    cols = keys.shape[2]
    block = keys.shape[1]
    xs = [lax.rem(x + d, 4) for d in range(4)]
    places = [(0, 0), (3, 1), (1, 3), (2, 2)]
    for side in range(2):
        which = lax.rem(core + side, 2)
        for k, place in enumerate(places):
            for p in range(2):
                at = pl.multiple_of((xs[place[p]] * 2 + which) * half, half)
                ref = pieces[side * 4 + k]
                keys[p, pl.ds(at, half), :] = ref[p, :, :cols]
                values[p, pl.ds(at, half), :] = ref[p, :, cols:]
    last = lax.axis_index("sp") == lax.axis_size("sp") - 1
    for p in range(2):
        scores = jnp.dot(keys[p], qm[p], preferred_element_type=jnp.float32)
        scores = scores * (HD**-0.5) - gates[p]
        fresh = jnp.dot(
            fk[...].astype(jnp.bfloat16), qm[p], preferred_element_type=jnp.float32
        )[p : p + 1] * (HD**-0.5)
        fresh = fresh - (gates[p, block - 1 : block, :] + fg[p : p + 1, :])
        fresh = jnp.where(last, fresh, MASKED)
        top = jnp.maximum(jnp.max(scores, axis=0, keepdims=True), fresh)
        weights = jnp.exp(scores - top)
        fresh_weight = jnp.exp(fresh - top)
        total = jnp.sum(weights, axis=0, keepdims=True) + fresh_weight
        acc = jnp.sum(weights * values[p].astype(jnp.float32), axis=0, keepdims=True)
        acc = acc + fresh_weight * fv[p : p + 1, :].astype(jnp.float32)
        for r, row in enumerate((top, total, acc)):
            part[:, p * 4 + r : p * 4 + r + 1, :] = jnp.broadcast_to(
                row[None], (part.shape[0], 1, cols)
            )
        part[:, p * 4 + 3 : p * 4 + 4, :] = jnp.zeros(
            (part.shape[0], 1, cols), jnp.float32
        )


def attend(pieces, gates, qm, q, fk, fv, fg, members):
    block, cols = gates.shape[1:]
    cache = jax.ShapeDtypeStruct((2, block, cols), jnp.bfloat16)
    return pl.pallas_call(
        attend_kernel,
        out_shape=(cache, cache, jax.ShapeDtypeStruct((members, 8, cols), jnp.float32)),
        in_specs=[VMEM] * 14,
        out_specs=(VMEM, VMEM, VMEM),
        compiler_params=pltpu.CompilerParams(vmem_limit_bytes=16 * 1024 * 1024),
        cost_estimate=pl.CostEstimate(
            flops=64 * 1024 * 1024, bytes_accessed=2 * 1024 * 1024, transcendentals=0
        ),
        name="attend",
    )(*pieces, gates, qm, q, fk, fv, fg)


def merge_kernel(parts, out):
    for p in range(2):
        tops = parts[:, p * 4, :]
        top = jnp.max(tops, axis=0, keepdims=True)
        scale = jnp.exp(tops - top)
        total = jnp.sum(scale * parts[:, p * 4 + 1, :], axis=0, keepdims=True)
        acc = jnp.sum(scale * parts[:, p * 4 + 2, :], axis=0, keepdims=True)
        out[p : p + 1, :] = (acc / total).astype(jnp.bfloat16)


def merge(parts):
    cols = parts.shape[2]
    return pl.pallas_call(
        merge_kernel,
        out_shape=jax.ShapeDtypeStruct((2, cols), jnp.bfloat16),
        in_specs=[VMEM],
        out_specs=VMEM,
        name="merge",
    )(parts)


def body(
    tokens, norm_gain, key_weight, value_weight, cum_gates, new_query, new_key, new_value, new_gate
):
    cols = key_weight.shape[1]
    members = lax.axis_size("sp")
    tps = lax.axis_size("tp")
    right = [(i, (i + 2) % tps) for i in range(tps)]
    left = [(i, (i - 2) % tps) for i in range(tps)]
    swap = [(i, i ^ 1) for i in range(tps)]
    gain = norm_gain.reshape(1, -1)
    a0, b0 = tokens[0], tokens[1]
    a_l = lax.ppermute(a0, "tp", right)
    b_r = lax.ppermute(b0, "tp", left)
    b_l = lax.ppermute(b0, "tp", right)
    a_r = lax.ppermute(a0, "tp", left)
    pk = lax.ppermute(key_weight, "tp", swap)
    pv = lax.ppermute(value_weight, "tp", swap)
    a_2 = lax.ppermute(a_l, "tp", right)
    b_2 = lax.ppermute(b_r, "tp", left)

    own, sent = [], []
    for xa, xb in ((a0, b0), (a_l, b_r), (a_r, b_l), (a_2, b_2)):
        o, s = project(xa, xb, gain, key_weight, value_weight, pk, pv)
        own.append(o)
        sent.append(lax.ppermute(s, "tp", swap))

    lanes = jnp.arange(cols) // HD
    same = lanes[:, None] == lanes[None, :]
    qm = jnp.where(same, new_query[:, :, None], jnp.zeros((), jnp.bfloat16))
    gates = jnp.repeat(cum_gates, HD, axis=2)
    fg = jnp.repeat(new_gate, HD, axis=1)
    keys, values, part = attend(
        own + sent, gates, qm, new_query, new_key, new_value, fg, members
    )
    parts = lax.all_to_all(part, "sp", split_axis=0, concat_axis=0, tiled=True)
    return keys, values, merge(parts)


def solution(mesh):
    in_specs = (
        P("gr", ("sp", "tp"), None),
        P(),
        P(None, "tp"),
        P(None, "tp"),
        P("gr", "sp", "tp"),
        P("gr", "tp"),
        P("gr", "tp"),
        P("gr", "tp"),
        P("gr", "tp"),
    )
    out_specs = (P("gr", "sp", "tp"), P("gr", "sp", "tp"), P("gr", "tp"))
    return jax.shard_map(body, mesh=mesh, in_specs=in_specs, out_specs=out_specs, check_vma=False)
```

```python
import functools

import jax
import jax.numpy as jnp
from jax import lax
from jax.experimental import pallas as pl
from jax.experimental.pallas import tpu as pltpu
from jax.sharding import PartitionSpec as P


HD = 64
EPS = 1e-06
MASKED = -1e30


VMEM = pl.BlockSpec(memory_space=pltpu.VMEM)

EARLY = ((0, 0), (0, 1), (3, 0), (1, 1), (1, 0), (3, 1))
LATE = ((2, 0), (2, 1))


def project_kernel(count, *refs):
    xs, (gain, wo, wp, own, par, n_s) = refs[:count], refs[count:]
    half, width = xs[0].shape
    step = 16

    def normalize(x, base):
        def rows_of(i, carry):
            rows = pl.ds(pl.multiple_of(i * step, step), step)
            total = jnp.zeros((step, 128), jnp.float32)
            for c in range(width // 1024):
                part = x[rows, pl.ds(c * 1024, 1024)].astype(jnp.float32)
                part = part * part
                for j in range(8):
                    total = total + part[:, j * 128 : (j + 1) * 128]
            mean = jnp.sum(total, axis=-1, keepdims=True) * (1.0 / width)
            scale = lax.rsqrt(mean + EPS)
            out = pl.ds(pl.multiple_of(base + i * step, step), step)
            for c in range(width // 1024):
                at = pl.ds(c * 1024, 1024)
                part = x[rows, at].astype(jnp.float32)
                part = part * scale * gain[:, at].astype(jnp.float32)
                n_s[out, at] = part.astype(jnp.bfloat16)
            return carry

        lax.fori_loop(0, half // step, rows_of, 0, unroll=2)

    for k, x in enumerate(xs):
        normalize(x, k * half)
    for w, out in ((wo, own), (wp, par)):
        acc = jnp.dot(n_s[...], w[...], preferred_element_type=jnp.float32)
        out[...] = acc.astype(jnp.bfloat16).reshape(out.shape)


def project(xs, gain, wo, wp):
    count = len(xs)
    half, width = xs[0].shape
    cols = wo.shape[1]
    out = jax.ShapeDtypeStruct((count, half, cols), jnp.bfloat16)
    return pl.pallas_call(
        functools.partial(project_kernel, count),
        out_shape=(out, out),
        in_specs=[VMEM] * (count + 3),
        out_specs=(VMEM, VMEM),
        scratch_shapes=[pltpu.VMEM((count * half, width), jnp.bfloat16)],
        compiler_params=pltpu.CompilerParams(vmem_limit_bytes=24 * 1024 * 1024),
        cost_estimate=pl.CostEstimate(
            flops=2 * count * half * width * 2 * cols,
            bytes_accessed=6 * 1024 * 1024,
            transcendentals=0,
        ),
        name="project",
    )(*xs, gain, wo, wp)


def prepare_kernel(cum, q, fk, fv, ng, gates, qm, small):
    block, cols = gates.shape[1:]
    shape = (cols, cols)
    same = lax.broadcasted_iota(jnp.int32, shape, 0) // HD == (
        lax.broadcasted_iota(jnp.int32, shape, 1) // HD
    )
    first = lax.broadcasted_iota(jnp.int32, (2, cols), 1) < HD
    for p in range(2):
        spread = [jnp.broadcast_to(cum[p, h : h + 1, :], (HD, block)) for h in range(2)]
        gates[p] = jnp.concatenate(spread, axis=0).T
        down = jnp.broadcast_to(q[p : p + 1, :].astype(jnp.float32), shape).T
        qm[p] = jnp.where(same, down, 0.0).astype(jnp.bfloat16)
        fresh = jnp.dot(fk[...], qm[p], preferred_element_type=jnp.float32)
        small[p : p + 1, :] = fresh[p : p + 1] * (HD**-0.5)
    small[2:4, :] = fv[...].astype(jnp.float32)
    small[4:6, :] = jnp.where(first, ng[:, 0:1], ng[:, 1:2])
    small[6:8, :] = jnp.zeros((2, cols), jnp.float32)


def prepare(cum, q, fk, fv, ng):
    block, cols = cum.shape[2], q.shape[1]
    return pl.pallas_call(
        prepare_kernel,
        out_shape=(
            jax.ShapeDtypeStruct((2, block, cols), jnp.float32),
            jax.ShapeDtypeStruct((2, cols, cols), jnp.bfloat16),
            jax.ShapeDtypeStruct((8, cols), jnp.float32),
        ),
        in_specs=[VMEM] * 5,
        out_specs=(VMEM,) * 3,
        compiler_params=pltpu.CompilerParams(vmem_limit_bytes=8 * 1024 * 1024),
        cost_estimate=pl.CostEstimate(
            flops=1024 * 1024, bytes_accessed=1024 * 1024, transcendentals=0
        ),
        name="prepare",
    )(cum, q, fk, fv, ng)


def attend_kernel(own1, own2, got1, got2, gates, qm, small, keys, values, part):
    tp = lax.axis_index("tp")
    x, core = tp // 2, lax.rem(tp, 2)
    half = own1.shape[1]
    members, _, cols = part.shape
    block = keys.shape[1]
    for side, refs in enumerate(((own1, own2), (got1, got2))):
        which = lax.rem(core + side, 2)
        for ref, places in zip(refs, (EARLY, LATE)):
            for k, (off, p) in enumerate(places):
                at = pl.multiple_of((lax.rem(x + off, 4) * 2 + which) * half, half)
                keys[p, pl.ds(at, half), :] = ref[k, :, :cols]
                values[p, pl.ds(at, half), :] = ref[k, :, cols:]
    last = lax.axis_index("sp") == lax.axis_size("sp") - 1
    s0, fv, fg = small[0:2, :], small[2:4, :], small[4:6, :]
    for p in range(2):
        one = slice(p, p + 1)
        scores = jnp.dot(keys[p], qm[p], preferred_element_type=jnp.float32)
        scores = scores * (HD**-0.5) - gates[p]
        fresh = s0[one] - (gates[p, block - 1 : block, :] + fg[one])
        fresh = jnp.where(last, fresh, MASKED)
        top = jnp.maximum(jnp.max(scores, axis=0, keepdims=True), fresh)
        weights = jnp.exp(scores - top)
        fresh_weight = jnp.exp(fresh - top)
        total = jnp.sum(weights, axis=0, keepdims=True) + fresh_weight
        acc = jnp.sum(weights * values[p].astype(jnp.float32), axis=0, keepdims=True)
        acc = acc + fresh_weight * fv[one]
        for r, row in ((2 * p, top), (2 * p + 1, top), (2 * p + 4, total), (2 * p + 5, acc)):
            part[:, r : r + 1, :] = jnp.broadcast_to(row[None], (members, 1, cols))


def attend(own1, own2, got1, got2, gates, qm, small, members):
    block, cols = gates.shape[1:]
    cache = jax.ShapeDtypeStruct((2, block, cols), jnp.bfloat16)
    return pl.pallas_call(
        attend_kernel,
        out_shape=(cache, cache, jax.ShapeDtypeStruct((members, 8, cols), jnp.float32)),
        in_specs=[VMEM] * 7,
        out_specs=(VMEM, VMEM, VMEM),
        compiler_params=pltpu.CompilerParams(vmem_limit_bytes=16 * 1024 * 1024),
        cost_estimate=pl.CostEstimate(
            flops=64 * 1024 * 1024, bytes_accessed=2 * 1024 * 1024, transcendentals=0
        ),
        name="attend",
    )(own1, own2, got1, got2, gates, qm, small)


def merge_kernel(parts, out):
    tops = parts[:, 0:4, :]
    scale = jnp.exp(tops - jnp.max(tops, axis=0, keepdims=True))
    sums = jnp.sum(scale * parts[:, 4:8, :], axis=0)
    for p in range(2):
        out[p : p + 1, :] = (
            sums[2 * p + 1 : 2 * p + 2] / sums[2 * p : 2 * p + 1]
        ).astype(jnp.bfloat16)


def merge(parts):
    cols = parts.shape[2]
    return pl.pallas_call(
        merge_kernel,
        out_shape=jax.ShapeDtypeStruct((2, cols), jnp.bfloat16),
        in_specs=[VMEM],
        out_specs=VMEM,
        name="merge",
    )(parts)


def shift(x, by):
    return lax.ppermute(x, "tp", by)


def body(
    tokens, norm_gain, key_weight, value_weight, cum_gates, new_query, new_key, new_value, new_gate
):
    members = lax.axis_size("sp")
    tps = lax.axis_size("tp")
    right = [(i, (i + 2) % tps) for i in range(tps)]
    left = [(i, (i - 2) % tps) for i in range(tps)]
    swap = [(i, i ^ 1) for i in range(tps)]
    gain = norm_gain.reshape(1, -1)
    a0, b0 = tokens[0], tokens[1]
    a_l = shift(a0, right)
    b_r = shift(b0, left)
    b_l = shift(b0, right)
    a_r = shift(a0, left)
    a_2 = shift(a_l, right)
    b_2 = shift(b_r, left)
    wo = jnp.concatenate([key_weight, value_weight], axis=1)
    wp = shift(wo, swap)

    made = prepare(
        jnp.swapaxes(cum_gates, 1, 2), new_query, new_key, new_value, new_gate
    )
    gain, wp, made = lax.optimization_barrier((gain, wp, made))
    gates, qm, small = made

    own1, par1 = project((a0, b0, a_l, b_r, a_r, b_l), gain, wo, wp)
    got1 = shift(par1, swap)
    own2, par2 = project((a_2, b_2), gain, wo, wp)
    got2 = shift(par2, swap)
    keys, values, part = attend(own1, own2, got1, got2, gates, qm, small, members)
    parts = lax.all_to_all(part, "sp", split_axis=0, concat_axis=0, tiled=True)
    return keys, values, merge(parts)


def solution(mesh):
    in_specs = (
        P("gr", ("sp", "tp"), None),
        P(),
        P(None, "tp"),
        P(None, "tp"),
        P("gr", "sp", "tp"),
        P("gr", "tp"),
        P("gr", "tp"),
        P("gr", "tp"),
        P("gr", "tp"),
    )
    out_specs = (P("gr", "sp", "tp"), P("gr", "sp", "tp"), P("gr", "tp"))
    return jax.shard_map(body, mesh=mesh, in_specs=in_specs, out_specs=out_specs, check_vma=False)
```

```python
import functools

import jax
import jax.numpy as jnp
from jax import lax
from jax.experimental import pallas as pl
from jax.experimental.pallas import tpu as pltpu
from jax.sharding import PartitionSpec as P


HD = 64
EPS = 1e-06
MASKED = -1e30


VMEM = pl.BlockSpec(memory_space=pltpu.VMEM)

EARLY = ((0, 0), (0, 1), (3, 0), (1, 1), (1, 0), (3, 1))
LATE = ((2, 0), (2, 1))


def project_kernel(count, *refs):
    xs, (gain, wo, wp, own, par, n_s) = refs[:count], refs[count:]
    half, width = xs[0].shape
    step = 16

    def normalize(x, base):
        def rows_of(i, carry):
            rows = pl.ds(pl.multiple_of(i * step, step), step)
            total = jnp.zeros((step, 128), jnp.float32)
            for c in range(width // 1024):
                part = x[rows, pl.ds(c * 1024, 1024)].astype(jnp.float32)
                part = part * part
                for j in range(8):
                    total = total + part[:, j * 128 : (j + 1) * 128]
            mean = jnp.sum(total, axis=-1, keepdims=True) * (1.0 / width)
            scale = lax.rsqrt(mean + EPS)
            out = pl.ds(pl.multiple_of(base + i * step, step), step)
            for c in range(width // 1024):
                at = pl.ds(c * 1024, 1024)
                part = x[rows, at].astype(jnp.float32)
                part = part * scale * gain[:, at].astype(jnp.float32)
                n_s[out, at] = part.astype(jnp.bfloat16)
            return carry

        lax.fori_loop(0, half // step, rows_of, 0, unroll=2)

    for k, x in enumerate(xs):
        normalize(x, k * half)
    for w, out in ((wo, own), (wp, par)):
        acc = jnp.dot(n_s[...], w[...], preferred_element_type=jnp.float32)
        out[...] = acc.astype(jnp.bfloat16).reshape(out.shape)


def project(xs, gain, wo, wp):
    count = len(xs)
    half, width = xs[0].shape
    cols = wo.shape[1]
    out = jax.ShapeDtypeStruct((count, half, cols), jnp.bfloat16)
    return pl.pallas_call(
        functools.partial(project_kernel, count),
        out_shape=(out, out),
        in_specs=[VMEM] * (count + 3),
        out_specs=(VMEM, VMEM),
        scratch_shapes=[pltpu.VMEM((count * half, width), jnp.bfloat16)],
        compiler_params=pltpu.CompilerParams(vmem_limit_bytes=24 * 1024 * 1024),
        cost_estimate=pl.CostEstimate(
            flops=2 * count * half * width * 2 * cols,
            bytes_accessed=6 * 1024 * 1024,
            transcendentals=0,
        ),
        name="project",
    )(*xs, gain, wo, wp)


def prepare_kernel(cum, q, fk, fv, ng, gates, qm, small):
    block, cols = gates.shape[1:]
    shape = (cols, cols)
    same = lax.broadcasted_iota(jnp.int32, shape, 0) // HD == (
        lax.broadcasted_iota(jnp.int32, shape, 1) // HD
    )
    first = lax.broadcasted_iota(jnp.int32, (2, cols), 1) < HD
    for p in range(2):
        spread = [jnp.broadcast_to(cum[p, h : h + 1, :], (HD, block)) for h in range(2)]
        gates[p] = jnp.concatenate(spread, axis=0).T
        down = jnp.broadcast_to(q[p : p + 1, :].astype(jnp.float32), shape).T
        qm[p] = jnp.where(same, down, 0.0).astype(jnp.bfloat16)
        fresh = jnp.dot(fk[...], qm[p], preferred_element_type=jnp.float32)
        small[p : p + 1, :] = fresh[p : p + 1] * (HD**-0.5)
    small[2:4, :] = fv[...].astype(jnp.float32)
    small[4:6, :] = jnp.where(first, ng[:, 0:1], ng[:, 1:2])
    small[6:8, :] = jnp.zeros((2, cols), jnp.float32)


def prepare(cum, q, fk, fv, ng):
    block, cols = cum.shape[2], q.shape[1]
    return pl.pallas_call(
        prepare_kernel,
        out_shape=(
            jax.ShapeDtypeStruct((2, block, cols), jnp.float32),
            jax.ShapeDtypeStruct((2, cols, cols), jnp.bfloat16),
            jax.ShapeDtypeStruct((8, cols), jnp.float32),
        ),
        in_specs=[VMEM] * 5,
        out_specs=(VMEM,) * 3,
        compiler_params=pltpu.CompilerParams(vmem_limit_bytes=8 * 1024 * 1024),
        cost_estimate=pl.CostEstimate(
            flops=1024 * 1024, bytes_accessed=1024 * 1024, transcendentals=0
        ),
        name="prepare",
    )(cum, q, fk, fv, ng)


def attend_kernel(own1, own2, got1, got2, gates, qm, small, keys, values, part):
    tp = lax.axis_index("tp")
    x, core = tp // 2, lax.rem(tp, 2)
    half = own1.shape[1]
    members, _, cols = part.shape
    block = keys.shape[1]
    for side, refs in enumerate(((own1, own2), (got1, got2.at[1 - core]))):
        which = lax.rem(core + side, 2)
        for ref, places in zip(refs, (EARLY, LATE)):
            for k, (off, p) in enumerate(places):
                place = lax.rem(x + jnp.where(which == 0, off, (4 - off) % 4), 4)
                at = pl.multiple_of((place * 2 + which) * half, half)
                keys[p, pl.ds(at, half), :] = ref[k, :, :cols]
                values[p, pl.ds(at, half), :] = ref[k, :, cols:]
    last = lax.axis_index("sp") == lax.axis_size("sp") - 1
    s0, fv, fg = small[0:2, :], small[2:4, :], small[4:6, :]
    for p in range(2):
        one = slice(p, p + 1)
        scores = jnp.dot(keys[p], qm[p], preferred_element_type=jnp.float32)
        scores = scores * (HD**-0.5) - gates[p]
        fresh = s0[one] - (gates[p, block - 1 : block, :] + fg[one])
        fresh = jnp.where(last, fresh, MASKED)
        top = jnp.maximum(jnp.max(scores, axis=0, keepdims=True), fresh)
        weights = jnp.exp(scores - top)
        fresh_weight = jnp.exp(fresh - top)
        total = jnp.sum(weights, axis=0, keepdims=True) + fresh_weight
        acc = jnp.sum(weights * values[p].astype(jnp.float32), axis=0, keepdims=True)
        acc = acc + fresh_weight * fv[one]
        for r, row in ((2 * p, top), (2 * p + 1, top), (2 * p + 4, total), (2 * p + 5, acc)):
            part[:, r : r + 1, :] = jnp.broadcast_to(row[None], (members, 1, cols))


def attend(own1, own2, got1, got2, gates, qm, small, members):
    block, cols = gates.shape[1:]
    cache = jax.ShapeDtypeStruct((2, block, cols), jnp.bfloat16)
    return pl.pallas_call(
        attend_kernel,
        out_shape=(cache, cache, jax.ShapeDtypeStruct((members, 8, cols), jnp.float32)),
        in_specs=[VMEM] * 7,
        out_specs=(VMEM, VMEM, VMEM),
        compiler_params=pltpu.CompilerParams(vmem_limit_bytes=16 * 1024 * 1024),
        cost_estimate=pl.CostEstimate(
            flops=64 * 1024 * 1024, bytes_accessed=2 * 1024 * 1024, transcendentals=0
        ),
        name="attend",
    )(own1, own2, got1, got2, gates, qm, small)


def merge_kernel(parts, out):
    tops = parts[:, 0:4, :]
    scale = jnp.exp(tops - jnp.max(tops, axis=0, keepdims=True))
    sums = jnp.sum(scale * parts[:, 4:8, :], axis=0)
    for p in range(2):
        out[p : p + 1, :] = (
            sums[2 * p + 1 : 2 * p + 2] / sums[2 * p : 2 * p + 1]
        ).astype(jnp.bfloat16)


def merge(parts):
    cols = parts.shape[2]
    return pl.pallas_call(
        merge_kernel,
        out_shape=jax.ShapeDtypeStruct((2, cols), jnp.bfloat16),
        in_specs=[VMEM],
        out_specs=VMEM,
        compiler_params=pltpu.CompilerParams(vmem_limit_bytes=4 * 1024 * 1024),
        name="merge",
    )(parts)


def shift(x, by):
    return lax.ppermute(x, "tp", by)


def body(
    tokens, norm_gain, key_weight, value_weight, cum_gates, new_query, new_key, new_value, new_gate
):
    members = lax.axis_size("sp")
    tps = lax.axis_size("tp")
    ahead = [(i, (i + 2 - 4 * (i % 2)) % tps) for i in range(tps)]
    back = [(i, (i - 2 + 4 * (i % 2)) % tps) for i in range(tps)]
    swap = [(i, i ^ 1) for i in range(tps)]
    gain = norm_gain.reshape(1, -1)
    a0 = tokens[0]
    held, a0 = lax.optimization_barrier((tokens, a0))
    b0 = held[1]
    a_3 = shift(a0, ahead)
    b_1 = shift(b0, back)
    b_3 = shift(b0, ahead)
    a_1 = shift(a0, back)
    a_2 = shift(a_3, ahead)
    b_2 = shift(b_1, back)
    wo = jnp.concatenate([key_weight, value_weight], axis=1)
    wp = shift(wo, swap)

    made = prepare(
        jnp.swapaxes(cum_gates, 1, 2), new_query, new_key, new_value, new_gate
    )
    gain, wp, made = lax.optimization_barrier((gain, wp, made))
    gates, qm, small = made

    own1, par1 = project((a0, b0, a_3, b_1, a_1, b_3), gain, wo, wp)
    got1 = shift(par1, swap)
    own2, par2 = project((a_2, b_2), gain, wo, wp)
    pairs = [[i, i + 1] for i in range(0, tps, 2)]
    got2 = lax.all_gather(par2, "tp", axis_index_groups=pairs)
    keys, values, part = attend(own1, own2, got1, got2, gates, qm, small, members)
    parts = lax.all_to_all(part, "sp", split_axis=0, concat_axis=0, tiled=True)
    return keys, values, merge(parts)


def solution(mesh):
    in_specs = (
        P("gr", ("sp", "tp"), None),
        P(),
        P(None, "tp"),
        P(None, "tp"),
        P("gr", "sp", "tp"),
        P("gr", "tp"),
        P("gr", "tp"),
        P("gr", "tp"),
        P("gr", "tp"),
    )
    out_specs = (P("gr", "sp", "tp"), P("gr", "sp", "tp"), P("gr", "tp"))
    return jax.shard_map(body, mesh=mesh, in_specs=in_specs, out_specs=out_specs, check_vma=False)
```

```python
import functools

import jax
import jax.numpy as jnp
from jax import lax
from jax.experimental import pallas as pl
from jax.experimental.pallas import tpu as pltpu
from jax.sharding import PartitionSpec as P


HD = 64
EPS = 1e-06
MASKED = -1e30


VMEM = pl.BlockSpec(memory_space=pltpu.VMEM)
ANY = pl.BlockSpec(memory_space=pl.ANY)

EARLY = ((0, 0), (0, 1), (3, 0), (3, 1), (1, 0), (1, 1))
LATE = ((2, 0), (2, 1))


def project_kernel(count, prior, *refs):
    xs, refs = refs[:count], refs[count:]
    before, (gain, wo, wp, own, par, n_s) = refs[: 2 * prior], refs[2 * prior :]
    width = xs[0].shape[1]
    half = own.shape[1]
    step = 16

    def normalize(x, base):
        def rows_of(i, carry):
            rows = pl.ds(pl.multiple_of(i * step, step), step)
            total = jnp.zeros((step, 128), jnp.float32)
            for c in range(width // 1024):
                part = x[rows, pl.ds(c * 1024, 1024)].astype(jnp.float32)
                part = part * part
                for j in range(8):
                    total = total + part[:, j * 128 : (j + 1) * 128]
            mean = jnp.sum(total, axis=-1, keepdims=True) * (1.0 / width)
            scale = lax.rsqrt(mean + EPS)
            out = pl.ds(pl.multiple_of(base + i * step, step), step)
            for c in range(width // 1024):
                at = pl.ds(c * 1024, 1024)
                part = x[rows, at].astype(jnp.float32)
                part = part * scale * gain[:, at].astype(jnp.float32)
                n_s[out, at] = part.astype(jnp.bfloat16)
            return carry

        lax.fori_loop(0, x.shape[0] // step, rows_of, 0, unroll=2)

    base = 0
    for x in xs:
        normalize(x, base)
        base += x.shape[0]
    for k, (w, out) in enumerate(((wo, own), (wp, par))):
        acc = jnp.dot(n_s[...], w[...], preferred_element_type=jnp.float32)
        done = before[k].shape[0] if prior else 0
        if prior:
            out[:done] = before[k][...]
        out[done:] = acc.astype(jnp.bfloat16).reshape(-1, half, out.shape[2])


def project(xs, gain, wo, wp, half, before=()):
    rows = sum(x.shape[0] for x in xs)
    width, cols = wo.shape
    done = before[0].shape[0] if before else 0
    out = jax.ShapeDtypeStruct((done + rows // half, half, cols), jnp.bfloat16)
    return pl.pallas_call(
        functools.partial(project_kernel, len(xs), bool(before)),
        out_shape=(out, out),
        in_specs=[VMEM] * (len(xs) + len(before) + 3),
        out_specs=(VMEM, VMEM),
        scratch_shapes=[pltpu.VMEM((rows, width), jnp.bfloat16)],
        compiler_params=pltpu.CompilerParams(vmem_limit_bytes=16 * 1024 * 1024),
        cost_estimate=pl.CostEstimate(
            flops=2 * rows * width * 2 * cols,
            bytes_accessed=6 * 1024 * 1024,
            transcendentals=0,
        ),
        name="project",
    )(*xs, *before, gain, wo, wp)


def prepare_kernel(cum, q, fk, fv, ng, gates, qm, small):
    block, cols = gates.shape[1:]
    shape = (cols, cols)
    same = lax.broadcasted_iota(jnp.int32, shape, 0) // HD == (
        lax.broadcasted_iota(jnp.int32, shape, 1) // HD
    )
    first = lax.broadcasted_iota(jnp.int32, (2, cols), 1) < HD
    for p in range(2):
        spread = [jnp.broadcast_to(cum[p, h : h + 1, :], (HD, block)) for h in range(2)]
        gates[p] = jnp.concatenate(spread, axis=0).T
        down = jnp.broadcast_to(q[p : p + 1, :].astype(jnp.float32), shape).T
        qm[p] = jnp.where(same, down, 0.0).astype(jnp.bfloat16)
        fresh = jnp.dot(fk[...], qm[p], preferred_element_type=jnp.float32)
        small[p : p + 1, :] = fresh[p : p + 1] * (HD**-0.5)
    small[2:4, :] = fv[...].astype(jnp.float32)
    small[4:6, :] = jnp.where(first, ng[:, 0:1], ng[:, 1:2])
    small[6:8, :] = jnp.zeros((2, cols), jnp.float32)


def prepare(cum, q, fk, fv, ng):
    block, cols = cum.shape[2], q.shape[1]
    return pl.pallas_call(
        prepare_kernel,
        out_shape=(
            jax.ShapeDtypeStruct((2, block, cols), jnp.float32),
            jax.ShapeDtypeStruct((2, cols, cols), jnp.bfloat16),
            jax.ShapeDtypeStruct((8, cols), jnp.float32),
        ),
        in_specs=[VMEM] * 5,
        out_specs=(VMEM,) * 3,
        compiler_params=pltpu.CompilerParams(vmem_limit_bytes=8 * 1024 * 1024),
        cost_estimate=pl.CostEstimate(
            flops=1024 * 1024, bytes_accessed=1024 * 1024, transcendentals=0
        ),
        name="prepare",
    )(cum, q, fk, fv, ng)


def halves(own, got, places):
    tp = lax.axis_index("tp")
    x, core = tp // 2, lax.rem(tp, 2)
    half = own.shape[1]
    found = []
    for side, ref in enumerate((own, got)):
        which = lax.rem(core + side, 2)
        for k, (off, p) in enumerate(places):
            place = lax.rem(x + jnp.where(which == 0, off, (4 - off) % 4), 4)
            found.append((ref, k, p, pl.multiple_of((place * 2 + which) * half, half)))
    return found


def stored(found, keys, values, sem):
    cols = keys.shape[2]
    copies = []
    for i, (ref, k, p, at) in enumerate(found):
        rows = pl.ds(at, ref.shape[1])
        for j, cache in enumerate((keys, values)):
            copies.append(
                pltpu.make_async_copy(
                    ref.at[k, :, pl.ds(j * cols, cols)], cache.at[p, rows, :], sem.at[i, j]
                )
            )
    for copy in copies:
        copy.start()
    return copies


def scored(found, p, gates, qm):
    cols = qm.shape[2]
    parts, seen = [], []
    for ref, k, prompt, at in found:
        if prompt == p:
            part = jnp.dot(ref[k, :, :cols], qm[p], preferred_element_type=jnp.float32)
            parts.append(part * (HD**-0.5) - gates[p, pl.ds(at, ref.shape[1]), :])
            seen.append(ref[k, :, cols:].astype(jnp.float32))
    return jnp.concatenate(parts, axis=0), jnp.concatenate(seen, axis=0)


def early_kernel(own, got, gates, qm, keys, values, state, sem):
    found = halves(own, got, EARLY)
    copies = stored(found, keys, values, sem)
    for p in range(2):
        scores, seen = scored(found, p, gates, qm)
        top = jnp.max(scores, axis=0, keepdims=True)
        weights = jnp.exp(scores - top)
        state[4 * p : 4 * p + 1, :] = top
        state[4 * p + 1 : 4 * p + 2, :] = jnp.sum(weights, axis=0, keepdims=True)
        state[4 * p + 2 : 4 * p + 3, :] = jnp.sum(weights * seen, axis=0, keepdims=True)
        state[4 * p + 3 : 4 * p + 4, :] = jnp.zeros_like(top)
    for copy in copies:
        copy.wait()


def early(own, got, gates, qm):
    block, cols = gates.shape[1:]
    cache = jax.ShapeDtypeStruct((2, block, cols), jnp.bfloat16)
    return pl.pallas_call(
        early_kernel,
        out_shape=(cache, cache, jax.ShapeDtypeStruct((8, cols), jnp.float32)),
        in_specs=[VMEM] * 4,
        out_specs=(ANY, ANY, VMEM),
        scratch_shapes=[pltpu.SemaphoreType.DMA((2 * len(EARLY), 2))],
        compiler_params=pltpu.CompilerParams(vmem_limit_bytes=8 * 1024 * 1024),
        cost_estimate=pl.CostEstimate(
            flops=64 * 1024 * 1024, bytes_accessed=2 * 1024 * 1024, transcendentals=0
        ),
        name="early",
    )(own, got, gates, qm)


def late_kernel(own, both, gates, qm, small, state, k_in, v_in, keys, values, part, sem):
    core = lax.rem(lax.axis_index("tp"), 2)
    found = halves(own, both.at[1 - core], LATE)
    copies = stored(found, keys, values, sem)
    members, _, cols = part.shape
    block = gates.shape[1]
    last = lax.axis_index("sp") == lax.axis_size("sp") - 1
    for p in range(2):
        scores, seen = scored(found, p, gates, qm)
        fresh = small[p : p + 1, :] - (
            gates[p, block - 1 : block, :] + small[4 + p : 5 + p, :]
        )
        fresh = jnp.where(last, fresh, MASKED)
        before = state[4 * p : 4 * p + 1, :]
        top = jnp.maximum(jnp.max(scores, axis=0, keepdims=True), fresh)
        top = jnp.maximum(top, before)
        weights = jnp.exp(scores - top)
        fresh_weight = jnp.exp(fresh - top)
        scale = jnp.exp(before - top)
        total = jnp.sum(weights, axis=0, keepdims=True) + fresh_weight
        total = total + scale * state[4 * p + 1 : 4 * p + 2, :]
        acc = jnp.sum(weights * seen, axis=0, keepdims=True)
        acc = acc + fresh_weight * small[2 + p : 3 + p, :]
        acc = acc + scale * state[4 * p + 2 : 4 * p + 3, :]
        for r, row in ((2 * p, top), (2 * p + 1, top), (2 * p + 4, total), (2 * p + 5, acc)):
            part[:, r : r + 1, :] = jnp.broadcast_to(row[None], (members, 1, cols))
    for copy in copies:
        copy.wait()


def late(own, both, gates, qm, small, state, keys, values, members):
    cols = gates.shape[2]
    cache = jax.ShapeDtypeStruct(keys.shape, keys.dtype)
    return pl.pallas_call(
        late_kernel,
        out_shape=(cache, cache, jax.ShapeDtypeStruct((members, 8, cols), jnp.float32)),
        in_specs=[VMEM] * 6 + [ANY, ANY],
        out_specs=(ANY, ANY, VMEM),
        input_output_aliases={6: 0, 7: 1},
        scratch_shapes=[pltpu.SemaphoreType.DMA((2 * len(LATE), 2))],
        compiler_params=pltpu.CompilerParams(vmem_limit_bytes=8 * 1024 * 1024),
        cost_estimate=pl.CostEstimate(
            flops=16 * 1024 * 1024, bytes_accessed=1024 * 1024, transcendentals=0
        ),
        name="late",
    )(own, both, gates, qm, small, state, keys, values)


def merge_kernel(parts, out):
    tops = parts[:, 0:4, :]
    scale = jnp.exp(tops - jnp.max(tops, axis=0, keepdims=True))
    sums = jnp.sum(scale * parts[:, 4:8, :], axis=0)
    for p in range(2):
        out[p : p + 1, :] = (
            sums[2 * p + 1 : 2 * p + 2] / sums[2 * p : 2 * p + 1]
        ).astype(jnp.bfloat16)


def merge(parts):
    cols = parts.shape[2]
    return pl.pallas_call(
        merge_kernel,
        out_shape=jax.ShapeDtypeStruct((2, cols), jnp.bfloat16),
        in_specs=[VMEM],
        out_specs=VMEM,
        compiler_params=pltpu.CompilerParams(vmem_limit_bytes=4 * 1024 * 1024),
        name="merge",
    )(parts)


def shift(x, by):
    return lax.ppermute(x, "tp", by)


def body(
    tokens, norm_gain, key_weight, value_weight, cum_gates, new_query, new_key, new_value, new_gate
):
    members = lax.axis_size("sp")
    tps = lax.axis_size("tp")
    ahead = [(i, (i + 2 - 4 * (i % 2)) % tps) for i in range(tps)]
    back = [(i, (i - 2 + 4 * (i % 2)) % tps) for i in range(tps)]
    swap = [(i, i ^ 1) for i in range(tps)]
    gain = norm_gain.reshape(1, -1)
    half, width = tokens.shape[1:]
    from_3 = shift(tokens, ahead)
    from_1 = shift(tokens, back)
    a_2 = shift(from_3[0], ahead)
    b_2 = shift(from_1[1], back)
    wo = jnp.concatenate([key_weight, value_weight], axis=1)
    wp = shift(wo, swap)

    made = prepare(
        jnp.swapaxes(cum_gates, 1, 2), new_query, new_key, new_value, new_gate
    )
    gain, wp, made = lax.optimization_barrier((gain, wp, made))
    gates, qm, small = made

    rows = (2 * half, width)
    done = project((tokens.reshape(rows),), gain, wo, wp, half)
    own1, par1 = project((from_3.reshape(rows), from_1.reshape(rows)), gain, wo, wp, half, done)
    got1 = shift(par1, swap)
    done = project((a_2,), gain, wo, wp, half)
    keys, values, state = early(own1, got1, gates, qm)
    own2, par2 = project((b_2,), gain, wo, wp, half, done)
    pairs = [[i, i + 1] for i in range(0, tps, 2)]
    both2 = lax.all_gather(par2, "tp", axis_index_groups=pairs)
    keys, values, part = late(
        own2, both2, gates, qm, small, state, keys, values, members
    )
    parts = lax.all_to_all(part, "sp", split_axis=0, concat_axis=0, tiled=True)
    return keys, values, merge(parts)


def solution(mesh):
    in_specs = (
        P("gr", ("sp", "tp"), None),
        P(),
        P(None, "tp"),
        P(None, "tp"),
        P("gr", "sp", "tp"),
        P("gr", "tp"),
        P("gr", "tp"),
        P("gr", "tp"),
        P("gr", "tp"),
    )
    out_specs = (P("gr", "sp", "tp"), P("gr", "sp", "tp"), P("gr", "tp"))
    return jax.shard_map(body, mesh=mesh, in_specs=in_specs, out_specs=out_specs, check_vma=False)
```

```python
import functools

import jax
import jax.numpy as jnp
from jax import lax
from jax.experimental import pallas as pl
from jax.experimental.pallas import tpu as pltpu
from jax.sharding import PartitionSpec as P


HD = 64
EPS = 1e-06
MASKED = -1e30


VMEM = pl.BlockSpec(memory_space=pltpu.VMEM)
ANY = pl.BlockSpec(memory_space=pl.ANY)

EARLY = ((0, 0), (0, 1), (3, 0), (3, 1), (1, 1), (1, 0))
LATE = ((2, 0), (2, 1))


def project_kernel(count, prior, *refs):
    xs, refs = refs[:count], refs[count:]
    before, (gain, wo, wp, own, par, n_s) = refs[: 2 * prior], refs[2 * prior :]
    width = xs[0].shape[1]
    half = own.shape[1]
    step = 16

    def normalize(x, base):
        def rows_of(i, carry):
            rows = pl.ds(pl.multiple_of(i * step, step), step)
            total = jnp.zeros((step, 128), jnp.float32)
            for c in range(width // 1024):
                part = x[rows, pl.ds(c * 1024, 1024)].astype(jnp.float32)
                part = part * part
                for j in range(8):
                    total = total + part[:, j * 128 : (j + 1) * 128]
            mean = jnp.sum(total, axis=-1, keepdims=True) * (1.0 / width)
            scale = lax.rsqrt(mean + EPS)
            out = pl.ds(pl.multiple_of(base + i * step, step), step)
            for c in range(width // 1024):
                at = pl.ds(c * 1024, 1024)
                part = x[rows, at].astype(jnp.float32)
                part = part * scale * gain[:, at].astype(jnp.float32)
                n_s[out, at] = part.astype(jnp.bfloat16)
            return carry

        lax.fori_loop(0, x.shape[0] // step, rows_of, 0, unroll=2)

    base = 0
    for x in xs:
        normalize(x, base)
        base += x.shape[0]
    for k, (w, out) in enumerate(((wo, own), (wp, par))):
        acc = jnp.dot(n_s[...], w[...], preferred_element_type=jnp.float32)
        done = before[k].shape[0] if prior else 0
        if prior:
            out[:done] = before[k][...]
        out[done:] = acc.astype(jnp.bfloat16).reshape(-1, half, out.shape[2])


def project(xs, gain, wo, wp, half, before=()):
    rows = sum(x.shape[0] for x in xs)
    width, cols = wo.shape
    done = before[0].shape[0] if before else 0
    out = jax.ShapeDtypeStruct((done + rows // half, half, cols), jnp.bfloat16)
    return pl.pallas_call(
        functools.partial(project_kernel, len(xs), bool(before)),
        out_shape=(out, out),
        in_specs=[VMEM] * (len(xs) + len(before) + 3),
        out_specs=(VMEM, VMEM),
        scratch_shapes=[pltpu.VMEM((rows, width), jnp.bfloat16)],
        compiler_params=pltpu.CompilerParams(vmem_limit_bytes=16 * 1024 * 1024),
        cost_estimate=pl.CostEstimate(
            flops=2 * rows * width * 2 * cols,
            bytes_accessed=6 * 1024 * 1024,
            transcendentals=0,
        ),
        name="project",
    )(*xs, *before, gain, wo, wp)


def prepare_kernel(cum, q, fk, fv, ng, gates, qm, small):
    block, cols = gates.shape[1:]
    shape = (cols, cols)
    same = lax.broadcasted_iota(jnp.int32, shape, 0) // HD == (
        lax.broadcasted_iota(jnp.int32, shape, 1) // HD
    )
    first = lax.broadcasted_iota(jnp.int32, (2, cols), 1) < HD
    for p in range(2):
        spread = [jnp.broadcast_to(cum[p, h : h + 1, :], (HD, block)) for h in range(2)]
        gates[p] = jnp.concatenate(spread, axis=0).T
        down = jnp.broadcast_to(q[p : p + 1, :].astype(jnp.float32), shape).T
        qm[p] = jnp.where(same, down, 0.0).astype(jnp.bfloat16)
        fresh = jnp.dot(fk[...], qm[p], preferred_element_type=jnp.float32)
        small[p : p + 1, :] = fresh[p : p + 1] * (HD**-0.5)
    small[2:4, :] = fv[...].astype(jnp.float32)
    small[4:6, :] = jnp.where(first, ng[:, 0:1], ng[:, 1:2])
    small[6:8, :] = jnp.zeros((2, cols), jnp.float32)


def prepare(cum, q, fk, fv, ng):
    block, cols = cum.shape[2], q.shape[1]
    return pl.pallas_call(
        prepare_kernel,
        out_shape=(
            jax.ShapeDtypeStruct((2, block, cols), jnp.float32),
            jax.ShapeDtypeStruct((2, cols, cols), jnp.bfloat16),
            jax.ShapeDtypeStruct((8, cols), jnp.float32),
        ),
        in_specs=[VMEM] * 5,
        out_specs=(VMEM,) * 3,
        compiler_params=pltpu.CompilerParams(vmem_limit_bytes=8 * 1024 * 1024),
        cost_estimate=pl.CostEstimate(
            flops=1024 * 1024, bytes_accessed=1024 * 1024, transcendentals=0
        ),
        name="prepare",
    )(cum, q, fk, fv, ng)


def halves(own, got, places):
    tp = lax.axis_index("tp")
    x, core = tp // 2, lax.rem(tp, 2)
    half = own.shape[1]
    found = []
    for side, ref in enumerate((own, got)):
        which = lax.rem(core + side, 2)
        for k, (off, p) in enumerate(places):
            place = lax.rem(x + jnp.where(which == 0, off, (4 - off) % 4), 4)
            found.append((ref, k, p, pl.multiple_of((place * 2 + which) * half, half)))
    return found


def stored(found, keys, values, sem):
    cols = keys.shape[2]
    copies = []
    for i, (ref, k, p, at) in enumerate(found):
        rows = pl.ds(at, ref.shape[1])
        for j, cache in enumerate((keys, values)):
            copies.append(
                pltpu.make_async_copy(
                    ref.at[k, :, pl.ds(j * cols, cols)], cache.at[p, rows, :], sem.at[i, j]
                )
            )
    for copy in copies:
        copy.start()
    return copies


def scored(found, p, gates, qm):
    cols = qm.shape[2]
    parts, seen = [], []
    for ref, k, prompt, at in found:
        if prompt == p:
            part = jnp.dot(ref[k, :, :cols], qm[p], preferred_element_type=jnp.float32)
            parts.append(part * (HD**-0.5) - gates[p, pl.ds(at, ref.shape[1]), :])
            seen.append(ref[k, :, cols:].astype(jnp.float32))
    return jnp.concatenate(parts, axis=0), jnp.concatenate(seen, axis=0)


def early_kernel(own, got, gates, qm, keys, values, state, sem):
    found = halves(own, got, EARLY)
    copies = stored(found, keys, values, sem)
    for p in range(2):
        scores, seen = scored(found, p, gates, qm)
        top = jnp.max(scores, axis=0, keepdims=True)
        weights = jnp.exp(scores - top)
        state[4 * p : 4 * p + 1, :] = top
        state[4 * p + 1 : 4 * p + 2, :] = jnp.sum(weights, axis=0, keepdims=True)
        state[4 * p + 2 : 4 * p + 3, :] = jnp.sum(weights * seen, axis=0, keepdims=True)
        state[4 * p + 3 : 4 * p + 4, :] = jnp.zeros_like(top)
    for copy in copies:
        copy.wait()


def early(own, got, gates, qm):
    block, cols = gates.shape[1:]
    cache = jax.ShapeDtypeStruct((2, block, cols), jnp.bfloat16)
    return pl.pallas_call(
        early_kernel,
        out_shape=(cache, cache, jax.ShapeDtypeStruct((8, cols), jnp.float32)),
        in_specs=[VMEM] * 4,
        out_specs=(ANY, ANY, VMEM),
        scratch_shapes=[pltpu.SemaphoreType.DMA((2 * len(EARLY), 2))],
        compiler_params=pltpu.CompilerParams(vmem_limit_bytes=8 * 1024 * 1024),
        cost_estimate=pl.CostEstimate(
            flops=64 * 1024 * 1024, bytes_accessed=2 * 1024 * 1024, transcendentals=0
        ),
        name="early",
    )(own, got, gates, qm)


def late_kernel(own, both, gates, qm, small, state, part):
    core = lax.rem(lax.axis_index("tp"), 2)
    found = halves(own, both.at[1 - core], LATE)
    members, _, cols = part.shape
    block = gates.shape[1]
    last = lax.axis_index("sp") == lax.axis_size("sp") - 1
    for p in range(2):
        scores, seen = scored(found, p, gates, qm)
        fresh = small[p : p + 1, :] - (
            gates[p, block - 1 : block, :] + small[4 + p : 5 + p, :]
        )
        fresh = jnp.where(last, fresh, MASKED)
        before = state[4 * p : 4 * p + 1, :]
        top = jnp.maximum(jnp.max(scores, axis=0, keepdims=True), fresh)
        top = jnp.maximum(top, before)
        weights = jnp.exp(scores - top)
        fresh_weight = jnp.exp(fresh - top)
        scale = jnp.exp(before - top)
        total = jnp.sum(weights, axis=0, keepdims=True) + fresh_weight
        total = total + scale * state[4 * p + 1 : 4 * p + 2, :]
        acc = jnp.sum(weights * seen, axis=0, keepdims=True)
        acc = acc + fresh_weight * small[2 + p : 3 + p, :]
        acc = acc + scale * state[4 * p + 2 : 4 * p + 3, :]
        for r, row in ((2 * p, top), (2 * p + 1, top), (2 * p + 4, total), (2 * p + 5, acc)):
            part[:, r : r + 1, :] = jnp.broadcast_to(row[None], (members, 1, cols))


def late(own, both, gates, qm, small, state, members):
    cols = gates.shape[2]
    return pl.pallas_call(
        late_kernel,
        out_shape=jax.ShapeDtypeStruct((members, 8, cols), jnp.float32),
        in_specs=[VMEM] * 6,
        out_specs=VMEM,
        compiler_params=pltpu.CompilerParams(vmem_limit_bytes=4 * 1024 * 1024),
        cost_estimate=pl.CostEstimate(
            flops=16 * 1024 * 1024, bytes_accessed=1024 * 1024, transcendentals=0
        ),
        name="late",
    )(own, both, gates, qm, small, state)


def merge_kernel(parts, own, both, k_in, v_in, keys, values, out, sem):
    core = lax.rem(lax.axis_index("tp"), 2)
    copies = stored(halves(own, both.at[1 - core], LATE), keys, values, sem)
    tops = parts[:, 0:4, :]
    scale = jnp.exp(tops - jnp.max(tops, axis=0, keepdims=True))
    sums = jnp.sum(scale * parts[:, 4:8, :], axis=0)
    for p in range(2):
        out[p : p + 1, :] = (
            sums[2 * p + 1 : 2 * p + 2] / sums[2 * p : 2 * p + 1]
        ).astype(jnp.bfloat16)
    for copy in copies:
        copy.wait()


def merge(parts, own, both, keys, values):
    cache = jax.ShapeDtypeStruct(keys.shape, keys.dtype)
    return pl.pallas_call(
        merge_kernel,
        out_shape=(cache, cache, jax.ShapeDtypeStruct((2, parts.shape[2]), jnp.bfloat16)),
        in_specs=[VMEM] * 3 + [ANY] * 2,
        out_specs=(ANY, ANY, VMEM),
        input_output_aliases={3: 0, 4: 1},
        scratch_shapes=[pltpu.SemaphoreType.DMA((2 * len(LATE), 2))],
        compiler_params=pltpu.CompilerParams(vmem_limit_bytes=4 * 1024 * 1024),
        name="merge",
    )(parts, own, both, keys, values)


def split_kernel(tokens, a, b):
    a[...] = tokens[0]
    b[...] = tokens[1]


def split(tokens):
    piece = jax.ShapeDtypeStruct(tokens.shape[1:], tokens.dtype)
    return pl.pallas_call(
        split_kernel,
        out_shape=(piece, piece),
        in_specs=[VMEM],
        out_specs=(VMEM, VMEM),
        compiler_params=pltpu.CompilerParams(vmem_limit_bytes=4 * 1024 * 1024),
        cost_estimate=pl.CostEstimate(
            flops=1024 * 1024, bytes_accessed=2 * 1024 * 1024, transcendentals=0
        ),
        name="split",
    )(tokens)


def shift(x, by):
    return lax.ppermute(x, "tp", by)


def body(
    tokens, norm_gain, key_weight, value_weight, cum_gates, new_query, new_key, new_value, new_gate
):
    members = lax.axis_size("sp")
    tps = lax.axis_size("tp")
    ahead = [(i, (i + 2 - 4 * (i % 2)) % tps) for i in range(tps)]
    back = [(i, (i - 2 + 4 * (i % 2)) % tps) for i in range(tps)]
    swap = [(i, i ^ 1) for i in range(tps)]
    gain = norm_gain.reshape(1, -1)
    half, width = tokens.shape[1:]
    from_3 = shift(tokens, ahead)
    a_0, b_0 = split(tokens)
    b_1 = shift(b_0, back)
    a_1 = shift(a_0, back)
    b_2 = shift(b_1, back)
    a_2 = shift(from_3[0], ahead)
    wo = jnp.concatenate([key_weight, value_weight], axis=1)
    wp = shift(wo, swap)

    made = prepare(
        jnp.swapaxes(cum_gates, 1, 2), new_query, new_key, new_value, new_gate
    )
    gain, wp, made = lax.optimization_barrier((gain, wp, made))
    gates, qm, small = made

    rows = (2 * half, width)
    done = project((tokens.reshape(rows),), gain, wo, wp, half)
    own1, par1 = project((from_3.reshape(rows), b_1, a_1), gain, wo, wp, half, done)
    got1 = shift(par1, swap)
    done = project((a_2,), gain, wo, wp, half)
    keys, values, state = early(own1, got1, gates, qm)
    own2, par2 = project((b_2,), gain, wo, wp, half, done)
    pairs = [[i, i + 1] for i in range(0, tps, 2)]
    both2 = lax.all_gather(par2, "tp", axis_index_groups=pairs)
    part = late(own2, both2, gates, qm, small, state, members)
    parts = lax.all_to_all(part, "sp", split_axis=0, concat_axis=0, tiled=True)
    return merge(parts, own2, both2, keys, values)


def solution(mesh):
    in_specs = (
        P("gr", ("sp", "tp"), None),
        P(),
        P(None, "tp"),
        P(None, "tp"),
        P("gr", "sp", "tp"),
        P("gr", "tp"),
        P("gr", "tp"),
        P("gr", "tp"),
        P("gr", "tp"),
    )
    out_specs = (P("gr", "sp", "tp"), P("gr", "sp", "tp"), P("gr", "tp"))
    return jax.shard_map(body, mesh=mesh, in_specs=in_specs, out_specs=out_specs, check_vma=False)
```

```python
import functools

import jax
import jax.numpy as jnp
from jax import lax
from jax.experimental import pallas as pl
from jax.experimental.pallas import tpu as pltpu
from jax.sharding import PartitionSpec as P


HD = 64
EPS = 1e-06
MASKED = -1e30


VMEM = pl.BlockSpec(memory_space=pltpu.VMEM)
ANY = pl.BlockSpec(memory_space=pl.ANY)

EARLY = ((0, 0), (0, 1), (3, 0), (3, 1), (1, 1), (1, 0))
LATE = ((2, 0), (2, 1))


def project_kernel(count, prior, *refs):
    xs, refs = refs[:count], refs[count:]
    before, (gain, wo, wp, own, par, n_s) = refs[: 2 * prior], refs[2 * prior :]
    width = xs[0].shape[1]
    half = own.shape[1]
    step = 16

    def normalize(x, base):
        def rows_of(i, carry):
            rows = pl.ds(pl.multiple_of(i * step, step), step)
            total = jnp.zeros((step, 128), jnp.float32)
            for c in range(width // 1024):
                part = x[rows, pl.ds(c * 1024, 1024)].astype(jnp.float32)
                part = part * part
                for j in range(8):
                    total = total + part[:, j * 128 : (j + 1) * 128]
            mean = jnp.sum(total, axis=-1, keepdims=True) * (1.0 / width)
            scale = lax.rsqrt(mean + EPS)
            out = pl.ds(pl.multiple_of(base + i * step, step), step)
            for c in range(width // 1024):
                at = pl.ds(c * 1024, 1024)
                part = x[rows, at].astype(jnp.float32)
                part = part * scale * gain[:, at].astype(jnp.float32)
                n_s[out, at] = part.astype(jnp.bfloat16)
            return carry

        lax.fori_loop(0, x.shape[0] // step, rows_of, 0, unroll=2)

    base = 0
    for x in xs:
        normalize(x, base)
        base += x.shape[0]
    for k, (w, out) in enumerate(((wo, own), (wp, par))):
        acc = jnp.dot(n_s[...], w[...], preferred_element_type=jnp.float32)
        done = before[k].shape[0] if prior else 0
        if prior:
            out[:done] = before[k][...]
        out[done:] = acc.astype(jnp.bfloat16).reshape(-1, half, out.shape[2])


def project(xs, gain, wo, wp, half, before=()):
    rows = sum(x.shape[0] for x in xs)
    width, cols = wo.shape
    done = before[0].shape[0] if before else 0
    out = jax.ShapeDtypeStruct((done + rows // half, half, cols), jnp.bfloat16)
    return pl.pallas_call(
        functools.partial(project_kernel, len(xs), bool(before)),
        out_shape=(out, out),
        in_specs=[VMEM] * (len(xs) + len(before) + 3),
        out_specs=(VMEM, VMEM),
        scratch_shapes=[pltpu.VMEM((rows, width), jnp.bfloat16)],
        compiler_params=pltpu.CompilerParams(vmem_limit_bytes=16 * 1024 * 1024),
        cost_estimate=pl.CostEstimate(
            flops=2 * rows * width * 2 * cols,
            bytes_accessed=6 * 1024 * 1024,
            transcendentals=0,
        ),
        name="project",
    )(*xs, *before, gain, wo, wp)


def prepare_kernel(cum, q, fk, fv, ng, gates, qm, small):
    block, cols = gates.shape[1:]
    shape = (cols, cols)
    same = lax.broadcasted_iota(jnp.int32, shape, 0) // HD == (
        lax.broadcasted_iota(jnp.int32, shape, 1) // HD
    )
    first = lax.broadcasted_iota(jnp.int32, (2, cols), 1) < HD
    for p in range(2):
        spread = [jnp.broadcast_to(cum[p, h : h + 1, :], (HD, block)) for h in range(2)]
        gates[p] = jnp.concatenate(spread, axis=0).T
        down = jnp.broadcast_to(q[p : p + 1, :].astype(jnp.float32), shape).T
        qm[p] = jnp.where(same, down, 0.0).astype(jnp.bfloat16)
        fresh = jnp.dot(fk[...], qm[p], preferred_element_type=jnp.float32)
        small[p : p + 1, :] = fresh[p : p + 1] * (HD**-0.5)
    small[2:4, :] = fv[...].astype(jnp.float32)
    small[4:6, :] = jnp.where(first, ng[:, 0:1], ng[:, 1:2])
    small[6:8, :] = jnp.zeros((2, cols), jnp.float32)


def prepare(cum, q, fk, fv, ng):
    block, cols = cum.shape[2], q.shape[1]
    return pl.pallas_call(
        prepare_kernel,
        out_shape=(
            jax.ShapeDtypeStruct((2, block, cols), jnp.float32),
            jax.ShapeDtypeStruct((2, cols, cols), jnp.bfloat16),
            jax.ShapeDtypeStruct((8, cols), jnp.float32),
        ),
        in_specs=[VMEM] * 5,
        out_specs=(VMEM,) * 3,
        compiler_params=pltpu.CompilerParams(vmem_limit_bytes=8 * 1024 * 1024),
        cost_estimate=pl.CostEstimate(
            flops=1024 * 1024, bytes_accessed=1024 * 1024, transcendentals=0
        ),
        name="prepare",
    )(cum, q, fk, fv, ng)


def halves(own, got, places):
    tp = lax.axis_index("tp")
    x, core = tp // 2, lax.rem(tp, 2)
    half = own.shape[1]
    found = []
    for side, ref in enumerate((own, got)):
        which = lax.rem(core + side, 2)
        for k, (off, p) in enumerate(places):
            place = lax.rem(x + jnp.where(which == 0, off, (4 - off) % 4), 4)
            found.append((ref, k, p, pl.multiple_of((place * 2 + which) * half, half)))
    return found


def stored(found, keys, values, sem):
    cols = keys.shape[2]
    copies = []
    for i, (ref, k, p, at) in enumerate(found):
        rows = pl.ds(at, ref.shape[1])
        for j, cache in enumerate((keys, values)):
            copies.append(
                pltpu.make_async_copy(
                    ref.at[k, :, pl.ds(j * cols, cols)], cache.at[p, rows, :], sem.at[i, j]
                )
            )
    for copy in copies:
        copy.start()
    return copies


def scored(found, p, gates, qm):
    cols = qm.shape[2]
    parts, seen = [], []
    for ref, k, prompt, at in found:
        if prompt == p:
            part = jnp.dot(ref[k, :, :cols], qm[p], preferred_element_type=jnp.float32)
            parts.append(part * (HD**-0.5) - gates[p, pl.ds(at, ref.shape[1]), :])
            seen.append(ref[k, :, cols:].astype(jnp.float32))
    return jnp.concatenate(parts, axis=0), jnp.concatenate(seen, axis=0)


def early_kernel(own, got, gates, qm, keys, values, state, sem):
    found = halves(own, got, EARLY)
    copies = stored(found, keys, values, sem)
    for p in range(2):
        scores, seen = scored(found, p, gates, qm)
        top = jnp.max(scores, axis=0, keepdims=True)
        weights = jnp.exp(scores - top)
        state[4 * p : 4 * p + 1, :] = top
        state[4 * p + 1 : 4 * p + 2, :] = jnp.sum(weights, axis=0, keepdims=True)
        state[4 * p + 2 : 4 * p + 3, :] = jnp.sum(weights * seen, axis=0, keepdims=True)
        state[4 * p + 3 : 4 * p + 4, :] = jnp.zeros_like(top)
    for copy in copies:
        copy.wait()


def early(own, got, gates, qm):
    block, cols = gates.shape[1:]
    cache = jax.ShapeDtypeStruct((2, block, cols), jnp.bfloat16)
    return pl.pallas_call(
        early_kernel,
        out_shape=(cache, cache, jax.ShapeDtypeStruct((8, cols), jnp.float32)),
        in_specs=[VMEM] * 4,
        out_specs=(ANY, ANY, VMEM),
        scratch_shapes=[pltpu.SemaphoreType.DMA((2 * len(EARLY), 2))],
        compiler_params=pltpu.CompilerParams(vmem_limit_bytes=8 * 1024 * 1024),
        cost_estimate=pl.CostEstimate(
            flops=64 * 1024 * 1024, bytes_accessed=2 * 1024 * 1024, transcendentals=0
        ),
        name="early",
    )(own, got, gates, qm)


def late_kernel(own, both, gates, qm, small, state, part):
    core = lax.rem(lax.axis_index("tp"), 2)
    found = halves(own, both.at[1 - core], LATE)
    members, _, cols = part.shape
    block = gates.shape[1]
    low = lax.broadcasted_iota(jnp.int32, (1, cols), 1) % HD < HD // 2
    last = lax.axis_index("sp") == lax.axis_size("sp") - 1
    for p in range(2):
        scores, seen = scored(found, p, gates, qm)
        fresh = small[p : p + 1, :] - (
            gates[p, block - 1 : block, :] + small[4 + p : 5 + p, :]
        )
        fresh = jnp.where(last, fresh, MASKED)
        before = state[4 * p : 4 * p + 1, :]
        top = jnp.maximum(jnp.max(scores, axis=0, keepdims=True), fresh)
        top = jnp.maximum(top, before)
        weights = jnp.exp(scores - top)
        fresh_weight = jnp.exp(fresh - top)
        scale = jnp.exp(before - top)
        total = jnp.sum(weights, axis=0, keepdims=True) + fresh_weight
        total = total + scale * state[4 * p + 1 : 4 * p + 2, :]
        acc = jnp.sum(weights * seen, axis=0, keepdims=True)
        acc = acc + fresh_weight * small[2 + p : 3 + p, :]
        acc = acc + scale * state[4 * p + 2 : 4 * p + 3, :]
        for r, row in ((p, jnp.where(low, top, total)), (p + 2, acc)):
            part[:, r : r + 1, :] = jnp.broadcast_to(row[None], (members, 1, cols))


def late(own, both, gates, qm, small, state, members):
    cols = gates.shape[2]
    return pl.pallas_call(
        late_kernel,
        out_shape=jax.ShapeDtypeStruct((members, 4, cols), jnp.float32),
        in_specs=[VMEM] * 6,
        out_specs=VMEM,
        compiler_params=pltpu.CompilerParams(vmem_limit_bytes=4 * 1024 * 1024),
        cost_estimate=pl.CostEstimate(
            flops=16 * 1024 * 1024, bytes_accessed=1024 * 1024, transcendentals=0
        ),
        name="late",
    )(own, both, gates, qm, small, state)


def merge_kernel(parts, own, both, k_in, v_in, keys, values, out, sem):
    core = lax.rem(lax.axis_index("tp"), 2)
    copies = stored(halves(own, both.at[1 - core], LATE), keys, values, sem)
    members, _, cols = parts.shape
    low = lax.broadcasted_iota(jnp.int32, (members, cols), 1) % HD < HD // 2
    for p in range(2):
        both_of = parts[:, p, :]
        tops = jnp.where(low, both_of, pltpu.roll(both_of, HD // 2, 1))
        totals = jnp.where(low, pltpu.roll(both_of, cols - HD // 2, 1), both_of)
        scale = jnp.exp(tops - jnp.max(tops, axis=0, keepdims=True))
        total = jnp.sum(scale * totals, axis=0, keepdims=True)
        acc = jnp.sum(scale * parts[:, p + 2, :], axis=0, keepdims=True)
        out[p : p + 1, :] = (acc / total).astype(jnp.bfloat16)
    for copy in copies:
        copy.wait()


def merge(parts, own, both, keys, values):
    cache = jax.ShapeDtypeStruct(keys.shape, keys.dtype)
    return pl.pallas_call(
        merge_kernel,
        out_shape=(cache, cache, jax.ShapeDtypeStruct((2, parts.shape[2]), jnp.bfloat16)),
        in_specs=[VMEM] * 3 + [ANY] * 2,
        out_specs=(ANY, ANY, VMEM),
        input_output_aliases={3: 0, 4: 1},
        scratch_shapes=[pltpu.SemaphoreType.DMA((2 * len(LATE), 2))],
        compiler_params=pltpu.CompilerParams(vmem_limit_bytes=4 * 1024 * 1024),
        name="merge",
    )(parts, own, both, keys, values)


def split_kernel(tokens, a, b):
    a[...] = tokens[0]
    b[...] = tokens[1]


def split(tokens):
    piece = jax.ShapeDtypeStruct(tokens.shape[1:], tokens.dtype)
    return pl.pallas_call(
        split_kernel,
        out_shape=(piece, piece),
        in_specs=[VMEM],
        out_specs=(VMEM, VMEM),
        compiler_params=pltpu.CompilerParams(vmem_limit_bytes=4 * 1024 * 1024),
        cost_estimate=pl.CostEstimate(
            flops=1024 * 1024, bytes_accessed=2 * 1024 * 1024, transcendentals=0
        ),
        name="split",
    )(tokens)


def shift(x, by):
    return lax.ppermute(x, "tp", by)


def body(
    tokens, norm_gain, key_weight, value_weight, cum_gates, new_query, new_key, new_value, new_gate
):
    members = lax.axis_size("sp")
    tps = lax.axis_size("tp")
    ahead = [(i, (i + 2 - 4 * (i % 2)) % tps) for i in range(tps)]
    back = [(i, (i - 2 + 4 * (i % 2)) % tps) for i in range(tps)]
    swap = [(i, i ^ 1) for i in range(tps)]
    gain = norm_gain.reshape(1, -1)
    half, width = tokens.shape[1:]
    from_3 = shift(tokens, ahead)
    a_0, b_0 = split(tokens)
    b_1 = shift(b_0, back)
    a_1 = shift(a_0, back)
    b_2 = shift(b_1, back)
    a_2 = shift(from_3[0], ahead)
    wo = jnp.concatenate([key_weight, value_weight], axis=1)
    wp = shift(wo, swap)

    made = prepare(
        jnp.swapaxes(cum_gates, 1, 2), new_query, new_key, new_value, new_gate
    )
    gain, wp, made = lax.optimization_barrier((gain, wp, made))
    gates, qm, small = made

    rows = (2 * half, width)
    done = project((tokens.reshape(rows),), gain, wo, wp, half)
    own1, par1 = project((from_3.reshape(rows), b_1, a_1), gain, wo, wp, half, done)
    got1 = shift(par1, swap)
    keys, values, state = early(own1, got1, gates, qm)
    own2, par2 = project((a_2, b_2), gain, wo, wp, half)
    pairs = [[i, i + 1] for i in range(0, tps, 2)]
    both2 = lax.all_gather(par2, "tp", axis_index_groups=pairs)
    part = late(own2, both2, gates, qm, small, state, members)
    parts = lax.all_to_all(part, "sp", split_axis=0, concat_axis=0, tiled=True)
    return merge(parts, own2, both2, keys, values)


def solution(mesh):
    in_specs = (
        P("gr", ("sp", "tp"), None),
        P(),
        P(None, "tp"),
        P(None, "tp"),
        P("gr", "sp", "tp"),
        P("gr", "tp"),
        P("gr", "tp"),
        P("gr", "tp"),
        P("gr", "tp"),
    )
    out_specs = (P("gr", "sp", "tp"), P("gr", "sp", "tp"), P("gr", "tp"))
    return jax.shard_map(body, mesh=mesh, in_specs=in_specs, out_specs=out_specs, check_vma=False)
```

```python
import functools

import jax
import jax.numpy as jnp
from jax import lax
from jax.experimental import pallas as pl
from jax.experimental.pallas import tpu as pltpu
from jax.sharding import PartitionSpec as P


HD = 64
EPS = 1e-06
MASKED = -1e30
CHUNKS = 4


VMEM = pl.BlockSpec(memory_space=pltpu.VMEM)
ANY = pl.BlockSpec(memory_space=pl.ANY)

EARLY = ((0, 0), (0, 1), (3, 0), (3, 1), (1, 1), (1, 0))
LATE = ((2, 0), (2, 1))


def project_kernel(count, prior, *refs):
    xs, refs = refs[:count], refs[count:]
    before, (gain, wo, wp, own, par, n_s) = refs[: 2 * prior], refs[2 * prior :]
    width = xs[0].shape[1]
    half = own.shape[1]
    step = 16

    def normalize(x, base):
        def rows_of(i, carry):
            rows = pl.ds(pl.multiple_of(i * step, step), step)
            total = jnp.zeros((step, 128), jnp.float32)
            for c in range(width // 1024):
                part = x[rows, pl.ds(c * 1024, 1024)].astype(jnp.float32)
                part = part * part
                for j in range(8):
                    total = total + part[:, j * 128 : (j + 1) * 128]
            mean = jnp.sum(total, axis=-1, keepdims=True) * (1.0 / width)
            scale = lax.rsqrt(mean + EPS)
            out = pl.ds(pl.multiple_of(base + i * step, step), step)
            for c in range(width // 1024):
                at = pl.ds(c * 1024, 1024)
                part = x[rows, at].astype(jnp.float32)
                part = part * scale * gain[:, at].astype(jnp.float32)
                n_s[out, at] = part.astype(jnp.bfloat16)
            return carry

        lax.fori_loop(0, x.shape[0] // step, rows_of, 0, unroll=2)

    base = 0
    for x in xs:
        normalize(x, base)
        base += x.shape[0]
    for k, (w, out) in enumerate(((wo, own), (wp, par))):
        acc = jnp.dot(n_s[...], w[...], preferred_element_type=jnp.float32)
        done = before[k].shape[0] if prior else 0
        if prior:
            out[:done] = before[k][...]
        out[done:] = acc.astype(jnp.bfloat16).reshape(-1, half, out.shape[2])


def finish_kernel(xa, xb, gain, wo, wp, own, par, n_s):
    half, width = xa.shape
    cols = wo.shape[1]
    piece = width // CHUNKS
    scales = []
    for x in (xa, xb):
        total = jnp.zeros((half, 128), jnp.float32)
        for j in range(width // 128):
            part = x[:, j * 128 : (j + 1) * 128].astype(jnp.float32)
            total = total + part * part
        mean = jnp.sum(total, axis=-1, keepdims=True) * (1.0 / width)
        scales.append(lax.rsqrt(mean + EPS))
    sums = [jnp.zeros((2 * half, cols), jnp.float32) for _ in range(2)]
    for c in range(CHUNKS):
        at = slice(c * piece, (c + 1) * piece)
        factor = gain[:, at].astype(jnp.float32)
        for k, x in enumerate((xa, xb)):
            part = x[:, at].astype(jnp.float32) * scales[k] * factor
            n_s[k * half : (k + 1) * half, at] = part.astype(jnp.bfloat16)
        for k, w in enumerate((wo, wp)):
            sums[k] = sums[k] + jnp.dot(
                n_s[:, at], w[at, :], preferred_element_type=jnp.float32
            )
    for out, acc in zip((own, par), sums):
        out[...] = acc.astype(jnp.bfloat16).reshape(out.shape)


def finish(xa, xb, gain, wo, wp):
    half, width = xa.shape
    cols = wo.shape[1]
    out = jax.ShapeDtypeStruct((2, half, cols), jnp.bfloat16)
    return pl.pallas_call(
        finish_kernel,
        out_shape=(out, out),
        in_specs=[VMEM] * 5,
        out_specs=(VMEM, VMEM),
        scratch_shapes=[pltpu.VMEM((2 * half, width), jnp.bfloat16)],
        compiler_params=pltpu.CompilerParams(vmem_limit_bytes=16 * 1024 * 1024),
        cost_estimate=pl.CostEstimate(
            flops=8 * half * width * cols, bytes_accessed=6 * 1024 * 1024, transcendentals=0
        ),
        name="finish",
    )(xa, xb, gain, wo, wp)


def project(xs, gain, wo, wp, half, before=()):
    rows = sum(x.shape[0] for x in xs)
    width, cols = wo.shape
    done = before[0].shape[0] if before else 0
    out = jax.ShapeDtypeStruct((done + rows // half, half, cols), jnp.bfloat16)
    return pl.pallas_call(
        functools.partial(project_kernel, len(xs), bool(before)),
        out_shape=(out, out),
        in_specs=[VMEM] * (len(xs) + len(before) + 3),
        out_specs=(VMEM, VMEM),
        scratch_shapes=[pltpu.VMEM((rows, width), jnp.bfloat16)],
        compiler_params=pltpu.CompilerParams(vmem_limit_bytes=16 * 1024 * 1024),
        cost_estimate=pl.CostEstimate(
            flops=2 * rows * width * 2 * cols,
            bytes_accessed=6 * 1024 * 1024,
            transcendentals=0,
        ),
        name="project",
    )(*xs, *before, gain, wo, wp)


def prepare_kernel(cum, q, fk, fv, ng, gates, qm, small):
    block, cols = gates.shape[1:]
    shape = (cols, cols)
    same = lax.broadcasted_iota(jnp.int32, shape, 0) // HD == (
        lax.broadcasted_iota(jnp.int32, shape, 1) // HD
    )
    first = lax.broadcasted_iota(jnp.int32, (2, cols), 1) < HD
    for p in range(2):
        spread = [jnp.broadcast_to(cum[p, h : h + 1, :], (HD, block)) for h in range(2)]
        gates[p] = jnp.concatenate(spread, axis=0).T
        down = jnp.broadcast_to(q[p : p + 1, :].astype(jnp.float32), shape).T
        qm[p] = jnp.where(same, down, 0.0).astype(jnp.bfloat16)
        fresh = jnp.dot(fk[...], qm[p], preferred_element_type=jnp.float32)
        small[p : p + 1, :] = fresh[p : p + 1] * (HD**-0.5)
    small[2:4, :] = fv[...].astype(jnp.float32)
    small[4:6, :] = jnp.where(first, ng[:, 0:1], ng[:, 1:2])
    small[6:8, :] = jnp.zeros((2, cols), jnp.float32)


def prepare(cum, q, fk, fv, ng):
    block, cols = cum.shape[2], q.shape[1]
    return pl.pallas_call(
        prepare_kernel,
        out_shape=(
            jax.ShapeDtypeStruct((2, block, cols), jnp.float32),
            jax.ShapeDtypeStruct((2, cols, cols), jnp.bfloat16),
            jax.ShapeDtypeStruct((8, cols), jnp.float32),
        ),
        in_specs=[VMEM] * 5,
        out_specs=(VMEM,) * 3,
        compiler_params=pltpu.CompilerParams(vmem_limit_bytes=8 * 1024 * 1024),
        cost_estimate=pl.CostEstimate(
            flops=1024 * 1024, bytes_accessed=1024 * 1024, transcendentals=0
        ),
        name="prepare",
    )(cum, q, fk, fv, ng)


def halves(own, got, places):
    tp = lax.axis_index("tp")
    x, core = tp // 2, lax.rem(tp, 2)
    half = own.shape[1]
    found = []
    for side, ref in enumerate((own, got)):
        which = lax.rem(core + side, 2)
        for k, (off, p) in enumerate(places):
            place = lax.rem(x + jnp.where(which == 0, off, (4 - off) % 4), 4)
            found.append((ref, k, p, pl.multiple_of((place * 2 + which) * half, half)))
    return found


def stored(found, keys, values, sem):
    cols = keys.shape[2]
    copies = []
    for i, (ref, k, p, at) in enumerate(found):
        rows = pl.ds(at, ref.shape[1])
        for j, cache in enumerate((keys, values)):
            copies.append(
                pltpu.make_async_copy(
                    ref.at[k, :, pl.ds(j * cols, cols)], cache.at[p, rows, :], sem.at[i, j]
                )
            )
    for copy in copies:
        copy.start()
    return copies


def scored(found, p, gates, qm):
    cols = qm.shape[2]
    parts, seen = [], []
    for ref, k, prompt, at in found:
        if prompt == p:
            part = jnp.dot(ref[k, :, :cols], qm[p], preferred_element_type=jnp.float32)
            parts.append(part * (HD**-0.5) - gates[p, pl.ds(at, ref.shape[1]), :])
            seen.append(ref[k, :, cols:].astype(jnp.float32))
    return jnp.concatenate(parts, axis=0), jnp.concatenate(seen, axis=0)


def early_kernel(own, got, gates, qm, keys, values, state, sem):
    found = halves(own, got, EARLY)
    copies = stored(found, keys, values, sem)
    for p in range(2):
        scores, seen = scored(found, p, gates, qm)
        top = jnp.max(scores, axis=0, keepdims=True)
        weights = jnp.exp(scores - top)
        state[4 * p : 4 * p + 1, :] = top
        state[4 * p + 1 : 4 * p + 2, :] = jnp.sum(weights, axis=0, keepdims=True)
        state[4 * p + 2 : 4 * p + 3, :] = jnp.sum(weights * seen, axis=0, keepdims=True)
        state[4 * p + 3 : 4 * p + 4, :] = jnp.zeros_like(top)
    for copy in copies:
        copy.wait()


def early(own, got, gates, qm):
    block, cols = gates.shape[1:]
    cache = jax.ShapeDtypeStruct((2, block, cols), jnp.bfloat16)
    return pl.pallas_call(
        early_kernel,
        out_shape=(cache, cache, jax.ShapeDtypeStruct((8, cols), jnp.float32)),
        in_specs=[VMEM] * 4,
        out_specs=(ANY, ANY, VMEM),
        scratch_shapes=[pltpu.SemaphoreType.DMA((2 * len(EARLY), 2))],
        compiler_params=pltpu.CompilerParams(vmem_limit_bytes=8 * 1024 * 1024),
        cost_estimate=pl.CostEstimate(
            flops=64 * 1024 * 1024, bytes_accessed=2 * 1024 * 1024, transcendentals=0
        ),
        name="early",
    )(own, got, gates, qm)


def late_kernel(own, both, gates, qm, small, state, part):
    core = lax.rem(lax.axis_index("tp"), 2)
    found = halves(own, both.at[1 - core], LATE)
    members, cols = part.shape[0], gates.shape[2]
    block = gates.shape[1]
    packed = jnp.zeros((1, cols), jnp.float32)
    quarter = lax.broadcasted_iota(jnp.int32, (1, cols), 1) % HD // (HD // 4)
    last = lax.axis_index("sp") == lax.axis_size("sp") - 1
    for p in range(2):
        scores, seen = scored(found, p, gates, qm)
        fresh = small[p : p + 1, :] - (
            gates[p, block - 1 : block, :] + small[4 + p : 5 + p, :]
        )
        fresh = jnp.where(last, fresh, MASKED)
        before = state[4 * p : 4 * p + 1, :]
        top = jnp.maximum(jnp.max(scores, axis=0, keepdims=True), fresh)
        top = jnp.maximum(top, before)
        weights = jnp.exp(scores - top)
        fresh_weight = jnp.exp(fresh - top)
        scale = jnp.exp(before - top)
        total = jnp.sum(weights, axis=0, keepdims=True) + fresh_weight
        total = total + scale * state[4 * p + 1 : 4 * p + 2, :]
        acc = jnp.sum(weights * seen, axis=0, keepdims=True)
        acc = acc + fresh_weight * small[2 + p : 3 + p, :]
        acc = acc + scale * state[4 * p + 2 : 4 * p + 3, :]
        packed = jnp.where(quarter == 2 * p, top, packed)
        packed = jnp.where(quarter == 2 * p + 1, total, packed)
        part[:, :, p * cols : (p + 1) * cols] = jnp.broadcast_to(
            acc[None], (members, 1, cols)
        )
    part[:, :, 2 * cols :] = jnp.broadcast_to(packed[None], (members, 1, cols))


def late(own, both, gates, qm, small, state, members):
    cols = gates.shape[2]
    return pl.pallas_call(
        late_kernel,
        out_shape=jax.ShapeDtypeStruct((members, 1, 3 * cols), jnp.float32),
        in_specs=[VMEM] * 6,
        out_specs=VMEM,
        compiler_params=pltpu.CompilerParams(vmem_limit_bytes=4 * 1024 * 1024),
        cost_estimate=pl.CostEstimate(
            flops=16 * 1024 * 1024, bytes_accessed=1024 * 1024, transcendentals=0
        ),
        name="late",
    )(own, both, gates, qm, small, state)


def merge_kernel(parts, own, both, k_in, v_in, keys, values, out, sem):
    core = lax.rem(lax.axis_index("tp"), 2)
    copies = stored(halves(own, both.at[1 - core], LATE), keys, values, sem)
    members, cols = parts.shape[0], out.shape[1]
    packed = parts[:, 0, 2 * cols :]
    quarter = lax.broadcasted_iota(jnp.int32, (members, cols), 1) % HD // (HD // 4)

    def spread(which):
        only = jnp.where(quarter == which, packed, 0.0)
        found = only
        for to in range(4):
            if to != which:
                found = found + pltpu.roll(only, (to - which) * (HD // 4) % cols, 1)
        return found

    for p in range(2):
        tops = spread(2 * p)
        scale = jnp.exp(tops - jnp.max(tops, axis=0, keepdims=True))
        total = jnp.sum(scale * spread(2 * p + 1), axis=0, keepdims=True)
        acc = parts[:, 0, p * cols : (p + 1) * cols]
        acc = jnp.sum(scale * acc, axis=0, keepdims=True)
        out[p : p + 1, :] = (acc / total).astype(jnp.bfloat16)
    for copy in copies:
        copy.wait()


def merge(parts, own, both, keys, values):
    cache = jax.ShapeDtypeStruct(keys.shape, keys.dtype)
    return pl.pallas_call(
        merge_kernel,
        out_shape=(cache, cache, jax.ShapeDtypeStruct((2, keys.shape[2]), jnp.bfloat16)),
        in_specs=[VMEM] * 3 + [ANY] * 2,
        out_specs=(ANY, ANY, VMEM),
        input_output_aliases={3: 0, 4: 1},
        scratch_shapes=[pltpu.SemaphoreType.DMA((2 * len(LATE), 2))],
        compiler_params=pltpu.CompilerParams(vmem_limit_bytes=4 * 1024 * 1024),
        name="merge",
    )(parts, own, both, keys, values)


def split_kernel(tokens, a, b):
    a[...] = tokens[0]
    b[...] = tokens[1]


def split(tokens):
    piece = jax.ShapeDtypeStruct(tokens.shape[1:], tokens.dtype)
    return pl.pallas_call(
        split_kernel,
        out_shape=(piece, piece),
        in_specs=[VMEM],
        out_specs=(VMEM, VMEM),
        compiler_params=pltpu.CompilerParams(vmem_limit_bytes=4 * 1024 * 1024),
        cost_estimate=pl.CostEstimate(
            flops=1024 * 1024, bytes_accessed=2 * 1024 * 1024, transcendentals=0
        ),
        name="split",
    )(tokens)


def shift(x, by):
    return lax.ppermute(x, "tp", by)


def body(
    tokens, norm_gain, key_weight, value_weight, cum_gates, new_query, new_key, new_value, new_gate
):
    members = lax.axis_size("sp")
    tps = lax.axis_size("tp")
    ahead = [(i, (i + 2 - 4 * (i % 2)) % tps) for i in range(tps)]
    back = [(i, (i - 2 + 4 * (i % 2)) % tps) for i in range(tps)]
    swap = [(i, i ^ 1) for i in range(tps)]
    gain = norm_gain.reshape(1, -1)
    half, width = tokens.shape[1:]
    from_3 = shift(tokens, ahead)
    a_0, b_0 = split(tokens)
    b_1 = shift(b_0, back)
    a_1 = shift(a_0, back)
    b_2 = shift(b_1, back)
    a_2 = shift(from_3[0], ahead)
    wo = jnp.concatenate([key_weight, value_weight], axis=1)
    wp = shift(wo, swap)

    made = prepare(
        jnp.swapaxes(cum_gates, 1, 2), new_query, new_key, new_value, new_gate
    )
    gain, wp, made = lax.optimization_barrier((gain, wp, made))
    gates, qm, small = made

    rows = (2 * half, width)
    done = project((tokens.reshape(rows),), gain, wo, wp, half)
    own1, par1 = project((from_3.reshape(rows), b_1, a_1), gain, wo, wp, half, done)
    got1 = shift(par1, swap)
    keys, values, state = early(own1, got1, gates, qm)
    own2, par2 = finish(a_2, b_2, gain, wo, wp)
    pairs = [[i, i + 1] for i in range(0, tps, 2)]
    both2 = lax.all_gather(par2, "tp", axis_index_groups=pairs)
    part = late(own2, both2, gates, qm, small, state, members)
    parts = lax.all_to_all(part, "sp", split_axis=0, concat_axis=0, tiled=True)
    return merge(parts, own2, both2, keys, values)


def solution(mesh):
    in_specs = (
        P("gr", ("sp", "tp"), None),
        P(),
        P(None, "tp"),
        P(None, "tp"),
        P("gr", "sp", "tp"),
        P("gr", "tp"),
        P("gr", "tp"),
        P("gr", "tp"),
        P("gr", "tp"),
    )
    out_specs = (P("gr", "sp", "tp"), P("gr", "sp", "tp"), P("gr", "tp"))
    return jax.shard_map(body, mesh=mesh, in_specs=in_specs, out_specs=out_specs, check_vma=False)
```

```python
import functools

import jax
import jax.numpy as jnp
from jax import lax
from jax.experimental import pallas as pl
from jax.experimental.pallas import tpu as pltpu
from jax.sharding import PartitionSpec as P


HD = 64
EPS = 1e-06
MASKED = -1e30
CHUNKS = 4


VMEM = pl.BlockSpec(memory_space=pltpu.VMEM)
ANY = pl.BlockSpec(memory_space=pl.ANY)

EARLY = ((0, 0), (0, 1), (3, 0), (3, 1), (1, 1), (1, 0))
LATE = ((2, 0), (2, 1))


def project_kernel(count, prior, *refs):
    xs, refs = refs[:count], refs[count:]
    before, (gain, wo, wp, own, par, n_s) = refs[: 2 * prior], refs[2 * prior :]
    width = xs[0].shape[1]
    half = own.shape[1]
    step = 16

    def normalize(x, base):
        def rows_of(i, carry):
            rows = pl.ds(pl.multiple_of(i * step, step), step)
            total = jnp.zeros((step, 128), jnp.float32)
            for c in range(width // 1024):
                part = x[rows, pl.ds(c * 1024, 1024)].astype(jnp.float32)
                part = part * part
                for j in range(8):
                    total = total + part[:, j * 128 : (j + 1) * 128]
            mean = jnp.sum(total, axis=-1, keepdims=True) * (1.0 / width)
            scale = lax.rsqrt(mean + EPS)
            out = pl.ds(pl.multiple_of(base + i * step, step), step)
            for c in range(width // 1024):
                at = pl.ds(c * 1024, 1024)
                part = x[rows, at].astype(jnp.float32)
                part = part * scale * gain[:, at].astype(jnp.float32)
                n_s[out, at] = part.astype(jnp.bfloat16)
            return carry

        lax.fori_loop(0, x.shape[0] // step, rows_of, 0, unroll=2)

    base = 0
    for x in xs:
        normalize(x, base)
        base += x.shape[0]
    for k, (w, out) in enumerate(((wo, own), (wp, par))):
        acc = jnp.dot(n_s[...], w[...], preferred_element_type=jnp.float32)
        done = before[k].shape[0] if prior else 0
        if prior:
            out[:done] = before[k][...]
        out[done:] = acc.astype(jnp.bfloat16).reshape(-1, half, out.shape[2])


def finish_kernel(xa, xb, gain, wo, wp, own, par, n_s):
    half, width = xa.shape
    cols = wo.shape[1]
    piece = width // CHUNKS
    scales = []
    for x in (xa, xb):
        total = jnp.zeros((half, 128), jnp.float32)
        for j in range(width // 128):
            part = x[:, j * 128 : (j + 1) * 128].astype(jnp.float32)
            total = total + part * part
        mean = jnp.sum(total, axis=-1, keepdims=True) * (1.0 / width)
        scales.append(lax.rsqrt(mean + EPS))
    sums = [jnp.zeros((2 * half, cols), jnp.float32) for _ in range(2)]
    for c in range(CHUNKS):
        at = slice(c * piece, (c + 1) * piece)
        factor = gain[:, at].astype(jnp.float32)
        for k, x in enumerate((xa, xb)):
            part = x[:, at].astype(jnp.float32) * scales[k] * factor
            n_s[k * half : (k + 1) * half, at] = part.astype(jnp.bfloat16)
        for k, w in enumerate((wo, wp)):
            sums[k] = sums[k] + jnp.dot(
                n_s[:, at], w[at, :], preferred_element_type=jnp.float32
            )
    for out, acc in zip((own, par), sums):
        out[...] = acc.astype(jnp.bfloat16).reshape(out.shape)


def finish(xa, xb, gain, wo, wp):
    half, width = xa.shape
    cols = wo.shape[1]
    out = jax.ShapeDtypeStruct((2, half, cols), jnp.bfloat16)
    return pl.pallas_call(
        finish_kernel,
        out_shape=(out, out),
        in_specs=[VMEM] * 5,
        out_specs=(VMEM, VMEM),
        scratch_shapes=[pltpu.VMEM((2 * half, width), jnp.bfloat16)],
        compiler_params=pltpu.CompilerParams(vmem_limit_bytes=16 * 1024 * 1024),
        cost_estimate=pl.CostEstimate(
            flops=8 * half * width * cols, bytes_accessed=6 * 1024 * 1024, transcendentals=0
        ),
        name="finish",
    )(xa, xb, gain, wo, wp)


def project(xs, gain, wo, wp, half, before=()):
    rows = sum(x.shape[0] for x in xs)
    width, cols = wo.shape
    done = before[0].shape[0] if before else 0
    out = jax.ShapeDtypeStruct((done + rows // half, half, cols), jnp.bfloat16)
    return pl.pallas_call(
        functools.partial(project_kernel, len(xs), bool(before)),
        out_shape=(out, out),
        in_specs=[VMEM] * (len(xs) + len(before) + 3),
        out_specs=(VMEM, VMEM),
        scratch_shapes=[pltpu.VMEM((rows, width), jnp.bfloat16)],
        compiler_params=pltpu.CompilerParams(vmem_limit_bytes=16 * 1024 * 1024),
        cost_estimate=pl.CostEstimate(
            flops=2 * rows * width * 2 * cols,
            bytes_accessed=6 * 1024 * 1024,
            transcendentals=0,
        ),
        name="project",
    )(*xs, *before, gain, wo, wp)


def prepare_kernel(cum, q, fk, fv, ng, gates, qm, small):
    block, cols = gates.shape[1:]
    shape = (cols, cols)
    same = lax.broadcasted_iota(jnp.int32, shape, 0) // HD == (
        lax.broadcasted_iota(jnp.int32, shape, 1) // HD
    )
    first = lax.broadcasted_iota(jnp.int32, (2, cols), 1) < HD
    for p in range(2):
        spread = [jnp.broadcast_to(cum[p, h : h + 1, :], (HD, block)) for h in range(2)]
        gates[p] = jnp.concatenate(spread, axis=0).T
        down = jnp.broadcast_to(q[p : p + 1, :].astype(jnp.float32), shape).T
        qm[p] = jnp.where(same, down, 0.0).astype(jnp.bfloat16)
        fresh = jnp.dot(fk[...], qm[p], preferred_element_type=jnp.float32)
        small[p : p + 1, :] = fresh[p : p + 1] * (HD**-0.5)
    small[2:4, :] = fv[...].astype(jnp.float32)
    small[4:6, :] = jnp.where(first, ng[:, 0:1], ng[:, 1:2])
    small[6:8, :] = jnp.zeros((2, cols), jnp.float32)


def prepare(cum, q, fk, fv, ng):
    block, cols = cum.shape[2], q.shape[1]
    return pl.pallas_call(
        prepare_kernel,
        out_shape=(
            jax.ShapeDtypeStruct((2, block, cols), jnp.float32),
            jax.ShapeDtypeStruct((2, cols, cols), jnp.bfloat16),
            jax.ShapeDtypeStruct((8, cols), jnp.float32),
        ),
        in_specs=[VMEM] * 5,
        out_specs=(VMEM,) * 3,
        compiler_params=pltpu.CompilerParams(vmem_limit_bytes=8 * 1024 * 1024),
        cost_estimate=pl.CostEstimate(
            flops=1024 * 1024, bytes_accessed=1024 * 1024, transcendentals=0
        ),
        name="prepare",
    )(cum, q, fk, fv, ng)


def halves(own, got, places):
    tp = lax.axis_index("tp")
    x, core = tp // 2, lax.rem(tp, 2)
    half = own.shape[1]
    found = []
    for side, ref in enumerate((own, got)):
        which = lax.rem(core + side, 2)
        for k, (off, p) in enumerate(places):
            place = lax.rem(x + jnp.where(which == 0, off, (4 - off) % 4), 4)
            found.append((ref, k, p, pl.multiple_of((place * 2 + which) * half, half)))
    return found


def stored(found, keys, values, sem):
    cols = keys.shape[2]
    copies = []
    for i, (ref, k, p, at) in enumerate(found):
        rows = pl.ds(at, ref.shape[1])
        for j, cache in enumerate((keys, values)):
            copies.append(
                pltpu.make_async_copy(
                    ref.at[k, :, pl.ds(j * cols, cols)], cache.at[p, rows, :], sem.at[i, j]
                )
            )
    return copies


def scored(found, p, gates, qm):
    cols = qm.shape[2]
    parts, seen = [], []
    for ref, k, prompt, at in found:
        if prompt == p:
            part = jnp.dot(ref[k, :, :cols], qm[p], preferred_element_type=jnp.float32)
            parts.append(part * (HD**-0.5) - gates[p, pl.ds(at, ref.shape[1]), :])
            seen.append(ref[k, :, cols:].astype(jnp.float32))
    return jnp.concatenate(parts, axis=0), jnp.concatenate(seen, axis=0)


def early_kernel(own, got, gates, qm, keys, values, state, sem):
    found = halves(own, got, EARLY)
    copies = stored(found, keys, values, sem)
    for copy in copies:
        copy.start()
    for p in range(2):
        scores, seen = scored(found, p, gates, qm)
        top = jnp.max(scores, axis=0, keepdims=True)
        weights = jnp.exp(scores - top)
        state[4 * p : 4 * p + 1, :] = top
        state[4 * p + 1 : 4 * p + 2, :] = jnp.sum(weights, axis=0, keepdims=True)
        state[4 * p + 2 : 4 * p + 3, :] = jnp.sum(weights * seen, axis=0, keepdims=True)
        state[4 * p + 3 : 4 * p + 4, :] = jnp.zeros_like(top)
    for copy in copies:
        copy.wait()


def early(own, got, gates, qm):
    block, cols = gates.shape[1:]
    cache = jax.ShapeDtypeStruct((2, block, cols), jnp.bfloat16)
    return pl.pallas_call(
        early_kernel,
        out_shape=(cache, cache, jax.ShapeDtypeStruct((8, cols), jnp.float32)),
        in_specs=[VMEM] * 4,
        out_specs=(ANY, ANY, VMEM),
        scratch_shapes=[pltpu.SemaphoreType.DMA((2 * len(EARLY), 2))],
        compiler_params=pltpu.CompilerParams(vmem_limit_bytes=8 * 1024 * 1024),
        cost_estimate=pl.CostEstimate(
            flops=64 * 1024 * 1024, bytes_accessed=2 * 1024 * 1024, transcendentals=0
        ),
        name="early",
    )(own, got, gates, qm)


def started(copies):
    for copy in copies:
        copy.start()


def awaited(copies):
    for copy in copies:
        copy.wait()


def at_turn(turn, act):
    first = lax.axis_index("sp") < lax.axis_size("sp") // 2
    pl.when(first if turn == 0 else jnp.logical_not(first))(act)


def late_kernel(
    own, both, gates, qm, small, state, k_in, v_in, keys, values, part, sem
):
    core = lax.rem(lax.axis_index("tp"), 2)
    found = halves(own, both.at[1 - core], LATE)
    copies = stored(found, keys, values, sem)
    at_turn(0, lambda: started(copies))
    members, cols = part.shape[0], gates.shape[2]
    block = gates.shape[1]
    packed = jnp.zeros((1, cols), jnp.float32)
    quarter = lax.broadcasted_iota(jnp.int32, (1, cols), 1) % HD // (HD // 4)
    last = lax.axis_index("sp") == lax.axis_size("sp") - 1
    for p in range(2):
        scores, seen = scored(found, p, gates, qm)
        fresh = small[p : p + 1, :] - (
            gates[p, block - 1 : block, :] + small[4 + p : 5 + p, :]
        )
        fresh = jnp.where(last, fresh, MASKED)
        before = state[4 * p : 4 * p + 1, :]
        top = jnp.maximum(jnp.max(scores, axis=0, keepdims=True), fresh)
        top = jnp.maximum(top, before)
        weights = jnp.exp(scores - top)
        fresh_weight = jnp.exp(fresh - top)
        scale = jnp.exp(before - top)
        total = jnp.sum(weights, axis=0, keepdims=True) + fresh_weight
        total = total + scale * state[4 * p + 1 : 4 * p + 2, :]
        acc = jnp.sum(weights * seen, axis=0, keepdims=True)
        acc = acc + fresh_weight * small[2 + p : 3 + p, :]
        acc = acc + scale * state[4 * p + 2 : 4 * p + 3, :]
        packed = jnp.where(quarter == 2 * p, top, packed)
        packed = jnp.where(quarter == 2 * p + 1, total, packed)
        part[:, :, p * cols : (p + 1) * cols] = jnp.broadcast_to(
            acc[None], (members, 1, cols)
        )
    part[:, :, 2 * cols :] = jnp.broadcast_to(packed[None], (members, 1, cols))
    at_turn(0, lambda: awaited(copies))


def late(own, both, gates, qm, small, state, keys, values, members):
    cols = gates.shape[2]
    cache = jax.ShapeDtypeStruct(keys.shape, keys.dtype)
    return pl.pallas_call(
        late_kernel,
        out_shape=(
            cache,
            cache,
            jax.ShapeDtypeStruct((members, 1, 3 * cols), jnp.float32),
        ),
        in_specs=[VMEM] * 6 + [ANY] * 2,
        out_specs=(ANY, ANY, VMEM),
        input_output_aliases={6: 0, 7: 1},
        scratch_shapes=[pltpu.SemaphoreType.DMA((2 * len(LATE), 2))],
        compiler_params=pltpu.CompilerParams(vmem_limit_bytes=4 * 1024 * 1024),
        cost_estimate=pl.CostEstimate(
            flops=16 * 1024 * 1024, bytes_accessed=1024 * 1024, transcendentals=0
        ),
        name="late",
    )(own, both, gates, qm, small, state, keys, values)


def merge_kernel(parts, own, both, k_in, v_in, keys, values, out, sem):
    core = lax.rem(lax.axis_index("tp"), 2)
    copies = stored(halves(own, both.at[1 - core], LATE), keys, values, sem)
    at_turn(1, lambda: started(copies))
    members, cols = parts.shape[0], out.shape[1]
    packed = parts[:, 0, 2 * cols :]
    quarter = lax.broadcasted_iota(jnp.int32, (members, cols), 1) % HD // (HD // 4)

    def spread(which):
        only = jnp.where(quarter == which, packed, 0.0)
        found = only
        for to in range(4):
            if to != which:
                found = found + pltpu.roll(only, (to - which) * (HD // 4) % cols, 1)
        return found

    for p in range(2):
        tops = spread(2 * p)
        scale = jnp.exp(tops - jnp.max(tops, axis=0, keepdims=True))
        total = jnp.sum(scale * spread(2 * p + 1), axis=0, keepdims=True)
        acc = parts[:, 0, p * cols : (p + 1) * cols]
        acc = jnp.sum(scale * acc, axis=0, keepdims=True)
        out[p : p + 1, :] = (acc / total).astype(jnp.bfloat16)
    at_turn(1, lambda: awaited(copies))


def merge(parts, own, both, keys, values):
    cache = jax.ShapeDtypeStruct(keys.shape, keys.dtype)
    return pl.pallas_call(
        merge_kernel,
        out_shape=(cache, cache, jax.ShapeDtypeStruct((2, keys.shape[2]), jnp.bfloat16)),
        in_specs=[VMEM] * 3 + [ANY] * 2,
        out_specs=(ANY, ANY, VMEM),
        input_output_aliases={3: 0, 4: 1},
        scratch_shapes=[pltpu.SemaphoreType.DMA((2 * len(LATE), 2))],
        compiler_params=pltpu.CompilerParams(vmem_limit_bytes=4 * 1024 * 1024),
        name="merge",
    )(parts, own, both, keys, values)


def split_kernel(tokens, a, b):
    a[...] = tokens[0]
    b[...] = tokens[1]


def split(tokens):
    piece = jax.ShapeDtypeStruct(tokens.shape[1:], tokens.dtype)
    return pl.pallas_call(
        split_kernel,
        out_shape=(piece, piece),
        in_specs=[VMEM],
        out_specs=(VMEM, VMEM),
        compiler_params=pltpu.CompilerParams(vmem_limit_bytes=4 * 1024 * 1024),
        cost_estimate=pl.CostEstimate(
            flops=1024 * 1024, bytes_accessed=2 * 1024 * 1024, transcendentals=0
        ),
        name="split",
    )(tokens)


def shift(x, by):
    return lax.ppermute(x, "tp", by)


def body(
    tokens, norm_gain, key_weight, value_weight, cum_gates, new_query, new_key, new_value, new_gate
):
    members = lax.axis_size("sp")
    tps = lax.axis_size("tp")
    ahead = [(i, (i + 2 - 4 * (i % 2)) % tps) for i in range(tps)]
    back = [(i, (i - 2 + 4 * (i % 2)) % tps) for i in range(tps)]
    swap = [(i, i ^ 1) for i in range(tps)]
    gain = norm_gain.reshape(1, -1)
    half, width = tokens.shape[1:]
    from_3 = shift(tokens, ahead)
    a_0, b_0 = split(tokens)
    b_1 = shift(b_0, back)
    a_1 = shift(a_0, back)
    b_2 = shift(b_1, back)
    a_2 = shift(from_3[0], ahead)
    wo = jnp.concatenate([key_weight, value_weight], axis=1)
    wp = shift(wo, swap)

    made = prepare(
        jnp.swapaxes(cum_gates, 1, 2), new_query, new_key, new_value, new_gate
    )
    gain, wp, made = lax.optimization_barrier((gain, wp, made))
    gates, qm, small = made

    rows = (2 * half, width)
    done = project((tokens.reshape(rows),), gain, wo, wp, half)
    own1, par1 = project((from_3.reshape(rows), b_1, a_1), gain, wo, wp, half, done)
    got1 = shift(par1, swap)
    keys, values, state = early(own1, got1, gates, qm)
    own2, par2 = finish(a_2, b_2, gain, wo, wp)
    pairs = [[i, i + 1] for i in range(0, tps, 2)]
    both2 = lax.all_gather(par2, "tp", axis_index_groups=pairs)
    keys, values, part = late(
        own2, both2, gates, qm, small, state, keys, values, members
    )
    parts = lax.all_to_all(part, "sp", split_axis=0, concat_axis=0, tiled=True)
    return merge(parts, own2, both2, keys, values)


def solution(mesh):
    in_specs = (
        P("gr", ("sp", "tp"), None),
        P(),
        P(None, "tp"),
        P(None, "tp"),
        P("gr", "sp", "tp"),
        P("gr", "tp"),
        P("gr", "tp"),
        P("gr", "tp"),
        P("gr", "tp"),
    )
    out_specs = (P("gr", "sp", "tp"), P("gr", "sp", "tp"), P("gr", "tp"))
    return jax.shard_map(body, mesh=mesh, in_specs=in_specs, out_specs=out_specs, check_vma=False)
```

```python
import functools

import jax
import jax.numpy as jnp
from jax import lax
from jax.experimental import pallas as pl
from jax.experimental.pallas import tpu as pltpu
from jax.sharding import PartitionSpec as P


HD = 64
EPS = 1e-06
MASKED = -1e30
CHUNKS = 4


VMEM = pl.BlockSpec(memory_space=pltpu.VMEM)
ANY = pl.BlockSpec(memory_space=pl.ANY)

EARLY = ((0, 0), (0, 1), (3, 0), (3, 1), (1, 1))
LATE = ((1, 0), (2, 0), (2, 1))


def project_kernel(count, prior, *refs):
    xs, refs = refs[:count], refs[count:]
    before, (gain, wo, wp, own, par, n_s) = refs[: 2 * prior], refs[2 * prior :]
    width = xs[0].shape[1]
    half = own.shape[1]
    step = 16

    def normalize(x, base):
        def rows_of(i, carry):
            rows = pl.ds(pl.multiple_of(i * step, step), step)
            total = jnp.zeros((step, 128), jnp.float32)
            for c in range(width // 1024):
                part = x[rows, pl.ds(c * 1024, 1024)].astype(jnp.float32)
                part = part * part
                for j in range(8):
                    total = total + part[:, j * 128 : (j + 1) * 128]
            mean = jnp.sum(total, axis=-1, keepdims=True) * (1.0 / width)
            scale = lax.rsqrt(mean + EPS)
            out = pl.ds(pl.multiple_of(base + i * step, step), step)
            for c in range(width // 1024):
                at = pl.ds(c * 1024, 1024)
                part = x[rows, at].astype(jnp.float32)
                part = part * scale * gain[:, at].astype(jnp.float32)
                n_s[out, at] = part.astype(jnp.bfloat16)
            return carry

        lax.fori_loop(0, x.shape[0] // step, rows_of, 0, unroll=2)

    base = 0
    for x in xs:
        normalize(x, base)
        base += x.shape[0]
    for k, (w, out) in enumerate(((wo, own), (wp, par))):
        acc = jnp.dot(n_s[...], w[...], preferred_element_type=jnp.float32)
        done = before[k].shape[0] if prior else 0
        if prior:
            out[:done] = before[k][...]
        out[done:] = acc.astype(jnp.bfloat16).reshape(-1, half, out.shape[2])


def finish_kernel(xa, xb, own_in, par_in, gain, wo, wp, own, par, n_s):
    half, width = xa.shape
    cols = wo.shape[1]
    piece = width // CHUNKS
    scales = []
    for x in (xa, xb):
        total = jnp.zeros((half, 128), jnp.float32)
        for j in range(width // 128):
            part = x[:, j * 128 : (j + 1) * 128].astype(jnp.float32)
            total = total + part * part
        mean = jnp.sum(total, axis=-1, keepdims=True) * (1.0 / width)
        scales.append(lax.rsqrt(mean + EPS))
    sums = [jnp.zeros((2 * half, cols), jnp.float32) for _ in range(2)]
    for c in range(CHUNKS):
        at = slice(c * piece, (c + 1) * piece)
        factor = gain[:, at].astype(jnp.float32)
        for k, x in enumerate((xa, xb)):
            part = x[:, at].astype(jnp.float32) * scales[k] * factor
            n_s[k * half : (k + 1) * half, at] = part.astype(jnp.bfloat16)
        for k, w in enumerate((wo, wp)):
            sums[k] = sums[k] + jnp.dot(
                n_s[:, at], w[at, :], preferred_element_type=jnp.float32
            )
    done = own_in.shape[0]
    for out, before, acc in zip((own, par), (own_in, par_in), sums):
        out[:done] = before[...]
        out[done:] = acc.astype(jnp.bfloat16).reshape(-1, half, cols)


def finish(xa, xb, own, par, gain, wo, wp):
    half, width = xa.shape
    cols = wo.shape[1]
    out = jax.ShapeDtypeStruct((2 + own.shape[0], half, cols), jnp.bfloat16)
    return pl.pallas_call(
        finish_kernel,
        out_shape=(out, out),
        in_specs=[VMEM] * 7,
        out_specs=(VMEM, VMEM),
        scratch_shapes=[pltpu.VMEM((2 * half, width), jnp.bfloat16)],
        compiler_params=pltpu.CompilerParams(vmem_limit_bytes=16 * 1024 * 1024),
        cost_estimate=pl.CostEstimate(
            flops=8 * half * width * cols, bytes_accessed=6 * 1024 * 1024, transcendentals=0
        ),
        name="finish",
    )(xa, xb, own, par, gain, wo, wp)


def project(xs, gain, wo, wp, half, before=()):
    rows = sum(x.shape[0] for x in xs)
    width, cols = wo.shape
    done = before[0].shape[0] if before else 0
    out = jax.ShapeDtypeStruct((done + rows // half, half, cols), jnp.bfloat16)
    return pl.pallas_call(
        functools.partial(project_kernel, len(xs), bool(before)),
        out_shape=(out, out),
        in_specs=[VMEM] * (len(xs) + len(before) + 3),
        out_specs=(VMEM, VMEM),
        scratch_shapes=[pltpu.VMEM((rows, width), jnp.bfloat16)],
        compiler_params=pltpu.CompilerParams(vmem_limit_bytes=16 * 1024 * 1024),
        cost_estimate=pl.CostEstimate(
            flops=2 * rows * width * 2 * cols,
            bytes_accessed=6 * 1024 * 1024,
            transcendentals=0,
        ),
        name="project",
    )(*xs, *before, gain, wo, wp)


def prepare_kernel(cum, q, fk, fv, ng, gates, qm, small):
    block, cols = gates.shape[1:]
    shape = (cols, cols)
    same = lax.broadcasted_iota(jnp.int32, shape, 0) // HD == (
        lax.broadcasted_iota(jnp.int32, shape, 1) // HD
    )
    first = lax.broadcasted_iota(jnp.int32, (2, cols), 1) < HD
    for p in range(2):
        spread = [jnp.broadcast_to(cum[p, h : h + 1, :], (HD, block)) for h in range(2)]
        gates[p] = jnp.concatenate(spread, axis=0).T
        down = jnp.broadcast_to(q[p : p + 1, :].astype(jnp.float32), shape).T
        qm[p] = jnp.where(same, down, 0.0).astype(jnp.bfloat16)
        fresh = jnp.dot(fk[...], qm[p], preferred_element_type=jnp.float32)
        small[p : p + 1, :] = fresh[p : p + 1] * (HD**-0.5)
    small[2:4, :] = fv[...].astype(jnp.float32)
    small[4:6, :] = jnp.where(first, ng[:, 0:1], ng[:, 1:2])
    small[6:8, :] = jnp.zeros((2, cols), jnp.float32)


def prepare(cum, q, fk, fv, ng):
    block, cols = cum.shape[2], q.shape[1]
    return pl.pallas_call(
        prepare_kernel,
        out_shape=(
            jax.ShapeDtypeStruct((2, block, cols), jnp.float32),
            jax.ShapeDtypeStruct((2, cols, cols), jnp.bfloat16),
            jax.ShapeDtypeStruct((8, cols), jnp.float32),
        ),
        in_specs=[VMEM] * 5,
        out_specs=(VMEM,) * 3,
        compiler_params=pltpu.CompilerParams(vmem_limit_bytes=8 * 1024 * 1024),
        cost_estimate=pl.CostEstimate(
            flops=1024 * 1024, bytes_accessed=1024 * 1024, transcendentals=0
        ),
        name="prepare",
    )(cum, q, fk, fv, ng)


def halves(own, got, places):
    tp = lax.axis_index("tp")
    x, core = tp // 2, lax.rem(tp, 2)
    half = own.shape[1]
    found = []
    for side, ref in enumerate((own, got)):
        which = lax.rem(core + side, 2)
        for k, (off, p) in enumerate(places):
            place = lax.rem(x + jnp.where(which == 0, off, (4 - off) % 4), 4)
            found.append((ref, k, p, pl.multiple_of((place * 2 + which) * half, half)))
    return found


def stored(found, keys, values, sem):
    cols = keys.shape[2]
    copies = []
    for i, (ref, k, p, at) in enumerate(found):
        rows = pl.ds(at, ref.shape[1])
        for j, cache in enumerate((keys, values)):
            copies.append(
                pltpu.make_async_copy(
                    ref.at[k, :, pl.ds(j * cols, cols)], cache.at[p, rows, :], sem.at[i, j]
                )
            )
    return copies


def scored(found, p, gates, qm):
    cols = qm.shape[2]
    parts, seen = [], []
    for ref, k, prompt, at in found:
        if prompt == p:
            part = jnp.dot(ref[k, :, :cols], qm[p], preferred_element_type=jnp.float32)
            parts.append(part * (HD**-0.5) - gates[p, pl.ds(at, ref.shape[1]), :])
            seen.append(ref[k, :, cols:].astype(jnp.float32))
    return jnp.concatenate(parts, axis=0), jnp.concatenate(seen, axis=0)


def early_kernel(own, got, gates, qm, keys, values, state, sem):
    found = halves(own, got, EARLY)
    copies = stored(found, keys, values, sem)
    for copy in copies:
        copy.start()
    for p in range(2):
        scores, seen = scored(found, p, gates, qm)
        top = jnp.max(scores, axis=0, keepdims=True)
        weights = jnp.exp(scores - top)
        state[4 * p : 4 * p + 1, :] = top
        state[4 * p + 1 : 4 * p + 2, :] = jnp.sum(weights, axis=0, keepdims=True)
        state[4 * p + 2 : 4 * p + 3, :] = jnp.sum(weights * seen, axis=0, keepdims=True)
        state[4 * p + 3 : 4 * p + 4, :] = jnp.zeros_like(top)
    for copy in copies:
        copy.wait()


def early(own, got, gates, qm):
    block, cols = gates.shape[1:]
    cache = jax.ShapeDtypeStruct((2, block, cols), jnp.bfloat16)
    return pl.pallas_call(
        early_kernel,
        out_shape=(cache, cache, jax.ShapeDtypeStruct((8, cols), jnp.float32)),
        in_specs=[VMEM] * 4,
        out_specs=(ANY, ANY, VMEM),
        scratch_shapes=[pltpu.SemaphoreType.DMA((2 * len(EARLY), 2))],
        compiler_params=pltpu.CompilerParams(vmem_limit_bytes=8 * 1024 * 1024),
        cost_estimate=pl.CostEstimate(
            flops=64 * 1024 * 1024, bytes_accessed=2 * 1024 * 1024, transcendentals=0
        ),
        name="early",
    )(own, got, gates, qm)


def started(copies):
    for copy in copies:
        copy.start()


def awaited(copies):
    for copy in copies:
        copy.wait()


def at_turn(turn, act):
    first = lax.axis_index("sp") < lax.axis_size("sp") // 2
    pl.when(first if turn == 0 else jnp.logical_not(first))(act)


def late_kernel(
    own, both, gates, qm, small, state, k_in, v_in, keys, values, part, sem
):
    core = lax.rem(lax.axis_index("tp"), 2)
    found = halves(own, both.at[1 - core], LATE)
    copies = stored(found, keys, values, sem)
    at_turn(0, lambda: started(copies))
    members, cols = part.shape[0], gates.shape[2]
    block = gates.shape[1]
    packed = jnp.zeros((1, cols), jnp.float32)
    quarter = lax.broadcasted_iota(jnp.int32, (1, cols), 1) % HD // (HD // 4)
    last = lax.axis_index("sp") == lax.axis_size("sp") - 1
    for p in range(2):
        scores, seen = scored(found, p, gates, qm)
        fresh = small[p : p + 1, :] - (
            gates[p, block - 1 : block, :] + small[4 + p : 5 + p, :]
        )
        fresh = jnp.where(last, fresh, MASKED)
        before = state[4 * p : 4 * p + 1, :]
        top = jnp.maximum(jnp.max(scores, axis=0, keepdims=True), fresh)
        top = jnp.maximum(top, before)
        weights = jnp.exp(scores - top)
        fresh_weight = jnp.exp(fresh - top)
        scale = jnp.exp(before - top)
        total = jnp.sum(weights, axis=0, keepdims=True) + fresh_weight
        total = total + scale * state[4 * p + 1 : 4 * p + 2, :]
        acc = jnp.sum(weights * seen, axis=0, keepdims=True)
        acc = acc + fresh_weight * small[2 + p : 3 + p, :]
        acc = acc + scale * state[4 * p + 2 : 4 * p + 3, :]
        packed = jnp.where(quarter == 2 * p, top, packed)
        packed = jnp.where(quarter == 2 * p + 1, total, packed)
        part[:, :, p * cols : (p + 1) * cols] = jnp.broadcast_to(
            acc[None], (members, 1, cols)
        )
    part[:, :, 2 * cols :] = jnp.broadcast_to(packed[None], (members, 1, cols))
    at_turn(0, lambda: awaited(copies))


def late(own, both, gates, qm, small, state, keys, values, members):
    cols = gates.shape[2]
    cache = jax.ShapeDtypeStruct(keys.shape, keys.dtype)
    return pl.pallas_call(
        late_kernel,
        out_shape=(
            cache,
            cache,
            jax.ShapeDtypeStruct((members, 1, 3 * cols), jnp.float32),
        ),
        in_specs=[VMEM] * 6 + [ANY] * 2,
        out_specs=(ANY, ANY, VMEM),
        input_output_aliases={6: 0, 7: 1},
        scratch_shapes=[pltpu.SemaphoreType.DMA((2 * len(LATE), 2))],
        compiler_params=pltpu.CompilerParams(vmem_limit_bytes=4 * 1024 * 1024),
        cost_estimate=pl.CostEstimate(
            flops=16 * 1024 * 1024, bytes_accessed=1024 * 1024, transcendentals=0
        ),
        name="late",
    )(own, both, gates, qm, small, state, keys, values)


def merge_kernel(parts, own, both, k_in, v_in, keys, values, out, sem):
    core = lax.rem(lax.axis_index("tp"), 2)
    copies = stored(halves(own, both.at[1 - core], LATE), keys, values, sem)
    at_turn(1, lambda: started(copies))
    members, cols = parts.shape[0], out.shape[1]
    packed = parts[:, 0, 2 * cols :]
    quarter = lax.broadcasted_iota(jnp.int32, (members, cols), 1) % HD // (HD // 4)

    def spread(which):
        only = jnp.where(quarter == which, packed, 0.0)
        found = only
        for to in range(4):
            if to != which:
                found = found + pltpu.roll(only, (to - which) * (HD // 4) % cols, 1)
        return found

    for p in range(2):
        tops = spread(2 * p)
        scale = jnp.exp(tops - jnp.max(tops, axis=0, keepdims=True))
        total = jnp.sum(scale * spread(2 * p + 1), axis=0, keepdims=True)
        acc = parts[:, 0, p * cols : (p + 1) * cols]
        acc = jnp.sum(scale * acc, axis=0, keepdims=True)
        out[p : p + 1, :] = (acc / total).astype(jnp.bfloat16)
    at_turn(1, lambda: awaited(copies))


def merge(parts, own, both, keys, values):
    cache = jax.ShapeDtypeStruct(keys.shape, keys.dtype)
    return pl.pallas_call(
        merge_kernel,
        out_shape=(cache, cache, jax.ShapeDtypeStruct((2, keys.shape[2]), jnp.bfloat16)),
        in_specs=[VMEM] * 3 + [ANY] * 2,
        out_specs=(ANY, ANY, VMEM),
        input_output_aliases={3: 0, 4: 1},
        scratch_shapes=[pltpu.SemaphoreType.DMA((2 * len(LATE), 2))],
        compiler_params=pltpu.CompilerParams(vmem_limit_bytes=4 * 1024 * 1024),
        name="merge",
    )(parts, own, both, keys, values)


def split_kernel(tokens, a, b):
    a[...] = tokens[0]
    b[...] = tokens[1]


def split(tokens):
    piece = jax.ShapeDtypeStruct(tokens.shape[1:], tokens.dtype)
    return pl.pallas_call(
        split_kernel,
        out_shape=(piece, piece),
        in_specs=[VMEM],
        out_specs=(VMEM, VMEM),
        compiler_params=pltpu.CompilerParams(vmem_limit_bytes=4 * 1024 * 1024),
        cost_estimate=pl.CostEstimate(
            flops=1024 * 1024, bytes_accessed=2 * 1024 * 1024, transcendentals=0
        ),
        name="split",
    )(tokens)


def shift(x, by):
    return lax.ppermute(x, "tp", by)


def body(
    tokens, norm_gain, key_weight, value_weight, cum_gates, new_query, new_key, new_value, new_gate
):
    members = lax.axis_size("sp")
    tps = lax.axis_size("tp")
    ahead = [(i, (i + 2 - 4 * (i % 2)) % tps) for i in range(tps)]
    back = [(i, (i - 2 + 4 * (i % 2)) % tps) for i in range(tps)]
    swap = [(i, i ^ 1) for i in range(tps)]
    gain = norm_gain.reshape(1, -1)
    half, width = tokens.shape[1:]
    from_3 = shift(tokens, ahead)
    a_0, b_0 = split(tokens)
    b_1 = shift(b_0, back)
    a_1 = shift(a_0, back)
    b_2 = shift(b_1, back)
    a_3 = from_3[0]
    a_2 = shift(a_3, ahead)
    wo = jnp.concatenate([key_weight, value_weight], axis=1)
    wp = shift(wo, swap)

    made = prepare(
        jnp.swapaxes(cum_gates, 1, 2), new_query, new_key, new_value, new_gate
    )
    gain, wp, made = lax.optimization_barrier((gain, wp, made))
    gates, qm, small = made

    rows = (2 * half, width)
    done = project((tokens.reshape(rows),), gain, wo, wp, half)
    own1, par1 = project(
        (from_3.reshape(rows), b_1), gain, wo, wp, half, done
    )
    got1 = shift(par1, swap)
    done = project((a_1,), gain, wo, wp, half)
    keys, values, state = early(own1, got1, gates, qm)
    own2, par2 = finish(a_2, b_2, *done, gain, wo, wp)
    pairs = [[i, i + 1] for i in range(0, tps, 2)]
    both2 = lax.all_gather(par2, "tp", axis_index_groups=pairs)
    keys, values, part = late(
        own2, both2, gates, qm, small, state, keys, values, members
    )
    parts = lax.all_to_all(part, "sp", split_axis=0, concat_axis=0, tiled=True)
    return merge(parts, own2, both2, keys, values)


def solution(mesh):
    in_specs = (
        P("gr", ("sp", "tp"), None),
        P(),
        P(None, "tp"),
        P(None, "tp"),
        P("gr", "sp", "tp"),
        P("gr", "tp"),
        P("gr", "tp"),
        P("gr", "tp"),
        P("gr", "tp"),
    )
    out_specs = (P("gr", "sp", "tp"), P("gr", "sp", "tp"), P("gr", "tp"))
    return jax.shard_map(body, mesh=mesh, in_specs=in_specs, out_specs=out_specs, check_vma=False)
```

```python
import functools

import jax
import jax.numpy as jnp
from jax import lax
from jax.experimental import pallas as pl
from jax.experimental.pallas import tpu as pltpu
from jax.sharding import PartitionSpec as P


HD = 64
EPS = 1e-06
MASKED = -1e30
CHUNKS = 16


VMEM = pl.BlockSpec(memory_space=pltpu.VMEM)
ANY = pl.BlockSpec(memory_space=pl.ANY)

EARLY = ((0, 0), (0, 1), (1, 1), (3, 0), (3, 1))
LATE = ((1, 0), (2, 1), (2, 0))


def project_kernel(count, prior, *refs):
    xs, refs = refs[:count], refs[count:]
    before, (gain, wo, wp, own, par, n_s) = refs[: 2 * prior], refs[2 * prior :]
    width = xs[0].shape[1]
    half = own.shape[1]
    step = 16

    def normalize(x, base):
        def rows_of(i, carry):
            rows = pl.ds(pl.multiple_of(i * step, step), step)
            total = jnp.zeros((step, 128), jnp.float32)
            for c in range(width // 1024):
                part = x[rows, pl.ds(c * 1024, 1024)].astype(jnp.float32)
                part = part * part
                for j in range(8):
                    total = total + part[:, j * 128 : (j + 1) * 128]
            mean = jnp.sum(total, axis=-1, keepdims=True) * (1.0 / width)
            scale = lax.rsqrt(mean + EPS)
            out = pl.ds(pl.multiple_of(base + i * step, step), step)
            for c in range(width // 1024):
                at = pl.ds(c * 1024, 1024)
                part = x[rows, at].astype(jnp.float32)
                part = part * scale * gain[:, at].astype(jnp.float32)
                n_s[out, at] = part.astype(jnp.bfloat16)
            return carry

        lax.fori_loop(0, x.shape[0] // step, rows_of, 0, unroll=2)

    base = 0
    for x in xs:
        normalize(x, base)
        base += x.shape[0]
    for k, (w, out) in enumerate(((wo, own), (wp, par))):
        acc = jnp.dot(n_s[...], w[...], preferred_element_type=jnp.float32)
        done = before[k].shape[0] if prior else 0
        if prior:
            out[:done] = before[k][...]
        out[done:] = acc.astype(jnp.bfloat16).reshape(-1, half, out.shape[2])


def finish_kernel(count, *refs):
    xs, (own_in, par_in, gain, wo, wp, own, par, n_s) = refs[:count], refs[count:]
    half, width = xs[0].shape
    cols = wo.shape[1]
    piece = width // CHUNKS
    scales = []
    for x in xs:
        total = jnp.zeros((half, 128), jnp.float32)
        for j in range(width // 128):
            part = x[:, j * 128 : (j + 1) * 128].astype(jnp.float32)
            total = total + part * part
        mean = jnp.sum(total, axis=-1, keepdims=True) * (1.0 / width)
        scales.append(lax.rsqrt(mean + EPS))
    sums = [jnp.zeros((count * half, cols), jnp.float32) for _ in range(2)]
    for c in range(CHUNKS):
        at = slice(c * piece, (c + 1) * piece)
        factor = gain[:, at].astype(jnp.float32)
        for k, x in enumerate(xs):
            part = x[:, at].astype(jnp.float32) * scales[k] * factor
            n_s[k * half : (k + 1) * half, at] = part.astype(jnp.bfloat16)
        for k, w in enumerate((wo, wp)):
            sums[k] = sums[k] + jnp.dot(
                n_s[:, at], w[at, :], preferred_element_type=jnp.float32
            )
    done = own_in.shape[0]
    for out, before, acc in zip((own, par), (own_in, par_in), sums):
        out[:done] = before[...]
        out[done:] = acc.astype(jnp.bfloat16).reshape(count, half, cols)


def finish(xs, own, par, gain, wo, wp):
    count, (half, width) = len(xs), xs[0].shape
    cols = wo.shape[1]
    out = jax.ShapeDtypeStruct((count + own.shape[0], half, cols), jnp.bfloat16)
    return pl.pallas_call(
        functools.partial(finish_kernel, count),
        out_shape=(out, out),
        in_specs=[VMEM] * (count + 5),
        out_specs=(VMEM, VMEM),
        scratch_shapes=[pltpu.VMEM((count * half, width), jnp.bfloat16)],
        compiler_params=pltpu.CompilerParams(vmem_limit_bytes=16 * 1024 * 1024),
        cost_estimate=pl.CostEstimate(
            flops=4 * count * half * width * cols,
            bytes_accessed=6 * 1024 * 1024,
            transcendentals=0,
        ),
        name="finish",
    )(*xs, own, par, gain, wo, wp)


def project(xs, gain, wo, wp, half, before=()):
    rows = sum(x.shape[0] for x in xs)
    width, cols = wo.shape
    done = before[0].shape[0] if before else 0
    out = jax.ShapeDtypeStruct((done + rows // half, half, cols), jnp.bfloat16)
    return pl.pallas_call(
        functools.partial(project_kernel, len(xs), bool(before)),
        out_shape=(out, out),
        in_specs=[VMEM] * (len(xs) + len(before) + 3),
        out_specs=(VMEM, VMEM),
        scratch_shapes=[pltpu.VMEM((rows, width), jnp.bfloat16)],
        compiler_params=pltpu.CompilerParams(vmem_limit_bytes=16 * 1024 * 1024),
        cost_estimate=pl.CostEstimate(
            flops=2 * rows * width * 2 * cols,
            bytes_accessed=6 * 1024 * 1024,
            transcendentals=0,
        ),
        name="project",
    )(*xs, *before, gain, wo, wp)


def prepare_kernel(cum, q, fk, fv, ng, gates, qm, small):
    block, cols = gates.shape[1:]
    shape = (cols, cols)
    same = lax.broadcasted_iota(jnp.int32, shape, 0) // HD == (
        lax.broadcasted_iota(jnp.int32, shape, 1) // HD
    )
    first = lax.broadcasted_iota(jnp.int32, (2, cols), 1) < HD
    for p in range(2):
        spread = [jnp.broadcast_to(cum[p, h : h + 1, :], (HD, block)) for h in range(2)]
        gates[p] = jnp.concatenate(spread, axis=0).T
        down = jnp.broadcast_to(q[p : p + 1, :].astype(jnp.float32), shape).T
        qm[p] = jnp.where(same, down, 0.0).astype(jnp.bfloat16)
        fresh = jnp.dot(fk[...], qm[p], preferred_element_type=jnp.float32)
        small[p : p + 1, :] = fresh[p : p + 1] * (HD**-0.5)
    small[2:4, :] = fv[...].astype(jnp.float32)
    small[4:6, :] = jnp.where(first, ng[:, 0:1], ng[:, 1:2])
    small[6:8, :] = jnp.zeros((2, cols), jnp.float32)


def prepare(cum, q, fk, fv, ng):
    block, cols = cum.shape[2], q.shape[1]
    return pl.pallas_call(
        prepare_kernel,
        out_shape=(
            jax.ShapeDtypeStruct((2, block, cols), jnp.float32),
            jax.ShapeDtypeStruct((2, cols, cols), jnp.bfloat16),
            jax.ShapeDtypeStruct((8, cols), jnp.float32),
        ),
        in_specs=[VMEM] * 5,
        out_specs=(VMEM,) * 3,
        compiler_params=pltpu.CompilerParams(vmem_limit_bytes=8 * 1024 * 1024),
        cost_estimate=pl.CostEstimate(
            flops=1024 * 1024, bytes_accessed=1024 * 1024, transcendentals=0
        ),
        name="prepare",
    )(cum, q, fk, fv, ng)


def halves(own, got, places):
    tp = lax.axis_index("tp")
    x, core = tp // 2, lax.rem(tp, 2)
    half = own.shape[1]
    found = []
    for side, ref in enumerate((own, got)):
        which = lax.rem(core + side, 2)
        for k, (off, p) in enumerate(places):
            place = lax.rem(x + jnp.where(which == 0, off, (4 - off) % 4), 4)
            found.append((ref, k, p, pl.multiple_of((place * 2 + which) * half, half)))
    return found


def stored(found, keys, values, sem):
    cols = keys.shape[2]
    copies = []
    for i, (ref, k, p, at) in enumerate(found):
        rows = pl.ds(at, ref.shape[1])
        for j, cache in enumerate((keys, values)):
            copies.append(
                pltpu.make_async_copy(
                    ref.at[k, :, pl.ds(j * cols, cols)], cache.at[p, rows, :], sem.at[i, j]
                )
            )
    return copies


def scored(found, p, gates, qm):
    cols = qm.shape[2]
    parts, seen = [], []
    for ref, k, prompt, at in found:
        if prompt == p:
            part = jnp.dot(ref[k, :, :cols], qm[p], preferred_element_type=jnp.float32)
            parts.append(part * (HD**-0.5) - gates[p, pl.ds(at, ref.shape[1]), :])
            seen.append(ref[k, :, cols:].astype(jnp.float32))
    return jnp.concatenate(parts, axis=0), jnp.concatenate(seen, axis=0)


def early_kernel(own, got, gates, qm, keys, values, state, sem):
    found = halves(own, got, EARLY)
    copies = stored(found, keys, values, sem)
    for copy in copies:
        copy.start()
    for p in range(2):
        scores, seen = scored(found, p, gates, qm)
        top = jnp.max(scores, axis=0, keepdims=True)
        weights = jnp.exp(scores - top)
        state[4 * p : 4 * p + 1, :] = top
        state[4 * p + 1 : 4 * p + 2, :] = jnp.sum(weights, axis=0, keepdims=True)
        state[4 * p + 2 : 4 * p + 3, :] = jnp.sum(weights * seen, axis=0, keepdims=True)
        state[4 * p + 3 : 4 * p + 4, :] = jnp.zeros_like(top)
    for copy in copies:
        copy.wait()


def early(own, got, gates, qm):
    block, cols = gates.shape[1:]
    cache = jax.ShapeDtypeStruct((2, block, cols), jnp.bfloat16)
    return pl.pallas_call(
        early_kernel,
        out_shape=(cache, cache, jax.ShapeDtypeStruct((8, cols), jnp.float32)),
        in_specs=[VMEM] * 4,
        out_specs=(ANY, ANY, VMEM),
        scratch_shapes=[pltpu.SemaphoreType.DMA((2 * len(EARLY), 2))],
        compiler_params=pltpu.CompilerParams(vmem_limit_bytes=8 * 1024 * 1024),
        cost_estimate=pl.CostEstimate(
            flops=64 * 1024 * 1024, bytes_accessed=2 * 1024 * 1024, transcendentals=0
        ),
        name="early",
    )(own, got, gates, qm)


def started(copies):
    for copy in copies:
        copy.start()


def awaited(copies):
    for copy in copies:
        copy.wait()


def at_turn(turn, act):
    first = lax.axis_index("sp") < lax.axis_size("sp") // 2
    pl.when(first if turn == 0 else jnp.logical_not(first))(act)


def late_kernel(
    own, both, gates, qm, small, state, k_in, v_in, keys, values, part, sem
):
    core = lax.rem(lax.axis_index("tp"), 2)
    found = halves(own, both.at[1 - core], LATE)
    copies = stored(found, keys, values, sem)
    at_turn(0, lambda: started(copies))
    members, cols = part.shape[0], gates.shape[2]
    block = gates.shape[1]
    packed = jnp.zeros((1, cols), jnp.float32)
    quarter = lax.broadcasted_iota(jnp.int32, (1, cols), 1) % HD // (HD // 4)
    last = lax.axis_index("sp") == lax.axis_size("sp") - 1
    for p in range(2):
        scores, seen = scored(found, p, gates, qm)
        fresh = small[p : p + 1, :] - (
            gates[p, block - 1 : block, :] + small[4 + p : 5 + p, :]
        )
        fresh = jnp.where(last, fresh, MASKED)
        before = state[4 * p : 4 * p + 1, :]
        top = jnp.maximum(jnp.max(scores, axis=0, keepdims=True), fresh)
        top = jnp.maximum(top, before)
        weights = jnp.exp(scores - top)
        fresh_weight = jnp.exp(fresh - top)
        scale = jnp.exp(before - top)
        total = jnp.sum(weights, axis=0, keepdims=True) + fresh_weight
        total = total + scale * state[4 * p + 1 : 4 * p + 2, :]
        acc = jnp.sum(weights * seen, axis=0, keepdims=True)
        acc = acc + fresh_weight * small[2 + p : 3 + p, :]
        acc = acc + scale * state[4 * p + 2 : 4 * p + 3, :]
        packed = jnp.where(quarter == 2 * p, top, packed)
        packed = jnp.where(quarter == 2 * p + 1, total, packed)
        part[:, :, p * cols : (p + 1) * cols] = jnp.broadcast_to(
            acc[None], (members, 1, cols)
        )
    part[:, :, 2 * cols :] = jnp.broadcast_to(packed[None], (members, 1, cols))
    at_turn(0, lambda: awaited(copies))


def late(own, both, gates, qm, small, state, keys, values, members):
    cols = gates.shape[2]
    cache = jax.ShapeDtypeStruct(keys.shape, keys.dtype)
    return pl.pallas_call(
        late_kernel,
        out_shape=(
            cache,
            cache,
            jax.ShapeDtypeStruct((members, 1, 3 * cols), jnp.float32),
        ),
        in_specs=[VMEM] * 6 + [ANY] * 2,
        out_specs=(ANY, ANY, VMEM),
        input_output_aliases={6: 0, 7: 1},
        scratch_shapes=[pltpu.SemaphoreType.DMA((2 * len(LATE), 2))],
        compiler_params=pltpu.CompilerParams(vmem_limit_bytes=4 * 1024 * 1024),
        cost_estimate=pl.CostEstimate(
            flops=16 * 1024 * 1024, bytes_accessed=1024 * 1024, transcendentals=0
        ),
        name="late",
    )(own, both, gates, qm, small, state, keys, values)


def merge_kernel(parts, own, both, k_in, v_in, keys, values, out, sem):
    core = lax.rem(lax.axis_index("tp"), 2)
    copies = stored(halves(own, both.at[1 - core], LATE), keys, values, sem)
    at_turn(1, lambda: started(copies))
    members, cols = parts.shape[0], out.shape[1]
    packed = parts[:, 0, 2 * cols :]
    quarter = lax.broadcasted_iota(jnp.int32, (members, cols), 1) % HD // (HD // 4)

    def spread(which):
        only = jnp.where(quarter == which, packed, 0.0)
        found = only
        for to in range(4):
            if to != which:
                found = found + pltpu.roll(only, (to - which) * (HD // 4) % cols, 1)
        return found

    for p in range(2):
        tops = spread(2 * p)
        scale = jnp.exp(tops - jnp.max(tops, axis=0, keepdims=True))
        total = jnp.sum(scale * spread(2 * p + 1), axis=0, keepdims=True)
        acc = parts[:, 0, p * cols : (p + 1) * cols]
        acc = jnp.sum(scale * acc, axis=0, keepdims=True)
        out[p : p + 1, :] = (acc / total).astype(jnp.bfloat16)
    at_turn(1, lambda: awaited(copies))


def merge(parts, own, both, keys, values):
    cache = jax.ShapeDtypeStruct(keys.shape, keys.dtype)
    return pl.pallas_call(
        merge_kernel,
        out_shape=(cache, cache, jax.ShapeDtypeStruct((2, keys.shape[2]), jnp.bfloat16)),
        in_specs=[VMEM] * 3 + [ANY] * 2,
        out_specs=(ANY, ANY, VMEM),
        input_output_aliases={3: 0, 4: 1},
        scratch_shapes=[pltpu.SemaphoreType.DMA((2 * len(LATE), 2))],
        compiler_params=pltpu.CompilerParams(vmem_limit_bytes=4 * 1024 * 1024),
        name="merge",
    )(parts, own, both, keys, values)


def split_kernel(tokens, a, b):
    a[...] = tokens[0]
    b[...] = tokens[1]


def split(tokens):
    piece = jax.ShapeDtypeStruct(tokens.shape[1:], tokens.dtype)
    return pl.pallas_call(
        split_kernel,
        out_shape=(piece, piece),
        in_specs=[VMEM],
        out_specs=(VMEM, VMEM),
        compiler_params=pltpu.CompilerParams(vmem_limit_bytes=4 * 1024 * 1024),
        cost_estimate=pl.CostEstimate(
            flops=1024 * 1024, bytes_accessed=2 * 1024 * 1024, transcendentals=0
        ),
        name="split",
    )(tokens)


def shift(x, by):
    return lax.ppermute(x, "tp", by)


def body(
    tokens, norm_gain, key_weight, value_weight, cum_gates, new_query, new_key, new_value, new_gate
):
    members = lax.axis_size("sp")
    tps = lax.axis_size("tp")
    ahead = [(i, (i + 2 - 4 * (i % 2)) % tps) for i in range(tps)]
    back = [(i, (i - 2 + 4 * (i % 2)) % tps) for i in range(tps)]
    swap = [(i, i ^ 1) for i in range(tps)]
    gain = norm_gain.reshape(1, -1)
    half, width = tokens.shape[1:]
    from_3 = shift(tokens, ahead)
    a_0, b_0 = split(tokens)
    b_1 = shift(b_0, back)
    a_1 = shift(a_0, back)
    b_2 = shift(b_1, back)
    a_3 = from_3[0]
    a_2 = shift(a_3, ahead)
    wo = jnp.concatenate([key_weight, value_weight], axis=1)
    wp = shift(wo, swap)

    made = prepare(
        jnp.swapaxes(cum_gates, 1, 2), new_query, new_key, new_value, new_gate
    )
    gain, wp, made = lax.optimization_barrier((gain, wp, made))
    gates, qm, small = made

    rows = (2 * half, width)
    done = project((tokens.reshape(rows), b_1), gain, wo, wp, half)
    own1, par1 = project(
        (from_3.reshape(rows),), gain, wo, wp, half, done
    )
    got1 = shift(par1, swap)
    done = project((a_1, b_2), gain, wo, wp, half)
    keys, values, state = early(own1, got1, gates, qm)
    own2, par2 = finish((a_2,), *done, gain, wo, wp)
    pairs = [[i, i + 1] for i in range(0, tps, 2)]
    both2 = lax.all_gather(par2, "tp", axis_index_groups=pairs)
    keys, values, part = late(
        own2, both2, gates, qm, small, state, keys, values, members
    )
    parts = lax.all_to_all(part, "sp", split_axis=0, concat_axis=0, tiled=True)
    return merge(parts, own2, both2, keys, values)


def solution(mesh):
    in_specs = (
        P("gr", ("sp", "tp"), None),
        P(),
        P(None, "tp"),
        P(None, "tp"),
        P("gr", "sp", "tp"),
        P("gr", "tp"),
        P("gr", "tp"),
        P("gr", "tp"),
        P("gr", "tp"),
    )
    out_specs = (P("gr", "sp", "tp"), P("gr", "sp", "tp"), P("gr", "tp"))
    return jax.shard_map(body, mesh=mesh, in_specs=in_specs, out_specs=out_specs, check_vma=False)
```

```python
import functools

import jax
import jax.numpy as jnp
from jax import lax
from jax.experimental import pallas as pl
from jax.experimental.pallas import tpu as pltpu
from jax.sharding import PartitionSpec as P


HD = 64
EPS = 1e-06
MASKED = -1e30
CHUNKS = 16


VMEM = pl.BlockSpec(memory_space=pltpu.VMEM)
ANY = pl.BlockSpec(memory_space=pl.ANY)

EARLY = ((0, 0), (0, 1), (3, 0), (3, 1), (1, 1))
LATE = ((1, 0), (2, 1), (2, 0))


def project_kernel(count, prior, *refs):
    xs, refs = refs[:count], refs[count:]
    before, (gain, wo, wp, own, par, n_s) = refs[: 2 * prior], refs[2 * prior :]
    width = xs[0].shape[1]
    half = own.shape[1]
    step = 16

    def normalize(x, base):
        def rows_of(i, carry):
            rows = pl.ds(pl.multiple_of(i * step, step), step)
            total = jnp.zeros((step, 128), jnp.float32)
            for c in range(width // 1024):
                part = x[rows, pl.ds(c * 1024, 1024)].astype(jnp.float32)
                part = part * part
                for j in range(8):
                    total = total + part[:, j * 128 : (j + 1) * 128]
            mean = jnp.sum(total, axis=-1, keepdims=True) * (1.0 / width)
            scale = lax.rsqrt(mean + EPS)
            out = pl.ds(pl.multiple_of(base + i * step, step), step)
            for c in range(width // 1024):
                at = pl.ds(c * 1024, 1024)
                part = x[rows, at].astype(jnp.float32)
                part = part * scale * gain[:, at].astype(jnp.float32)
                n_s[out, at] = part.astype(jnp.bfloat16)
            return carry

        lax.fori_loop(0, x.shape[0] // step, rows_of, 0, unroll=2)

    base = 0
    for x in xs:
        normalize(x, base)
        base += x.shape[0]
    for k, (w, out) in enumerate(((wo, own), (wp, par))):
        acc = jnp.dot(n_s[...], w[...], preferred_element_type=jnp.float32)
        done = before[k].shape[0] if prior else 0
        if prior:
            out[:done] = before[k][...]
        out[done:] = acc.astype(jnp.bfloat16).reshape(-1, half, out.shape[2])


def finish_kernel(count, *refs):
    xs, (own_in, par_in, gain, wo, wp, own, par, n_s) = refs[:count], refs[count:]
    half, width = xs[0].shape
    cols = wo.shape[1]
    piece = width // CHUNKS
    scales = []
    for x in xs:
        total = jnp.zeros((half, 128), jnp.float32)
        for j in range(width // 128):
            part = x[:, j * 128 : (j + 1) * 128].astype(jnp.float32)
            total = total + part * part
        mean = jnp.sum(total, axis=-1, keepdims=True) * (1.0 / width)
        scales.append(lax.rsqrt(mean + EPS))
    sums = [jnp.zeros((count * half, cols), jnp.float32) for _ in range(2)]
    for c in range(CHUNKS):
        at = slice(c * piece, (c + 1) * piece)
        factor = gain[:, at].astype(jnp.float32)
        for k, x in enumerate(xs):
            part = x[:, at].astype(jnp.float32) * scales[k] * factor
            n_s[k * half : (k + 1) * half, at] = part.astype(jnp.bfloat16)
        for k, w in enumerate((wo, wp)):
            sums[k] = sums[k] + jnp.dot(
                n_s[:, at], w[at, :], preferred_element_type=jnp.float32
            )
    done = own_in.shape[0]
    for out, before, acc in zip((own, par), (own_in, par_in), sums):
        out[:done] = before[...]
        out[done:] = acc.astype(jnp.bfloat16).reshape(count, half, cols)


def finish(xs, own, par, gain, wo, wp):
    count, (half, width) = len(xs), xs[0].shape
    cols = wo.shape[1]
    out = jax.ShapeDtypeStruct((count + own.shape[0], half, cols), jnp.bfloat16)
    return pl.pallas_call(
        functools.partial(finish_kernel, count),
        out_shape=(out, out),
        in_specs=[VMEM] * (count + 5),
        out_specs=(VMEM, VMEM),
        scratch_shapes=[pltpu.VMEM((count * half, width), jnp.bfloat16)],
        compiler_params=pltpu.CompilerParams(vmem_limit_bytes=16 * 1024 * 1024),
        cost_estimate=pl.CostEstimate(
            flops=4 * count * half * width * cols,
            bytes_accessed=6 * 1024 * 1024,
            transcendentals=0,
        ),
        name="finish",
    )(*xs, own, par, gain, wo, wp)


def project(xs, gain, wo, wp, half, before=()):
    rows = sum(x.shape[0] for x in xs)
    width, cols = wo.shape
    done = before[0].shape[0] if before else 0
    out = jax.ShapeDtypeStruct((done + rows // half, half, cols), jnp.bfloat16)
    return pl.pallas_call(
        functools.partial(project_kernel, len(xs), bool(before)),
        out_shape=(out, out),
        in_specs=[VMEM] * (len(xs) + len(before) + 3),
        out_specs=(VMEM, VMEM),
        scratch_shapes=[pltpu.VMEM((rows, width), jnp.bfloat16)],
        compiler_params=pltpu.CompilerParams(vmem_limit_bytes=16 * 1024 * 1024),
        cost_estimate=pl.CostEstimate(
            flops=2 * rows * width * 2 * cols,
            bytes_accessed=6 * 1024 * 1024,
            transcendentals=0,
        ),
        name="project",
    )(*xs, *before, gain, wo, wp)


def prepare_kernel(cum, q, fk, fv, ng, gates, qm, small):
    block, cols = gates.shape[1:]
    shape = (cols, cols)
    same = lax.broadcasted_iota(jnp.int32, shape, 0) // HD == (
        lax.broadcasted_iota(jnp.int32, shape, 1) // HD
    )
    first = lax.broadcasted_iota(jnp.int32, (2, cols), 1) < HD
    for p in range(2):
        spread = [jnp.broadcast_to(cum[p, h : h + 1, :], (HD, block)) for h in range(2)]
        gates[p] = jnp.concatenate(spread, axis=0).T
        down = jnp.broadcast_to(q[p : p + 1, :].astype(jnp.float32), shape).T
        qm[p] = jnp.where(same, down, 0.0).astype(jnp.bfloat16)
        fresh = jnp.dot(fk[...], qm[p], preferred_element_type=jnp.float32)
        small[p : p + 1, :] = fresh[p : p + 1] * (HD**-0.5)
    small[2:4, :] = fv[...].astype(jnp.float32)
    small[4:6, :] = jnp.where(first, ng[:, 0:1], ng[:, 1:2])
    small[6:8, :] = jnp.zeros((2, cols), jnp.float32)


def prepare(cum, q, fk, fv, ng):
    block, cols = cum.shape[2], q.shape[1]
    return pl.pallas_call(
        prepare_kernel,
        out_shape=(
            jax.ShapeDtypeStruct((2, block, cols), jnp.float32),
            jax.ShapeDtypeStruct((2, cols, cols), jnp.bfloat16),
            jax.ShapeDtypeStruct((8, cols), jnp.float32),
        ),
        in_specs=[VMEM] * 5,
        out_specs=(VMEM,) * 3,
        compiler_params=pltpu.CompilerParams(vmem_limit_bytes=8 * 1024 * 1024),
        cost_estimate=pl.CostEstimate(
            flops=1024 * 1024, bytes_accessed=1024 * 1024, transcendentals=0
        ),
        name="prepare",
    )(cum, q, fk, fv, ng)


def halves(own, got, places):
    tp = lax.axis_index("tp")
    x, core = tp // 2, lax.rem(tp, 2)
    half = own.shape[1]
    found = []
    for side, ref in enumerate((own, got)):
        which = lax.rem(core + side, 2)
        for k, (off, p) in enumerate(places):
            place = lax.rem(x + jnp.where(which == 0, off, (4 - off) % 4), 4)
            found.append((ref, k, p, pl.multiple_of((place * 2 + which) * half, half)))
    return found


def stored(found, keys, values, sem):
    cols = keys.shape[2]
    copies = []
    for i, (ref, k, p, at) in enumerate(found):
        rows = pl.ds(at, ref.shape[1])
        for j, cache in enumerate((keys, values)):
            copies.append(
                pltpu.make_async_copy(
                    ref.at[k, :, pl.ds(j * cols, cols)], cache.at[p, rows, :], sem.at[i, j]
                )
            )
    return copies


def scored(found, p, gates, qm):
    cols = qm.shape[2]
    parts, seen = [], []
    for ref, k, prompt, at in found:
        if prompt == p:
            part = jnp.dot(ref[k, :, :cols], qm[p], preferred_element_type=jnp.float32)
            parts.append(part * (HD**-0.5) - gates[p, pl.ds(at, ref.shape[1]), :])
            seen.append(ref[k, :, cols:].astype(jnp.float32))
    return jnp.concatenate(parts, axis=0), jnp.concatenate(seen, axis=0)


def early_kernel(own, got, gates, qm, keys, values, state, sem):
    found = halves(own, got, EARLY)
    copies = stored(found, keys, values, sem)
    for copy in copies:
        copy.start()
    for p in range(2):
        scores, seen = scored(found, p, gates, qm)
        top = jnp.max(scores, axis=0, keepdims=True)
        weights = jnp.exp(scores - top)
        state[4 * p : 4 * p + 1, :] = top
        state[4 * p + 1 : 4 * p + 2, :] = jnp.sum(weights, axis=0, keepdims=True)
        state[4 * p + 2 : 4 * p + 3, :] = jnp.sum(weights * seen, axis=0, keepdims=True)
        state[4 * p + 3 : 4 * p + 4, :] = jnp.zeros_like(top)
    for copy in copies:
        copy.wait()


def early(own, got, gates, qm):
    block, cols = gates.shape[1:]
    cache = jax.ShapeDtypeStruct((2, block, cols), jnp.bfloat16)
    return pl.pallas_call(
        early_kernel,
        out_shape=(cache, cache, jax.ShapeDtypeStruct((8, cols), jnp.float32)),
        in_specs=[VMEM] * 4,
        out_specs=(ANY, ANY, VMEM),
        scratch_shapes=[pltpu.SemaphoreType.DMA((2 * len(EARLY), 2))],
        compiler_params=pltpu.CompilerParams(vmem_limit_bytes=8 * 1024 * 1024),
        cost_estimate=pl.CostEstimate(
            flops=64 * 1024 * 1024, bytes_accessed=2 * 1024 * 1024, transcendentals=0
        ),
        name="early",
    )(own, got, gates, qm)


def started(copies):
    for copy in copies:
        copy.start()


def awaited(copies):
    for copy in copies:
        copy.wait()


def at_turn(turn, act):
    first = lax.axis_index("sp") < lax.axis_size("sp") // 2
    pl.when(first if turn == 0 else jnp.logical_not(first))(act)


def late_kernel(
    own, both, gates, qm, small, state, k_in, v_in, keys, values, part, sem
):
    core = lax.rem(lax.axis_index("tp"), 2)
    found = halves(own, both.at[1 - core], LATE)
    copies = stored(found, keys, values, sem)
    at_turn(0, lambda: started(copies))
    members, cols = part.shape[0], gates.shape[2]
    block = gates.shape[1]
    packed = jnp.zeros((1, cols), jnp.float32)
    quarter = lax.broadcasted_iota(jnp.int32, (1, cols), 1) % HD // (HD // 4)
    last = lax.axis_index("sp") == lax.axis_size("sp") - 1
    for p in range(2):
        scores, seen = scored(found, p, gates, qm)
        fresh = small[p : p + 1, :] - (
            gates[p, block - 1 : block, :] + small[4 + p : 5 + p, :]
        )
        fresh = jnp.where(last, fresh, MASKED)
        before = state[4 * p : 4 * p + 1, :]
        top = jnp.maximum(jnp.max(scores, axis=0, keepdims=True), fresh)
        top = jnp.maximum(top, before)
        weights = jnp.exp(scores - top)
        fresh_weight = jnp.exp(fresh - top)
        scale = jnp.exp(before - top)
        total = jnp.sum(weights, axis=0, keepdims=True) + fresh_weight
        total = total + scale * state[4 * p + 1 : 4 * p + 2, :]
        acc = jnp.sum(weights * seen, axis=0, keepdims=True)
        acc = acc + fresh_weight * small[2 + p : 3 + p, :]
        acc = acc + scale * state[4 * p + 2 : 4 * p + 3, :]
        packed = jnp.where(quarter == 2 * p, top, packed)
        packed = jnp.where(quarter == 2 * p + 1, total, packed)
        part[:, :, p * cols : (p + 1) * cols] = jnp.broadcast_to(
            acc[None], (members, 1, cols)
        )
    part[:, :, 2 * cols :] = jnp.broadcast_to(packed[None], (members, 1, cols))
    at_turn(0, lambda: awaited(copies))


def late(own, both, gates, qm, small, state, keys, values, members):
    cols = gates.shape[2]
    cache = jax.ShapeDtypeStruct(keys.shape, keys.dtype)
    return pl.pallas_call(
        late_kernel,
        out_shape=(
            cache,
            cache,
            jax.ShapeDtypeStruct((members, 1, 3 * cols), jnp.float32),
        ),
        in_specs=[VMEM] * 6 + [ANY] * 2,
        out_specs=(ANY, ANY, VMEM),
        input_output_aliases={6: 0, 7: 1},
        scratch_shapes=[pltpu.SemaphoreType.DMA((2 * len(LATE), 2))],
        compiler_params=pltpu.CompilerParams(vmem_limit_bytes=4 * 1024 * 1024),
        cost_estimate=pl.CostEstimate(
            flops=16 * 1024 * 1024, bytes_accessed=1024 * 1024, transcendentals=0
        ),
        name="late",
    )(own, both, gates, qm, small, state, keys, values)


def merge_kernel(parts, own, both, k_in, v_in, keys, values, out, sem):
    core = lax.rem(lax.axis_index("tp"), 2)
    copies = stored(halves(own, both.at[1 - core], LATE), keys, values, sem)
    at_turn(1, lambda: started(copies))
    members, cols = parts.shape[0], out.shape[1]
    packed = parts[:, 0, 2 * cols :]
    quarter = lax.broadcasted_iota(jnp.int32, (members, cols), 1) % HD // (HD // 4)

    def spread(which):
        only = jnp.where(quarter == which, packed, 0.0)
        found = only
        for to in range(4):
            if to != which:
                found = found + pltpu.roll(only, (to - which) * (HD // 4) % cols, 1)
        return found

    for p in range(2):
        tops = spread(2 * p)
        scale = jnp.exp(tops - jnp.max(tops, axis=0, keepdims=True))
        total = jnp.sum(scale * spread(2 * p + 1), axis=0, keepdims=True)
        acc = parts[:, 0, p * cols : (p + 1) * cols]
        acc = jnp.sum(scale * acc, axis=0, keepdims=True)
        out[p : p + 1, :] = (acc / total).astype(jnp.bfloat16)
    at_turn(1, lambda: awaited(copies))


def merge(parts, own, both, keys, values):
    cache = jax.ShapeDtypeStruct(keys.shape, keys.dtype)
    return pl.pallas_call(
        merge_kernel,
        out_shape=(cache, cache, jax.ShapeDtypeStruct((2, keys.shape[2]), jnp.bfloat16)),
        in_specs=[VMEM] * 3 + [ANY] * 2,
        out_specs=(ANY, ANY, VMEM),
        input_output_aliases={3: 0, 4: 1},
        scratch_shapes=[pltpu.SemaphoreType.DMA((2 * len(LATE), 2))],
        compiler_params=pltpu.CompilerParams(vmem_limit_bytes=4 * 1024 * 1024),
        name="merge",
    )(parts, own, both, keys, values)


def split_kernel(tokens, a, b):
    a[...] = tokens[0]
    b[...] = tokens[1]


def split(tokens):
    piece = jax.ShapeDtypeStruct(tokens.shape[1:], tokens.dtype)
    return pl.pallas_call(
        split_kernel,
        out_shape=(piece, piece),
        in_specs=[VMEM],
        out_specs=(VMEM, VMEM),
        compiler_params=pltpu.CompilerParams(vmem_limit_bytes=4 * 1024 * 1024),
        cost_estimate=pl.CostEstimate(
            flops=1024 * 1024, bytes_accessed=2 * 1024 * 1024, transcendentals=0
        ),
        name="split",
    )(tokens)


def shift(x, by):
    return lax.ppermute(x, "tp", by)


def body(
    tokens, norm_gain, key_weight, value_weight, cum_gates, new_query, new_key, new_value, new_gate
):
    members = lax.axis_size("sp")
    tps = lax.axis_size("tp")
    ahead = [(i, (i + 2 - 4 * (i % 2)) % tps) for i in range(tps)]
    back = [(i, (i - 2 + 4 * (i % 2)) % tps) for i in range(tps)]
    swap = [(i, i ^ 1) for i in range(tps)]
    gain = norm_gain.reshape(1, -1)
    half, width = tokens.shape[1:]
    from_3 = shift(tokens, ahead)
    a_0, b_0 = split(tokens)
    b_1 = shift(b_0, back)
    a_1 = shift(a_0, back)
    b_2 = shift(b_1, back)
    a_3 = from_3[0]
    a_2 = shift(a_3, ahead)
    wo = jnp.concatenate([key_weight, value_weight], axis=1)
    wp = shift(wo, swap)

    made = prepare(
        jnp.swapaxes(cum_gates, 1, 2), new_query, new_key, new_value, new_gate
    )
    gain, wp, made = lax.optimization_barrier((gain, wp, made))
    gates, qm, small = made

    rows = (2 * half, width)
    done = project((tokens.reshape(rows),), gain, wo, wp, half)
    own1, par1 = project(
        (from_3.reshape(rows), b_1), gain, wo, wp, half, done
    )
    got1 = shift(par1, swap)
    done = project((a_1, b_2), gain, wo, wp, half)
    keys, values, state = early(own1, got1, gates, qm)
    own2, par2 = finish((a_2,), *done, gain, wo, wp)
    pairs = [[i, i + 1] for i in range(0, tps, 2)]
    both2 = lax.all_gather(par2, "tp", axis_index_groups=pairs)
    keys, values, part = late(
        own2, both2, gates, qm, small, state, keys, values, members
    )
    parts = lax.all_to_all(part, "sp", split_axis=0, concat_axis=0, tiled=True)
    return merge(parts, own2, both2, keys, values)


def solution(mesh):
    in_specs = (
        P("gr", ("sp", "tp"), None),
        P(),
        P(None, "tp"),
        P(None, "tp"),
        P("gr", "sp", "tp"),
        P("gr", "tp"),
        P("gr", "tp"),
        P("gr", "tp"),
        P("gr", "tp"),
    )
    out_specs = (P("gr", "sp", "tp"), P("gr", "sp", "tp"), P("gr", "tp"))
    return jax.shard_map(body, mesh=mesh, in_specs=in_specs, out_specs=out_specs, check_vma=False)
```

```python
import functools

import jax
import jax.numpy as jnp
from jax import lax
from jax.experimental import pallas as pl
from jax.experimental.pallas import tpu as pltpu
from jax.sharding import PartitionSpec as P


HD = 64
EPS = 1e-06
MASKED = -1e30
CHUNKS = 16


VMEM = pl.BlockSpec(memory_space=pltpu.VMEM)
ANY = pl.BlockSpec(memory_space=pl.ANY)

EARLY = ((0, 0), (0, 1), (1, 0), (1, 1), (3, 1))
LATE = ((3, 0), (2, 0), (2, 1))


def project_kernel(count, prior, *refs):
    xs, refs = refs[:count], refs[count:]
    before, (gain, wo, wp, own, par, n_s) = refs[: 2 * prior], refs[2 * prior :]
    width = xs[0].shape[1]
    half = own.shape[1]
    step = 16

    def normalize(x, base):
        def rows_of(i, carry):
            rows = pl.ds(pl.multiple_of(i * step, step), step)
            total = jnp.zeros((step, 128), jnp.float32)
            for c in range(width // 1024):
                part = x[rows, pl.ds(c * 1024, 1024)].astype(jnp.float32)
                part = part * part
                for j in range(8):
                    total = total + part[:, j * 128 : (j + 1) * 128]
            mean = jnp.sum(total, axis=-1, keepdims=True) * (1.0 / width)
            scale = lax.rsqrt(mean + EPS)
            out = pl.ds(pl.multiple_of(base + i * step, step), step)
            for c in range(width // 1024):
                at = pl.ds(c * 1024, 1024)
                part = x[rows, at].astype(jnp.float32)
                part = part * scale * gain[:, at].astype(jnp.float32)
                n_s[out, at] = part.astype(jnp.bfloat16)
            return carry

        lax.fori_loop(0, x.shape[0] // step, rows_of, 0, unroll=2)

    base = 0
    for x in xs:
        normalize(x, base)
        base += x.shape[0]
    for k, (w, out) in enumerate(((wo, own), (wp, par))):
        acc = jnp.dot(n_s[...], w[...], preferred_element_type=jnp.float32)
        done = before[k].shape[0] if prior else 0
        if prior:
            out[:done] = before[k][...]
        out[done:] = acc.astype(jnp.bfloat16).reshape(-1, half, out.shape[2])


def finish_kernel(count, *refs):
    xs, (own_in, par_in, gain, wo, wp, own, par, n_s) = refs[:count], refs[count:]
    half, width = xs[0].shape
    cols = wo.shape[1]
    piece = width // CHUNKS
    scales = []
    for x in xs:
        total = jnp.zeros((half, 128), jnp.float32)
        for j in range(width // 128):
            part = x[:, j * 128 : (j + 1) * 128].astype(jnp.float32)
            total = total + part * part
        mean = jnp.sum(total, axis=-1, keepdims=True) * (1.0 / width)
        scales.append(lax.rsqrt(mean + EPS))
    sums = [jnp.zeros((count * half, cols), jnp.float32) for _ in range(2)]
    for c in range(CHUNKS):
        at = slice(c * piece, (c + 1) * piece)
        factor = gain[:, at].astype(jnp.float32)
        for k, x in enumerate(xs):
            part = x[:, at].astype(jnp.float32) * scales[k] * factor
            n_s[k * half : (k + 1) * half, at] = part.astype(jnp.bfloat16)
        for k, w in enumerate((wo, wp)):
            sums[k] = sums[k] + jnp.dot(
                n_s[:, at], w[at, :], preferred_element_type=jnp.float32
            )
    done = own_in.shape[0]
    for out, before, acc in zip((own, par), (own_in, par_in), sums):
        out[:done] = before[...]
        out[done:] = acc.astype(jnp.bfloat16).reshape(count, half, cols)


def finish(xs, own, par, gain, wo, wp):
    count, (half, width) = len(xs), xs[0].shape
    cols = wo.shape[1]
    out = jax.ShapeDtypeStruct((count + own.shape[0], half, cols), jnp.bfloat16)
    return pl.pallas_call(
        functools.partial(finish_kernel, count),
        out_shape=(out, out),
        in_specs=[VMEM] * (count + 5),
        out_specs=(VMEM, VMEM),
        scratch_shapes=[pltpu.VMEM((count * half, width), jnp.bfloat16)],
        compiler_params=pltpu.CompilerParams(vmem_limit_bytes=16 * 1024 * 1024),
        cost_estimate=pl.CostEstimate(
            flops=4 * count * half * width * cols,
            bytes_accessed=6 * 1024 * 1024,
            transcendentals=0,
        ),
        name="finish",
    )(*xs, own, par, gain, wo, wp)


def project(xs, gain, wo, wp, half, before=()):
    rows = sum(x.shape[0] for x in xs)
    width, cols = wo.shape
    done = before[0].shape[0] if before else 0
    out = jax.ShapeDtypeStruct((done + rows // half, half, cols), jnp.bfloat16)
    return pl.pallas_call(
        functools.partial(project_kernel, len(xs), bool(before)),
        out_shape=(out, out),
        in_specs=[VMEM] * (len(xs) + len(before) + 3),
        out_specs=(VMEM, VMEM),
        scratch_shapes=[pltpu.VMEM((rows, width), jnp.bfloat16)],
        compiler_params=pltpu.CompilerParams(vmem_limit_bytes=16 * 1024 * 1024),
        cost_estimate=pl.CostEstimate(
            flops=2 * rows * width * 2 * cols,
            bytes_accessed=6 * 1024 * 1024,
            transcendentals=0,
        ),
        name="project",
    )(*xs, *before, gain, wo, wp)


def prepare_kernel(cum, q, fk, fv, ng, gates, qm, small):
    block, cols = gates.shape[1:]
    shape = (cols, cols)
    same = lax.broadcasted_iota(jnp.int32, shape, 0) // HD == (
        lax.broadcasted_iota(jnp.int32, shape, 1) // HD
    )
    first = lax.broadcasted_iota(jnp.int32, (2, cols), 1) < HD
    for p in range(2):
        spread = [jnp.broadcast_to(cum[p, h : h + 1, :], (HD, block)) for h in range(2)]
        gates[p] = jnp.concatenate(spread, axis=0).T
        down = jnp.broadcast_to(q[p : p + 1, :].astype(jnp.float32), shape).T
        qm[p] = jnp.where(same, down, 0.0).astype(jnp.bfloat16)
        fresh = jnp.dot(fk[...], qm[p], preferred_element_type=jnp.float32)
        small[p : p + 1, :] = fresh[p : p + 1] * (HD**-0.5)
    small[2:4, :] = fv[...].astype(jnp.float32)
    small[4:6, :] = jnp.where(first, ng[:, 0:1], ng[:, 1:2])
    small[6:8, :] = jnp.zeros((2, cols), jnp.float32)


def prepare(cum, q, fk, fv, ng):
    block, cols = cum.shape[2], q.shape[1]
    return pl.pallas_call(
        prepare_kernel,
        out_shape=(
            jax.ShapeDtypeStruct((2, block, cols), jnp.float32),
            jax.ShapeDtypeStruct((2, cols, cols), jnp.bfloat16),
            jax.ShapeDtypeStruct((8, cols), jnp.float32),
        ),
        in_specs=[VMEM] * 5,
        out_specs=(VMEM,) * 3,
        compiler_params=pltpu.CompilerParams(vmem_limit_bytes=8 * 1024 * 1024),
        cost_estimate=pl.CostEstimate(
            flops=1024 * 1024, bytes_accessed=1024 * 1024, transcendentals=0
        ),
        name="prepare",
    )(cum, q, fk, fv, ng)


def halves(own, got, places):
    tp = lax.axis_index("tp")
    x, core = tp // 2, lax.rem(tp, 2)
    half = own.shape[1]
    found = []
    for side, ref in enumerate((own, got)):
        which = lax.rem(core + side, 2)
        for k, (off, p) in enumerate(places):
            place = lax.rem(x + jnp.where(which == 0, off, (4 - off) % 4), 4)
            found.append((ref, k, p, pl.multiple_of((place * 2 + which) * half, half)))
    return found


def stored(found, keys, values, sem):
    cols = keys.shape[2]
    copies = []
    for i, (ref, k, p, at) in enumerate(found):
        rows = pl.ds(at, ref.shape[1])
        for j, cache in enumerate((keys, values)):
            copies.append(
                pltpu.make_async_copy(
                    ref.at[k, :, pl.ds(j * cols, cols)], cache.at[p, rows, :], sem.at[i, j]
                )
            )
    return copies


def scored(found, p, gates, qm):
    cols = qm.shape[2]
    parts, seen = [], []
    for ref, k, prompt, at in found:
        if prompt == p:
            part = jnp.dot(ref[k, :, :cols], qm[p], preferred_element_type=jnp.float32)
            parts.append(part * (HD**-0.5) - gates[p, pl.ds(at, ref.shape[1]), :])
            seen.append(ref[k, :, cols:].astype(jnp.float32))
    return jnp.concatenate(parts, axis=0), jnp.concatenate(seen, axis=0)


def early_kernel(own, got, gates, qm, keys, values, state, sem):
    found = halves(own, got, EARLY)
    copies = stored(found, keys, values, sem)
    for copy in copies:
        copy.start()
    for p in range(2):
        scores, seen = scored(found, p, gates, qm)
        top = jnp.max(scores, axis=0, keepdims=True)
        weights = jnp.exp(scores - top)
        state[4 * p : 4 * p + 1, :] = top
        state[4 * p + 1 : 4 * p + 2, :] = jnp.sum(weights, axis=0, keepdims=True)
        state[4 * p + 2 : 4 * p + 3, :] = jnp.sum(weights * seen, axis=0, keepdims=True)
        state[4 * p + 3 : 4 * p + 4, :] = jnp.zeros_like(top)
    for copy in copies:
        copy.wait()


def early(own, got, gates, qm):
    block, cols = gates.shape[1:]
    cache = jax.ShapeDtypeStruct((2, block, cols), jnp.bfloat16)
    return pl.pallas_call(
        early_kernel,
        out_shape=(cache, cache, jax.ShapeDtypeStruct((8, cols), jnp.float32)),
        in_specs=[VMEM] * 4,
        out_specs=(ANY, ANY, VMEM),
        scratch_shapes=[pltpu.SemaphoreType.DMA((2 * len(EARLY), 2))],
        compiler_params=pltpu.CompilerParams(vmem_limit_bytes=8 * 1024 * 1024),
        cost_estimate=pl.CostEstimate(
            flops=64 * 1024 * 1024, bytes_accessed=2 * 1024 * 1024, transcendentals=0
        ),
        name="early",
    )(own, got, gates, qm)


def started(copies):
    for copy in copies:
        copy.start()


def awaited(copies):
    for copy in copies:
        copy.wait()


def at_turn(turn, act):
    first = lax.axis_index("sp") < lax.axis_size("sp") // 2
    pl.when(first if turn == 0 else jnp.logical_not(first))(act)


def late_kernel(
    own, both, gates, qm, small, state, k_in, v_in, keys, values, part, sem
):
    core = lax.rem(lax.axis_index("tp"), 2)
    found = halves(own, both.at[1 - core], LATE)
    copies = stored(found, keys, values, sem)
    at_turn(0, lambda: started(copies))
    members, cols = part.shape[0], gates.shape[2]
    block = gates.shape[1]
    packed = jnp.zeros((1, cols), jnp.float32)
    quarter = lax.broadcasted_iota(jnp.int32, (1, cols), 1) % HD // (HD // 4)
    last = lax.axis_index("sp") == lax.axis_size("sp") - 1
    for p in range(2):
        scores, seen = scored(found, p, gates, qm)
        fresh = small[p : p + 1, :] - (
            gates[p, block - 1 : block, :] + small[4 + p : 5 + p, :]
        )
        fresh = jnp.where(last, fresh, MASKED)
        before = state[4 * p : 4 * p + 1, :]
        top = jnp.maximum(jnp.max(scores, axis=0, keepdims=True), fresh)
        top = jnp.maximum(top, before)
        weights = jnp.exp(scores - top)
        fresh_weight = jnp.exp(fresh - top)
        scale = jnp.exp(before - top)
        total = jnp.sum(weights, axis=0, keepdims=True) + fresh_weight
        total = total + scale * state[4 * p + 1 : 4 * p + 2, :]
        acc = jnp.sum(weights * seen, axis=0, keepdims=True)
        acc = acc + fresh_weight * small[2 + p : 3 + p, :]
        acc = acc + scale * state[4 * p + 2 : 4 * p + 3, :]
        packed = jnp.where(quarter == 2 * p, top, packed)
        packed = jnp.where(quarter == 2 * p + 1, total, packed)
        part[:, :, p * cols : (p + 1) * cols] = jnp.broadcast_to(
            acc[None], (members, 1, cols)
        )
    part[:, :, 2 * cols :] = jnp.broadcast_to(packed[None], (members, 1, cols))
    at_turn(0, lambda: awaited(copies))


def late(own, both, gates, qm, small, state, keys, values, members):
    cols = gates.shape[2]
    cache = jax.ShapeDtypeStruct(keys.shape, keys.dtype)
    return pl.pallas_call(
        late_kernel,
        out_shape=(
            cache,
            cache,
            jax.ShapeDtypeStruct((members, 1, 3 * cols), jnp.float32),
        ),
        in_specs=[VMEM] * 6 + [ANY] * 2,
        out_specs=(ANY, ANY, VMEM),
        input_output_aliases={6: 0, 7: 1},
        scratch_shapes=[pltpu.SemaphoreType.DMA((2 * len(LATE), 2))],
        compiler_params=pltpu.CompilerParams(vmem_limit_bytes=4 * 1024 * 1024),
        cost_estimate=pl.CostEstimate(
            flops=16 * 1024 * 1024, bytes_accessed=1024 * 1024, transcendentals=0
        ),
        name="late",
    )(own, both, gates, qm, small, state, keys, values)


def merge_kernel(parts, own, both, k_in, v_in, keys, values, out, sem):
    core = lax.rem(lax.axis_index("tp"), 2)
    copies = stored(halves(own, both.at[1 - core], LATE), keys, values, sem)
    at_turn(1, lambda: started(copies))
    members, cols = parts.shape[0], out.shape[1]
    packed = parts[:, 0, 2 * cols :]
    quarter = lax.broadcasted_iota(jnp.int32, (members, cols), 1) % HD // (HD // 4)

    def spread(which):
        only = jnp.where(quarter == which, packed, 0.0)
        found = only
        for to in range(4):
            if to != which:
                found = found + pltpu.roll(only, (to - which) * (HD // 4) % cols, 1)
        return found

    for p in range(2):
        tops = spread(2 * p)
        scale = jnp.exp(tops - jnp.max(tops, axis=0, keepdims=True))
        total = jnp.sum(scale * spread(2 * p + 1), axis=0, keepdims=True)
        acc = parts[:, 0, p * cols : (p + 1) * cols]
        acc = jnp.sum(scale * acc, axis=0, keepdims=True)
        out[p : p + 1, :] = (acc / total).astype(jnp.bfloat16)
    at_turn(1, lambda: awaited(copies))


def merge(parts, own, both, keys, values):
    cache = jax.ShapeDtypeStruct(keys.shape, keys.dtype)
    return pl.pallas_call(
        merge_kernel,
        out_shape=(cache, cache, jax.ShapeDtypeStruct((2, keys.shape[2]), jnp.bfloat16)),
        in_specs=[VMEM] * 3 + [ANY] * 2,
        out_specs=(ANY, ANY, VMEM),
        input_output_aliases={3: 0, 4: 1},
        scratch_shapes=[pltpu.SemaphoreType.DMA((2 * len(LATE), 2))],
        compiler_params=pltpu.CompilerParams(vmem_limit_bytes=4 * 1024 * 1024),
        name="merge",
    )(parts, own, both, keys, values)


def split_kernel(tokens, a, b):
    a[...] = tokens[0]
    b[...] = tokens[1]


def split(tokens):
    piece = jax.ShapeDtypeStruct(tokens.shape[1:], tokens.dtype)
    return pl.pallas_call(
        split_kernel,
        out_shape=(piece, piece),
        in_specs=[VMEM],
        out_specs=(VMEM, VMEM),
        compiler_params=pltpu.CompilerParams(vmem_limit_bytes=4 * 1024 * 1024),
        cost_estimate=pl.CostEstimate(
            flops=1024 * 1024, bytes_accessed=2 * 1024 * 1024, transcendentals=0
        ),
        name="split",
    )(tokens)


def shift(x, by):
    return lax.ppermute(x, "tp", by)


def body(
    tokens, norm_gain, key_weight, value_weight, cum_gates, new_query, new_key, new_value, new_gate
):
    members = lax.axis_size("sp")
    tps = lax.axis_size("tp")
    ahead = [(i, (i - 2 + 4 * (i % 2)) % tps) for i in range(tps)]
    back = [(i, (i + 2 - 4 * (i % 2)) % tps) for i in range(tps)]
    swap = [(i, i ^ 1) for i in range(tps)]
    gain = norm_gain.reshape(1, -1)
    half, width = tokens.shape[1:]
    whole = shift(tokens, ahead)
    a_0, b_0 = split(tokens)
    b_far = shift(b_0, back)
    a_far = shift(a_0, back)
    b_2 = shift(b_far, back)
    a_half = whole[0]
    a_2 = shift(a_half, ahead)
    wo = jnp.concatenate([key_weight, value_weight], axis=1)
    wp = shift(wo, swap)

    made = prepare(
        jnp.swapaxes(cum_gates, 1, 2), new_query, new_key, new_value, new_gate
    )
    gain, wp, made = lax.optimization_barrier((gain, wp, made))
    gates, qm, small = made

    rows = (2 * half, width)
    done = project((tokens.reshape(rows),), gain, wo, wp, half)
    own1, par1 = project(
        (whole.reshape(rows), b_far), gain, wo, wp, half, done
    )
    got1 = shift(par1, swap)
    done = project((a_far, a_2), gain, wo, wp, half)
    keys, values, state = early(own1, got1, gates, qm)
    own2, par2 = finish((b_2,), *done, gain, wo, wp)
    pairs = [[i, i + 1] for i in range(0, tps, 2)]
    both2 = lax.all_gather(par2, "tp", axis_index_groups=pairs)
    keys, values, part = late(
        own2, both2, gates, qm, small, state, keys, values, members
    )
    parts = lax.all_to_all(part, "sp", split_axis=0, concat_axis=0, tiled=True)
    return merge(parts, own2, both2, keys, values)


def solution(mesh):
    in_specs = (
        P("gr", ("sp", "tp"), None),
        P(),
        P(None, "tp"),
        P(None, "tp"),
        P("gr", "sp", "tp"),
        P("gr", "tp"),
        P("gr", "tp"),
        P("gr", "tp"),
        P("gr", "tp"),
    )
    out_specs = (P("gr", "sp", "tp"), P("gr", "sp", "tp"), P("gr", "tp"))
    return jax.shard_map(body, mesh=mesh, in_specs=in_specs, out_specs=out_specs, check_vma=False)
```

```python
import functools

import jax
import jax.numpy as jnp
from jax import lax
from jax.experimental import pallas as pl
from jax.experimental.pallas import tpu as pltpu
from jax.sharding import PartitionSpec as P


HD = 64
EPS = 1e-06
MASKED = -1e30
CHUNKS = 16


VMEM = pl.BlockSpec(memory_space=pltpu.VMEM)
ANY = pl.BlockSpec(memory_space=pl.ANY)

EARLY = ((0, 0), (0, 1), (3, 0), (3, 1), (1, 1))
LATE = ((1, 0), (2, 0), (2, 1))


def project_kernel(count, prior, *refs):
    xs, refs = refs[:count], refs[count:]
    before, (gain, wo, wp, own, par, n_s) = refs[: 2 * prior], refs[2 * prior :]
    width = xs[0].shape[1]
    half = own.shape[1]
    step = 16

    def normalize(x, base):
        def rows_of(i, carry):
            rows = pl.ds(pl.multiple_of(i * step, step), step)
            total = jnp.zeros((step, 128), jnp.float32)
            for c in range(width // 1024):
                part = x[rows, pl.ds(c * 1024, 1024)].astype(jnp.float32)
                part = part * part
                for j in range(8):
                    total = total + part[:, j * 128 : (j + 1) * 128]
            mean = jnp.sum(total, axis=-1, keepdims=True) * (1.0 / width)
            scale = lax.rsqrt(mean + EPS)
            out = pl.ds(pl.multiple_of(base + i * step, step), step)
            for c in range(width // 1024):
                at = pl.ds(c * 1024, 1024)
                part = x[rows, at].astype(jnp.float32)
                part = part * scale * gain[:, at].astype(jnp.float32)
                n_s[out, at] = part.astype(jnp.bfloat16)
            return carry

        lax.fori_loop(0, x.shape[0] // step, rows_of, 0, unroll=2)

    base = 0
    for x in xs:
        normalize(x, base)
        base += x.shape[0]
    for k, (w, out) in enumerate(((wo, own), (wp, par))):
        acc = jnp.dot(n_s[...], w[...], preferred_element_type=jnp.float32)
        done = before[k].shape[0] if prior else 0
        if prior:
            out[:done] = before[k][...]
        out[done:] = acc.astype(jnp.bfloat16).reshape(-1, half, out.shape[2])


def finish_kernel(count, *refs):
    xs, (own_in, par_in, gain, wo, wp, own, par, n_s) = refs[:count], refs[count:]
    half, width = xs[0].shape
    cols = wo.shape[1]
    piece = width // CHUNKS
    scales = []
    for x in xs:
        total = jnp.zeros((half, 128), jnp.float32)
        for j in range(width // 128):
            part = x[:, j * 128 : (j + 1) * 128].astype(jnp.float32)
            total = total + part * part
        mean = jnp.sum(total, axis=-1, keepdims=True) * (1.0 / width)
        scales.append(lax.rsqrt(mean + EPS))
    sums = [jnp.zeros((count * half, cols), jnp.float32) for _ in range(2)]
    for c in range(CHUNKS):
        at = slice(c * piece, (c + 1) * piece)
        factor = gain[:, at].astype(jnp.float32)
        for k, x in enumerate(xs):
            part = x[:, at].astype(jnp.float32) * scales[k] * factor
            n_s[k * half : (k + 1) * half, at] = part.astype(jnp.bfloat16)
        for k, w in enumerate((wo, wp)):
            sums[k] = sums[k] + jnp.dot(
                n_s[:, at], w[at, :], preferred_element_type=jnp.float32
            )
    done = own_in.shape[0]
    for out, before, acc in zip((own, par), (own_in, par_in), sums):
        out[:done] = before[...]
        out[done:] = acc.astype(jnp.bfloat16).reshape(count, half, cols)


def finish(xs, own, par, gain, wo, wp):
    count, (half, width) = len(xs), xs[0].shape
    cols = wo.shape[1]
    out = jax.ShapeDtypeStruct((count + own.shape[0], half, cols), jnp.bfloat16)
    return pl.pallas_call(
        functools.partial(finish_kernel, count),
        out_shape=(out, out),
        in_specs=[VMEM] * (count + 5),
        out_specs=(VMEM, VMEM),
        scratch_shapes=[pltpu.VMEM((count * half, width), jnp.bfloat16)],
        compiler_params=pltpu.CompilerParams(vmem_limit_bytes=16 * 1024 * 1024),
        cost_estimate=pl.CostEstimate(
            flops=4 * count * half * width * cols,
            bytes_accessed=6 * 1024 * 1024,
            transcendentals=0,
        ),
        name="finish",
    )(*xs, own, par, gain, wo, wp)


def project(xs, gain, wo, wp, half, before=()):
    rows = sum(x.shape[0] for x in xs)
    width, cols = wo.shape
    done = before[0].shape[0] if before else 0
    out = jax.ShapeDtypeStruct((done + rows // half, half, cols), jnp.bfloat16)
    return pl.pallas_call(
        functools.partial(project_kernel, len(xs), bool(before)),
        out_shape=(out, out),
        in_specs=[VMEM] * (len(xs) + len(before) + 3),
        out_specs=(VMEM, VMEM),
        scratch_shapes=[pltpu.VMEM((rows, width), jnp.bfloat16)],
        compiler_params=pltpu.CompilerParams(vmem_limit_bytes=16 * 1024 * 1024),
        cost_estimate=pl.CostEstimate(
            flops=2 * rows * width * 2 * cols,
            bytes_accessed=6 * 1024 * 1024,
            transcendentals=0,
        ),
        name="project",
    )(*xs, *before, gain, wo, wp)


def prepare_kernel(cum, q, fk, fv, ng, gates, qm, small):
    block, cols = gates.shape[1:]
    shape = (cols, cols)
    same = lax.broadcasted_iota(jnp.int32, shape, 0) // HD == (
        lax.broadcasted_iota(jnp.int32, shape, 1) // HD
    )
    first = lax.broadcasted_iota(jnp.int32, (2, cols), 1) < HD
    for p in range(2):
        spread = [jnp.broadcast_to(cum[p, h : h + 1, :], (HD, block)) for h in range(2)]
        gates[p] = jnp.concatenate(spread, axis=0).T
        down = jnp.broadcast_to(q[p : p + 1, :].astype(jnp.float32), shape).T
        qm[p] = jnp.where(same, down, 0.0).astype(jnp.bfloat16)
        fresh = jnp.dot(fk[...], qm[p], preferred_element_type=jnp.float32)
        small[p : p + 1, :] = fresh[p : p + 1] * (HD**-0.5)
    small[2:4, :] = fv[...].astype(jnp.float32)
    small[4:6, :] = jnp.where(first, ng[:, 0:1], ng[:, 1:2])
    small[6:8, :] = jnp.zeros((2, cols), jnp.float32)


def prepare(cum, q, fk, fv, ng):
    block, cols = cum.shape[2], q.shape[1]
    return pl.pallas_call(
        prepare_kernel,
        out_shape=(
            jax.ShapeDtypeStruct((2, block, cols), jnp.float32),
            jax.ShapeDtypeStruct((2, cols, cols), jnp.bfloat16),
            jax.ShapeDtypeStruct((8, cols), jnp.float32),
        ),
        in_specs=[VMEM] * 5,
        out_specs=(VMEM,) * 3,
        compiler_params=pltpu.CompilerParams(vmem_limit_bytes=8 * 1024 * 1024),
        cost_estimate=pl.CostEstimate(
            flops=1024 * 1024, bytes_accessed=1024 * 1024, transcendentals=0
        ),
        name="prepare",
    )(cum, q, fk, fv, ng)


def halves(own, got, places):
    tp = lax.axis_index("tp")
    x, core = tp // 2, lax.rem(tp, 2)
    half = own.shape[1]
    found = []
    for side, ref in enumerate((own, got)):
        which = lax.rem(core + side, 2)
        for k, (off, p) in enumerate(places):
            place = lax.rem(x + jnp.where(which == 0, off, (4 - off) % 4), 4)
            found.append((ref, k, p, pl.multiple_of((place * 2 + which) * half, half)))
    return found


def stored(found, keys, values, sem):
    cols = keys.shape[2]
    copies = []
    for i, (ref, k, p, at) in enumerate(found):
        rows = pl.ds(at, ref.shape[1])
        for j, cache in enumerate((keys, values)):
            copies.append(
                pltpu.make_async_copy(
                    ref.at[k, :, pl.ds(j * cols, cols)], cache.at[p, rows, :], sem.at[i, j]
                )
            )
    return copies


def scored(found, p, gates, qm):
    cols = qm.shape[2]
    parts, seen = [], []
    for ref, k, prompt, at in found:
        if prompt == p:
            part = jnp.dot(ref[k, :, :cols], qm[p], preferred_element_type=jnp.float32)
            parts.append(part * (HD**-0.5) - gates[p, pl.ds(at, ref.shape[1]), :])
            seen.append(ref[k, :, cols:].astype(jnp.float32))
    return jnp.concatenate(parts, axis=0), jnp.concatenate(seen, axis=0)


def early_kernel(own, got, gates, qm, keys, values, state, sem):
    found = halves(own, got, EARLY)
    copies = stored(found, keys, values, sem)
    for copy in copies:
        copy.start()
    for p in range(2):
        scores, seen = scored(found, p, gates, qm)
        top = jnp.max(scores, axis=0, keepdims=True)
        weights = jnp.exp(scores - top)
        state[4 * p : 4 * p + 1, :] = top
        state[4 * p + 1 : 4 * p + 2, :] = jnp.sum(weights, axis=0, keepdims=True)
        state[4 * p + 2 : 4 * p + 3, :] = jnp.sum(weights * seen, axis=0, keepdims=True)
        state[4 * p + 3 : 4 * p + 4, :] = jnp.zeros_like(top)
    for copy in copies:
        copy.wait()


def early(own, got, gates, qm):
    block, cols = gates.shape[1:]
    cache = jax.ShapeDtypeStruct((2, block, cols), jnp.bfloat16)
    return pl.pallas_call(
        early_kernel,
        out_shape=(cache, cache, jax.ShapeDtypeStruct((8, cols), jnp.float32)),
        in_specs=[VMEM] * 4,
        out_specs=(ANY, ANY, VMEM),
        scratch_shapes=[pltpu.SemaphoreType.DMA((2 * len(EARLY), 2))],
        compiler_params=pltpu.CompilerParams(vmem_limit_bytes=8 * 1024 * 1024),
        cost_estimate=pl.CostEstimate(
            flops=64 * 1024 * 1024, bytes_accessed=2 * 1024 * 1024, transcendentals=0
        ),
        name="early",
    )(own, got, gates, qm)


def started(copies):
    for copy in copies:
        copy.start()


def awaited(copies):
    for copy in copies:
        copy.wait()


def at_turn(turn, act):
    first = lax.axis_index("sp") < lax.axis_size("sp") // 2
    pl.when(first if turn == 0 else jnp.logical_not(first))(act)


def late_kernel(
    own, both, gates, qm, small, state, k_in, v_in, keys, values, part, sem
):
    core = lax.rem(lax.axis_index("tp"), 2)
    found = halves(own, both.at[1 - core], LATE)
    copies = stored(found, keys, values, sem)
    at_turn(0, lambda: started(copies))
    members, cols = part.shape[0], gates.shape[2]
    block = gates.shape[1]
    packed = jnp.zeros((1, cols), jnp.float32)
    quarter = lax.broadcasted_iota(jnp.int32, (1, cols), 1) % HD // (HD // 4)
    last = lax.axis_index("sp") == lax.axis_size("sp") - 1
    for p in range(2):
        scores, seen = scored(found, p, gates, qm)
        fresh = small[p : p + 1, :] - (
            gates[p, block - 1 : block, :] + small[4 + p : 5 + p, :]
        )
        fresh = jnp.where(last, fresh, MASKED)
        before = state[4 * p : 4 * p + 1, :]
        top = jnp.maximum(jnp.max(scores, axis=0, keepdims=True), fresh)
        top = jnp.maximum(top, before)
        weights = jnp.exp(scores - top)
        fresh_weight = jnp.exp(fresh - top)
        scale = jnp.exp(before - top)
        total = jnp.sum(weights, axis=0, keepdims=True) + fresh_weight
        total = total + scale * state[4 * p + 1 : 4 * p + 2, :]
        acc = jnp.sum(weights * seen, axis=0, keepdims=True)
        acc = acc + fresh_weight * small[2 + p : 3 + p, :]
        acc = acc + scale * state[4 * p + 2 : 4 * p + 3, :]
        packed = jnp.where(quarter == 2 * p, top, packed)
        packed = jnp.where(quarter == 2 * p + 1, total, packed)
        part[:, :, p * cols : (p + 1) * cols] = jnp.broadcast_to(
            acc[None], (members, 1, cols)
        )
    part[:, :, 2 * cols :] = jnp.broadcast_to(packed[None], (members, 1, cols))
    at_turn(0, lambda: awaited(copies))


def late(own, both, gates, qm, small, state, keys, values, members):
    cols = gates.shape[2]
    cache = jax.ShapeDtypeStruct(keys.shape, keys.dtype)
    return pl.pallas_call(
        late_kernel,
        out_shape=(
            cache,
            cache,
            jax.ShapeDtypeStruct((members, 1, 3 * cols), jnp.float32),
        ),
        in_specs=[VMEM] * 6 + [ANY] * 2,
        out_specs=(ANY, ANY, VMEM),
        input_output_aliases={6: 0, 7: 1},
        scratch_shapes=[pltpu.SemaphoreType.DMA((2 * len(LATE), 2))],
        compiler_params=pltpu.CompilerParams(vmem_limit_bytes=4 * 1024 * 1024),
        cost_estimate=pl.CostEstimate(
            flops=16 * 1024 * 1024, bytes_accessed=1024 * 1024, transcendentals=0
        ),
        name="late",
    )(own, both, gates, qm, small, state, keys, values)


def merge_kernel(parts, own, both, k_in, v_in, keys, values, out, sem):
    core = lax.rem(lax.axis_index("tp"), 2)
    copies = stored(halves(own, both.at[1 - core], LATE), keys, values, sem)
    at_turn(1, lambda: started(copies))
    members, cols = parts.shape[0], out.shape[1]
    packed = parts[:, 0, 2 * cols :]
    quarter = lax.broadcasted_iota(jnp.int32, (members, cols), 1) % HD // (HD // 4)

    def spread(which):
        only = jnp.where(quarter == which, packed, 0.0)
        found = only
        for to in range(4):
            if to != which:
                found = found + pltpu.roll(only, (to - which) * (HD // 4) % cols, 1)
        return found

    for p in range(2):
        tops = spread(2 * p)
        scale = jnp.exp(tops - jnp.max(tops, axis=0, keepdims=True))
        total = jnp.sum(scale * spread(2 * p + 1), axis=0, keepdims=True)
        acc = parts[:, 0, p * cols : (p + 1) * cols]
        acc = jnp.sum(scale * acc, axis=0, keepdims=True)
        out[p : p + 1, :] = (acc / total).astype(jnp.bfloat16)
    at_turn(1, lambda: awaited(copies))


def merge(parts, own, both, keys, values):
    cache = jax.ShapeDtypeStruct(keys.shape, keys.dtype)
    return pl.pallas_call(
        merge_kernel,
        out_shape=(cache, cache, jax.ShapeDtypeStruct((2, keys.shape[2]), jnp.bfloat16)),
        in_specs=[VMEM] * 3 + [ANY] * 2,
        out_specs=(ANY, ANY, VMEM),
        input_output_aliases={3: 0, 4: 1},
        scratch_shapes=[pltpu.SemaphoreType.DMA((2 * len(LATE), 2))],
        compiler_params=pltpu.CompilerParams(vmem_limit_bytes=4 * 1024 * 1024),
        name="merge",
    )(parts, own, both, keys, values)


def split_kernel(tokens, a, b):
    a[...] = tokens[0]
    b[...] = tokens[1]


def split(tokens):
    piece = jax.ShapeDtypeStruct(tokens.shape[1:], tokens.dtype)
    return pl.pallas_call(
        split_kernel,
        out_shape=(piece, piece),
        in_specs=[VMEM],
        out_specs=(VMEM, VMEM),
        compiler_params=pltpu.CompilerParams(vmem_limit_bytes=4 * 1024 * 1024),
        cost_estimate=pl.CostEstimate(
            flops=1024 * 1024, bytes_accessed=2 * 1024 * 1024, transcendentals=0
        ),
        name="split",
    )(tokens)


def shift(x, by):
    return lax.ppermute(x, "tp", by)


def body(
    tokens, norm_gain, key_weight, value_weight, cum_gates, new_query, new_key, new_value, new_gate
):
    members = lax.axis_size("sp")
    tps = lax.axis_size("tp")
    ahead = [(i, (i + 2 - 4 * (i % 2)) % tps) for i in range(tps)]
    back = [(i, (i - 2 + 4 * (i % 2)) % tps) for i in range(tps)]
    swap = [(i, i ^ 1) for i in range(tps)]
    gain = norm_gain.reshape(1, -1)
    half, width = tokens.shape[1:]
    from_3 = shift(tokens, ahead)
    a_0, b_0 = split(tokens)
    b_1 = shift(b_0, back)
    a_1 = shift(a_0, back)
    b_2 = shift(b_1, back)
    a_3 = from_3[0]
    a_2 = shift(a_3, ahead)
    wo = jnp.concatenate([key_weight, value_weight], axis=1)
    wp = shift(wo, swap)

    made = prepare(
        jnp.swapaxes(cum_gates, 1, 2), new_query, new_key, new_value, new_gate
    )
    gain, wp, made = lax.optimization_barrier((gain, wp, made))
    gates, qm, small = made

    rows = (2 * half, width)
    done = project((tokens.reshape(rows),), gain, wo, wp, half)
    own1, par1 = project(
        (from_3.reshape(rows), b_1), gain, wo, wp, half, done
    )
    got1 = shift(par1, swap)
    done = project((a_1, a_2), gain, wo, wp, half)
    keys, values, state = early(own1, got1, gates, qm)
    own2, par2 = finish((b_2,), *done, gain, wo, wp)
    pairs = [[i, i + 1] for i in range(0, tps, 2)]
    both2 = lax.all_gather(par2, "tp", axis_index_groups=pairs)
    keys, values, part = late(
        own2, both2, gates, qm, small, state, keys, values, members
    )
    parts = lax.all_to_all(part, "sp", split_axis=0, concat_axis=0, tiled=True)
    return merge(parts, own2, both2, keys, values)


def solution(mesh):
    in_specs = (
        P("gr", ("sp", "tp"), None),
        P(),
        P(None, "tp"),
        P(None, "tp"),
        P("gr", "sp", "tp"),
        P("gr", "tp"),
        P("gr", "tp"),
        P("gr", "tp"),
        P("gr", "tp"),
    )
    out_specs = (P("gr", "sp", "tp"), P("gr", "sp", "tp"), P("gr", "tp"))
    return jax.shard_map(body, mesh=mesh, in_specs=in_specs, out_specs=out_specs, check_vma=False)
```
